32 devices in a mesh: sp: 8 (over z, y), tp: 4 (over x, core).
Axes of the slice: x: 2, y: 2, z: 4, core: 2. Of those that a mesh axis runs over, the one named last changes fastest.
Arguments:
- gate_in: bfloat16 [4096, 2048], P('sp', 'tp'), may hold values from -6 to 6
- value_in: bfloat16 [4096, 2048], P('sp', 'tp'), may hold values from -6 to 6
- gate_out: bfloat16 [4096, 2048], P('sp', 'tp'), may hold values from -6 to 6
- conv_taps: float32 [3, 2048], P(None, 'tp'), may hold values from -3.5 to 3.5
- proj_weight: bfloat16 [2048, 2048], P('tp'), may hold values from -0.125 to 0.125
- residual: bfloat16 [4096, 2048], P(('sp', 'tp')), may hold values from -6 to 6
- norm_gain: float32 [2048], replicated, may hold values from 0.1 to 1.9
- routes: int32 [4096, 2], P('sp'), may hold values from 0 to 7, all different within a row; in each aligned block of 128 rows (0 to 127, 128 to 255, ...) at most 64 rows name the same one
- route_weight: float32 [4096, 2], P('sp'), may hold values from 0.1 to 0.9
- expert_gate: bfloat16 [8, 2048, 2048], P('sp', None, 'tp'), may hold values from -0.125 to 0.125
- expert_up: bfloat16 [8, 2048, 2048], P('sp', None, 'tp'), may hold values from -0.125 to 0.125
- expert_down: bfloat16 [8, 2048, 2048], P('sp', 'tp'), may hold values from -0.125 to 0.125
Outputs:
- layer_out: bfloat16 [4096, 2048], P(('sp', 'tp'))
The draws below stay inside these ranges and needn't reach their ends.
Inputs may be any that keep to these rules, and one draw needn't show every extreme that they name: `routes`: A token's 2 experts differ. In each aligned block of 128 tokens no expert is named by more than 64 tokens, a bound that some block reaches.
All inputs are finite; a program needn't handle non-finite values.
Results may differ from the reference program's by a relative error of at most 0.012.
Values may be sent and summed in bfloat16 or wider, within the bound.
A program may use at most 128 MiB of HBM per device.

```python
import math
import jax
import jax.numpy as jnp
import numpy as np
from jax import lax

D = 2048
FE = 2048
TOP = 2
TAPS = 3
TOK_DEV = 512
TOKQ = 128
EXPERTS = 8
CAPQ = 64
TOKENS = 4096
N_SP = 8
N_TP = 4


def levels(key, shape, shards, least, largest):
    gain, own = 1.0, jax.random.fold_in(key, 6)
    for position, blocks in shards:
        heights = jnp.exp(jax.random.uniform(jax.random.fold_in(own, position), (blocks,), jnp.float32, least / len(shards), largest / len(shards)))
        gain = gain * jnp.repeat(heights, shape[position] // blocks).reshape([-1 if axis == position else 1 for axis in range(len(shape))])
    return gain


def routed_block(key, own, number, rows, count, top, bound, lean):
    sequence = jax.random.permutation(key, count)
    heavy_load, ordinary = shares(count, rows * top, bound, lean, True), shares(count, rows * top, bound, lean, False)
    places = jnp.arange(count)

    def named(lengths, rotation):
        used = int((lengths > 0).sum())
        fixed = max(1, used // 4)
        moved = fixed + (places - fixed + rotation * (used - fixed)) % max(1, count - fixed)
        return jnp.zeros((count,), jnp.int32).at[sequence[jnp.where(places < fixed, places, moved)]].set(jnp.asarray(lengths, jnp.int32))

    lengths = jnp.where(number % 4 == 0, named(heavy_load, number // 4), named(ordinary, number - number // 4 - 1))
    mixed = jax.random.permutation(jax.random.fold_in(own, 3), count)
    giver, sink = mixed[0:count // 2 * 2:2], mixed[1:count // 2 * 2:2]
    slack = jnp.minimum(lengths[giver] - 1, bound - lengths[sink]) // 2
    slack = jnp.where((giver == sequence[0]) | (sink == sequence[0]) | (lengths[sink] == 0), 0, jnp.maximum(slack, 0))
    moved = jax.random.randint(jax.random.fold_in(own, 4), (count // 2,), 0, 1 << 20) % (slack + 1)
    lengths = lengths.at[giver].add(-moved).at[sink].add(moved)
    items = jnp.searchsorted(jnp.cumsum(lengths), jnp.arange(rows * top), side="right").astype(jnp.int32)
    table = items.reshape(top, rows).T
    table = table[jax.random.permutation(jax.random.fold_in(own, 1), rows)]
    rotation = jax.random.randint(jax.random.fold_in(own, 2), (rows, 1), 0, top)
    return jnp.take_along_axis(table, (jnp.arange(top)[None, :] + rotation) % top, axis=1)


def shares(count, total, most, slope, full):
    loads = [(1 << 20) // math.isqrt(rank ** slope) + 1 for rank in range(1, count + 1)]
    largest = most if full else min(most, max(-(-total // count), total * loads[0] // sum(loads)))
    least = 1 if total - largest >= count - 1 else 0
    given, rest = [largest] + [least] * (count - 1), total - largest - least * (count - 1)
    while rest > 0:
        candidates = [i for i in range(1, count) if given[i] < largest] or [i for i in range(1, count) if given[i] < most]
        pool, left = sum([loads[i] for i in candidates]), rest
        for i in candidates:
            extra = min(most - given[i], max(1, left * loads[i] // pool), rest)
            given[i] = given[i] + extra
            rest = rest - extra
    return np.array(given)


def bell_draw(key, extent, spread, reach, cuts=(), kind=jnp.bfloat16):
    array = jax.random.normal(key, extent, jnp.float32) * spread
    if len(cuts) > 0:
        array = levels(key, extent, cuts, -0.22, 0.18) * array
    return jnp.clip(array, min=-reach, max=reach).astype(kind)


def setup_inputs(seed: int = 0) -> dict:
    key_list = jax.random.split(jax.random.key(seed), 13)
    gate_in = bell_draw(key_list[0], (TOKENS, D), 1.0, 6.0, ((0, 8), (1, 4)))
    value_in = bell_draw(key_list[1], (TOKENS, D), 1.0, 6.0, ((0, 8), (1, 4)))
    gate_out = bell_draw(key_list[2], (TOKENS, D), 1.0, 6.0, ((0, 8), (1, 4)))
    conv_taps = bell_draw(key_list[3], (TAPS, D), TAPS ** -0.5, 3.5, ((1, 4),), jnp.float32)
    proj_weight = bell_draw(key_list[4], (D, D), D ** -0.5, 0.125, ((0, 4),))
    residual = bell_draw(key_list[5], (TOKENS, D), 1.0, 6.0, ((0, 32),))
    norm_gain = jnp.clip(1.0 + 0.18 * jax.random.normal(key_list[6], (D,), jnp.float32), 0.1, 1.9)
    routes_keys = jax.random.split(jax.random.fold_in(key_list[7], 1), TOKENS // TOKQ)
    routes_turns = jax.random.permutation(jax.random.fold_in(key_list[7], 3), TOKENS // TOKQ)
    routes = jax.vmap(lambda own, number: routed_block(jax.random.fold_in(key_list[7], 2), own, number, TOKQ, EXPERTS, TOP, CAPQ, 2))(routes_keys, routes_turns).reshape((TOKENS, TOP))
    route_weight = jnp.clip(0.1 + 0.79999997 * jax.random.uniform(key_list[8], (TOKENS, TOP), jnp.float32) ** levels(key_list[8], (TOKENS, TOP), ((0, 8),), -0.2, 0.2), 0.1, 0.9)
    expert_gate = bell_draw(key_list[9], (EXPERTS, D, FE), D ** -0.5, 0.125, ((0, 8), (2, 4)))
    expert_up = bell_draw(key_list[10], (EXPERTS, D, FE), D ** -0.5, 0.125, ((0, 8), (2, 4)))
    expert_down = bell_draw(key_list[11], (EXPERTS, FE, D), FE ** -0.5, 0.125, ((0, 8), (1, 4)))
    return dict(gate_in=gate_in, value_in=value_in, gate_out=gate_out, conv_taps=conv_taps, proj_weight=proj_weight, residual=residual, norm_gain=norm_gain, routes=routes, route_weight=route_weight, expert_gate=expert_gate, expert_up=expert_up, expert_down=expert_down)


def rounded(values):
    return lax.optimization_barrier(values.astype(jnp.bfloat16)).astype(jnp.float32)

def slot_numbers(route_ids, block_rows, expert_count):
    block_count = route_ids.shape[0] // block_rows
    flat_ids = route_ids.reshape(block_count, block_rows * route_ids.shape[1])
    one_hot = (flat_ids[:, :, None] == jnp.arange(expert_count, dtype=jnp.int32)[None, None, :]).astype(jnp.int32)
    before = jnp.cumsum(one_hot, axis=1) - one_hot
    return lax.optimization_barrier(jnp.sum(before * one_hot, axis=2)).reshape(route_ids.shape).astype(jnp.int32)

def normalize(hidden_rows, norm_gain):
    inverse = lax.rsqrt(lax.optimization_barrier(jnp.mean(hidden_rows * hidden_rows, axis=-1, keepdims=True)) + 1e-05)
    return (hidden_rows * inverse * norm_gain.astype(jnp.float32)).astype(jnp.bfloat16)

def mixer_output(gate_in, value_in, gate_out, conv_taps, prior_gate, prior_value):
    product = gate_in.astype(jnp.float32) * value_in.astype(jnp.float32)
    prior_mix = prior_gate.astype(jnp.float32) * prior_value.astype(jnp.float32)
    padded = jnp.concatenate([prior_mix, product], axis=0)
    taps = conv_taps.astype(jnp.float32)
    conv_sum = taps[0] * padded[:-2] + taps[1] * padded[1:-1] + taps[2] * padded[2:]
    return (gate_out.astype(jnp.float32) * conv_sum).astype(jnp.bfloat16)

def reference(gate_in, value_in, gate_out, conv_taps, proj_weight, residual, norm_gain, routes, route_weight, expert_gate, expert_up, expert_down):
    model_width = residual.shape[1]
    zero_rows = jnp.zeros((2, gate_in.shape[1]), jnp.bfloat16)
    mixed_out = mixer_output(gate_in, value_in, gate_out, conv_taps, zero_rows, zero_rows)
    slice_width = model_width // N_TP
    summed = jnp.zeros(residual.shape, jnp.float32)
    for group in range(N_TP):
        lower = group * slice_width
        summed = summed + rounded(jnp.dot(mixed_out[:, lower:lower + slice_width], proj_weight[lower:lower + slice_width], preferred_element_type=jnp.float32))
    hidden_rows = residual.astype(jnp.float32) + summed
    normed = normalize(hidden_rows, norm_gain)
    token_count = residual.shape[0]
    top_count = routes.shape[1]
    slots = slot_numbers(routes, TOKQ, EXPERTS)
    token_ids = jnp.arange(token_count, dtype=jnp.int32)
    source = token_ids // TOK_DEV
    quarter = token_ids % TOK_DEV // TOKQ
    flat_index = ((routes * N_TP + quarter[:, None]) * N_SP + source[:, None]) * CAPQ + slots
    per_expert = N_TP * N_SP * CAPQ
    slot_count = EXPERTS * per_expert
    slot_token = jnp.full((slot_count,), token_count, jnp.int32).at[flat_index.reshape(-1)].set(jnp.repeat(token_ids, top_count))
    slot_weight = jnp.zeros((slot_count,), jnp.float32).at[flat_index.reshape(-1)].set(route_weight.reshape(-1))
    padded_rows = jnp.concatenate([normed, jnp.zeros((1, model_width), jnp.bfloat16)], axis=0)
    hidden_width = expert_gate.shape[2] // N_TP

    def one_expert(total, expert):
        start_row = (expert * per_expert).astype(jnp.int32)
        chosen = lax.dynamic_slice_in_dim(slot_token, start_row, per_expert, 0)
        weights_now = lax.dynamic_slice_in_dim(slot_weight, start_row, per_expert, 0)
        row_block = padded_rows[chosen]
        gate_pre = jnp.dot(row_block, expert_gate[expert], preferred_element_type=jnp.float32)
        up_pre = jnp.dot(row_block, expert_up[expert], preferred_element_type=jnp.float32)
        hidden = (jax.nn.silu(gate_pre) * up_pre).astype(jnp.bfloat16)
        down_weight = expert_down[expert]
        partial_sum = jnp.zeros((per_expert, model_width), jnp.float32)
        for group in range(N_TP):
            lower = group * hidden_width
            partial_sum = partial_sum + rounded(jnp.dot(hidden[:, lower:lower + hidden_width], down_weight[lower:lower + hidden_width], preferred_element_type=jnp.float32))
        expert_rows = rounded(partial_sum)
        total = total.at[chosen].add(weights_now[:, None] * expert_rows)
        return (total, None)
    total, _ = lax.scan(one_expert, jnp.zeros((token_count + 1, model_width), jnp.float32), jnp.arange(EXPERTS, dtype=jnp.int32))
    return (hidden_rows + total[:token_count]).astype(jnp.bfloat16)
```

```python
import functools

import jax
import jax.numpy as jnp
from jax import lax
from jax.experimental import pallas as pl
from jax.experimental.pallas import tpu as pltpu
from jax.sharding import PartitionSpec as P


def slot_numbers(route_ids, block_rows, expert_count):
    block_count = route_ids.shape[0] // block_rows
    flat_ids = route_ids.reshape(block_count, block_rows * route_ids.shape[1])
    one_hot = (
        flat_ids[:, :, None] == jnp.arange(expert_count, dtype=jnp.int32)[None, None, :]
    ).astype(jnp.int32)
    before = jnp.cumsum(one_hot, axis=1) - one_hot
    return jnp.sum(before * one_hot, axis=2).reshape(route_ids.shape)


def dispatch_rows(normed, flat_pick, slot_count):
    slot_ids = jnp.arange(slot_count, dtype=jnp.int32)
    chosen = jnp.any(flat_pick[None, :, :] == slot_ids[:, None, None], axis=2)
    return jnp.dot(
        chosen.astype(jnp.bfloat16), normed, preferred_element_type=jnp.float32
    ).astype(jnp.bfloat16)


MESH = pl.DeviceIdType.MESH


def mixer_kernel(
    n, tp, halo, pieces, gate_ref, value_ref, out_gate_ref, taps_ref, proj_ref, res_ref, gain_ref,
    rows_ref, normed_ref, edge, product, mixed, part, mrecv, psum, xrecv, send, got,
):
    s = lax.axis_index("sp")
    t = lax.axis_index("tp")
    mate = t + 1 - 2 * (t % 2)
    across = (t + 2) % tp
    mate_across = (mate + 2) % tp
    tokens = gate_ref.shape[0]
    quarter, width = res_ref.shape
    piece = quarter // pieces
    after, before = (s + 1) % n, (s + n - 1) % n

    barrier = pltpu.get_barrier_semaphore()
    for peer in ((s, mate), (s, across), (after, t), (before, t)):
        pl.semaphore_signal(barrier, inc=1, device_id=peer, device_id_type=MESH)

    def remote(src, dst, lane, device):
        return pltpu.make_async_remote_copy(
            src_ref=src,
            dst_ref=dst,
            send_sem=send.at[lane],
            recv_sem=got.at[lane],
            device_id=device,
            device_id_type=MESH,
        )

    tail = pl.ds(tokens - halo, halo)
    edges = [
        remote(ref.at[tail], edge.at[i], i, (after, t))
        for i, ref in enumerate((gate_ref, value_ref))
    ]
    pl.semaphore_wait(barrier, 4)
    for copy in edges:
        copy.start()

    body_rows = pl.ds(halo, tokens)
    product[body_rows] = gate_ref[...].astype(jnp.float32) * value_ref[...].astype(jnp.float32)
    for copy in edges:
        copy.wait_recv()
    prior = edge[0].astype(jnp.float32) * edge[1].astype(jnp.float32)
    product[pl.ds(0, halo)] = jnp.where(s == 0, 0.0, prior)
    conv_sum = (
        taps_ref[0:1] * product[pl.ds(halo - 2, tokens)]
        + taps_ref[1:2] * product[pl.ds(halo - 1, tokens)]
        + taps_ref[2:3] * product[body_rows]
    )
    mixed[...] = (out_gate_ref[...].astype(jnp.float32) * conv_sum).astype(jnp.bfloat16)

    def project(block, p):
        first = pl.multiple_of(block * quarter + p * piece, piece)
        y = jnp.dot(
            mixed[pl.ds(first, piece)], proj_ref[...], preferred_element_type=jnp.float32
        )
        part[block, p] = y.astype(jnp.bfloat16)

    def lane(kind, p):
        return 2 + kind * pieces + p

    def to_mate(kind, block, p):
        return remote(part.at[block, p], mrecv.at[kind, p], lane(kind, p), (s, mate))

    def over(p):
        return remote(psum.at[p], xrecv.at[p], lane(2, p), (s, across))

    def wide(block):
        return block.astype(jnp.float32)

    for p in range(pieces):
        project(mate_across, p)
        to_mate(0, mate_across, p).start()
    for p in range(pieces):
        project(across, p)
        to_mate(0, mate_across, p).wait_recv()
        psum[p] = (wide(part[across, p]) + wide(mrecv[0, p])).astype(jnp.bfloat16)
        over(p).start()
    for p in range(pieces):
        project(mate, p)
        to_mate(1, mate, p).start()
    for p in range(pieces):
        project(t, p)
    for p in range(pieces):
        to_mate(1, mate, p).wait_recv()
        over(p).wait_recv()
        at = pl.ds(p * piece, piece)
        summed = wide(part[t, p]) + wide(mrecv[1, p]) + wide(xrecv[p])
        hidden_rows = wide(res_ref[at]) + summed
        inverse = lax.rsqrt(jnp.mean(hidden_rows * hidden_rows, axis=-1, keepdims=True) + 1e-05)
        rows_ref[at] = hidden_rows
        normed_ref[at] = (hidden_rows * inverse * gain_ref[...]).astype(jnp.bfloat16)
    for copy in edges:
        copy.wait_send()
    for p in range(pieces):
        to_mate(0, mate_across, p).wait_send()
        to_mate(1, mate, p).wait_send()
        over(p).wait_send()


def run_mixer(gate_in, value_in, gate_out, conv_taps, proj_weight, residual, norm_gain):
    n, tp = lax.axis_size("sp"), lax.axis_size("tp")
    tokens, channels = gate_in.shape
    quarter, width = residual.shape
    halo, pieces = 16, 4
    piece = quarter // pieces
    vmem = pl.BlockSpec(memory_space=pltpu.VMEM)
    bf16, f32 = jnp.bfloat16, jnp.float32
    return pl.pallas_call(
        functools.partial(mixer_kernel, n, tp, halo, pieces),
        out_shape=(
            jax.ShapeDtypeStruct((quarter, width), f32),
            jax.ShapeDtypeStruct((quarter, width), bf16),
        ),
        in_specs=[vmem] * 7,
        out_specs=(vmem, vmem),
        scratch_shapes=[
            pltpu.VMEM((2, halo, channels), bf16),
            pltpu.VMEM((halo + tokens, channels), f32),
            pltpu.VMEM((tokens, channels), bf16),
            pltpu.VMEM((tp, pieces, piece, width), bf16),
            pltpu.VMEM((2, pieces, piece, width), bf16),
            pltpu.VMEM((pieces, piece, width), bf16),
            pltpu.VMEM((pieces, piece, width), bf16),
            pltpu.SemaphoreType.DMA((2 + 3 * pieces,)),
            pltpu.SemaphoreType.DMA((2 + 3 * pieces,)),
        ],
        compiler_params=pltpu.CompilerParams(
            collective_id=2, has_side_effects=True, vmem_limit_bytes=60 * 1024 * 1024
        ),
    )(gate_in, value_in, gate_out, conv_taps, proj_weight, residual, norm_gain.reshape(1, width))


def expert_kernel(
    n, tp, halves, out_ref, gate_hbm, up_hbm, down_hbm, ret_ref,
    recv, part, mrecv, psum, xrecv, fin, gate_w, up_w, down_w, hid, local_sem, send, got,
):
    s = lax.axis_index("sp")
    t = lax.axis_index("tp")
    mate = t + 1 - 2 * (t % 2)
    across = (t + 2) % tp
    mate_across = (mate + 2) % tp
    cap, width = out_ref.shape[1], out_ref.shape[2]
    units = gate_w.shape[1]
    rows = tp * cap
    steps = n * halves

    weight_copies = [
        pltpu.make_async_copy(src, dst, local_sem.at[i])
        for i, (src, dst) in enumerate(
            [(gate_hbm, gate_w), (up_hbm, up_w), (down_hbm, down_w)]
        )
    ]
    for copy in weight_copies:
        copy.start()

    barrier = pltpu.get_barrier_semaphore()

    @pl.loop(1, n)
    def _(k):
        pl.semaphore_signal(barrier, inc=1, device_id=((s + k) % n, t), device_id_type=MESH)

    for peer in (mate, across):
        pl.semaphore_signal(barrier, inc=1, device_id=(s, peer), device_id_type=MESH)
    pl.semaphore_wait(barrier, n + 1)

    def remote(src, dst, lane, k, device):
        return pltpu.make_async_remote_copy(
            src_ref=src,
            dst_ref=dst,
            send_sem=send.at[lane, k],
            recv_sem=got.at[lane, k],
            device_id=device,
            device_id_type=MESH,
        )

    def outward(k):
        to = (s + k // halves) % n
        return remote(out_ref.at[to * halves + k % halves], recv.at[k, t], 0, k, (to, t))

    def over(k, block):
        return remote(recv.at[k, block], recv.at[k, block], 1, k, (s, across))

    def pair_own(k, block):
        return remote(recv.at[k, block], recv.at[k, block], 2, k, (s, mate))

    def pair_far(k, block):
        return remote(recv.at[k, block], recv.at[k, block], 3, k, (s, mate))

    def part_near(k):
        return remote(part.at[k, mate], mrecv.at[k, 0], 4, k, (s, mate))

    def part_far(k):
        return remote(part.at[k, mate_across], mrecv.at[k, 1], 5, k, (s, mate))

    def sum_over(k):
        return remote(psum.at[k], xrecv.at[k], 6, k, (s, across))

    def homeward(k):
        to = (s + n - k // halves) % n
        return remote(fin.at[k], ret_ref.at[s * halves + k % halves], 7, k, (to, t))

    own = [
        pltpu.make_async_copy(out_ref.at[s * halves + h], recv.at[h, t], local_sem.at[3 + h])
        for h in range(halves)
    ]
    for copy in own:
        copy.start()

    @pl.loop(halves, steps)
    def _(k):
        outward(k).start()

    for copy in own:
        copy.wait()

    def ffn(k):
        def load():
            block = recv[k]
            if cap % 16:
                return block.astype(jnp.float32).reshape(rows, width).astype(jnp.bfloat16)
            return block.reshape(rows, width)

        cols = min(256, units)

        @pl.loop(0, units // cols)
        def _(c):
            at = pl.ds(pl.multiple_of(c * cols, cols), cols)
            x = load()
            gate = jnp.dot(x, gate_w[:, at], preferred_element_type=jnp.float32)
            up = jnp.dot(x, up_w[:, at], preferred_element_type=jnp.float32)
            hid[:, at] = (gate / (1.0 + jnp.exp(-gate)) * up).astype(jnp.bfloat16)

        wide = min(512, width)

        @pl.loop(0, width // wide)
        def _(c):
            at = pl.ds(pl.multiple_of(c * wide, wide), wide)
            y = jnp.dot(hid[...], down_w[:, at], preferred_element_type=jnp.float32)
            part[k, :, :, at] = y.reshape(tp, cap, wide).astype(jnp.bfloat16)

    def wide_sum(*blocks):
        total = blocks[0].astype(jnp.float32)
        for block in blocks[1:]:
            total = total + block.astype(jnp.float32)
        return total

    @pl.loop(0, steps + 4)
    def _(i):
        @pl.when(i < steps)
        def _():
            @pl.when(i >= halves)
            def _():
                outward(i).wait_recv()

            over(i, t).start()
            pair_own(i, t).start()

        @pl.when((i >= 1) & (i < steps + 1))
        def _():
            k = i - 1
            over(k, across).wait_recv()
            pair_far(k, across).start()

        @pl.when((i >= 3) & (i < steps + 3))
        def _():
            k = i - 3
            part_far(k).wait_recv()
            psum[k] = wide_sum(part[k, across], mrecv[k, 1]).astype(jnp.bfloat16)
            sum_over(k).start()

        @pl.when(i >= 4)
        def _():
            k = i - 4
            part_near(k).wait_recv()
            sum_over(k).wait_recv()
            total = wide_sum(part[k, t], mrecv[k, 0], xrecv[k]).astype(jnp.bfloat16)

            @pl.when(k < halves)
            def _():
                ret_ref[s * halves + k] = total

            @pl.when(k >= halves)
            def _():
                fin[k] = total
                homeward(k).start()

        @pl.when(i == 2)
        def _():
            for copy in weight_copies:
                copy.wait()

        @pl.when((i >= 2) & (i < steps + 2))
        def _():
            k = i - 2
            pair_own(k, mate).wait_recv()
            pair_far(k, mate_across).wait_recv()
            ffn(k)
            part_far(k).start()
            part_near(k).start()

    @pl.loop(0, steps)
    def _(k):
        over(k, t).wait_send()
        pair_own(k, t).wait_send()
        pair_far(k, across).wait_send()
        part_near(k).wait_send()
        part_far(k).wait_send()
        sum_over(k).wait_send()

        @pl.when(k >= halves)
        def _():
            outward(k).wait_send()
            homeward(k).wait_send()
            homeward(k).wait_recv()


def run_experts(outgoing, gate_weight, up_weight, down_weight):
    n, cap, width = outgoing.shape
    tp = lax.axis_size("tp")
    units = gate_weight.shape[1]
    halves = 2 if cap % 32 == 0 else 1
    steps, cap = n * halves, cap // halves
    vmem = pl.BlockSpec(memory_space=pltpu.VMEM)
    hbm = pl.BlockSpec(memory_space=pl.ANY)
    bf16 = jnp.bfloat16
    return pl.pallas_call(
        functools.partial(expert_kernel, n, tp, halves),
        out_shape=jax.ShapeDtypeStruct((steps, cap, width), bf16),
        in_specs=[vmem, hbm, hbm, hbm],
        out_specs=vmem,
        scratch_shapes=[
            pltpu.VMEM((steps, tp, cap, width), bf16),
            pltpu.VMEM((steps, tp, cap, width), bf16),
            pltpu.VMEM((steps, 2, cap, width), bf16),
            pltpu.VMEM((steps, cap, width), bf16),
            pltpu.VMEM((steps, cap, width), bf16),
            pltpu.VMEM((steps, cap, width), bf16),
            pltpu.VMEM(gate_weight.shape, bf16),
            pltpu.VMEM(up_weight.shape, bf16),
            pltpu.VMEM(down_weight.shape, bf16),
            pltpu.VMEM((tp * cap, units), bf16),
            pltpu.SemaphoreType.DMA((3 + halves,)),
            pltpu.SemaphoreType.DMA((8, steps)),
            pltpu.SemaphoreType.DMA((8, steps)),
        ],
        compiler_params=pltpu.CompilerParams(
            collective_id=1, has_side_effects=True, vmem_limit_bytes=60 * 1024 * 1024
        ),
    )(outgoing.reshape(steps, cap, width), gate_weight, up_weight, down_weight)


def exchange_body(
    gate_in,
    value_in,
    gate_out,
    conv_taps,
    proj_weight,
    residual,
    norm_gain,
    routes,
    route_weight,
    expert_gate,
    expert_up,
    expert_down,
):
    model_width = residual.shape[1]
    tp_count = lax.axis_size("tp")
    groups = lax.axis_size("sp")
    quarter = residual.shape[0]
    top_count = routes.shape[1]
    capacity = 2 * quarter * top_count // groups
    tp_index = lax.axis_index("tp")
    first_own = tp_index * quarter
    own_routes = lax.dynamic_slice_in_dim(routes, first_own, quarter, 0)
    own_weights = lax.dynamic_slice_in_dim(route_weight, first_own, quarter, 0)
    my_rows, normed = run_mixer(
        gate_in, value_in, gate_out, conv_taps, proj_weight, residual, norm_gain
    )
    own_slots = slot_numbers(own_routes, quarter, groups)
    flat_pick = own_routes * capacity + own_slots
    slot_count = groups * capacity
    outgoing = dispatch_rows(normed, flat_pick, slot_count)
    returned = run_experts(
        outgoing.reshape(groups, capacity, model_width),
        expert_gate[0],
        expert_up[0],
        expert_down[0],
    ).reshape(slot_count, model_width)
    total = my_rows
    for k in range(top_count):
        pick = flat_pick[:, k, None] == jnp.arange(slot_count, dtype=jnp.int32)
        picked = jnp.dot(
            pick.astype(jnp.bfloat16), returned, preferred_element_type=jnp.float32
        )
        total = total + own_weights[:, k, None] * picked
    return total.astype(jnp.bfloat16)


def plane_of(j, z, planes):
    upper = z >= planes // 2
    near = jnp.where(upper, planes - 1 - z, z)
    swing = jnp.where(j % 2 == 1, near - (j + 1) // 2, near + j // 2)
    place = jnp.where(j <= 2 * near, swing, j)
    return jnp.where(upper, planes - 1 - place, place)


def layer_kernel(
    n, tp, halo, pieces, cap,
    routes_ref, weights_ref, taps_ref, gain_ref,
    gate_hbm, value_hbm, out_gate_hbm, proj_hbm, res_hbm, wg_hbm, wu_hbm, wd_hbm,
    out_ref,
    gate_ref, value_ref, out_gate_ref, proj_ref, res_ref, gate_w, up_w, down_w,
    edge, product, mixed, mpart, mmate, msum, mfar,
    rows, info, spread, raw, ysend, recv, part, mrecv, psum, xrecv, fin, ret, hid,
    local_sem, msend, mgot, isend, igot, rsend, rgot, ysem, ygot, dsend, dgot, psend, pgot, hsend, hgot,
):
    s = lax.axis_index("sp")
    t = lax.axis_index("tp")
    planes = n // 2
    z, y = s // 2, s % 2
    other_y = 1 - y
    mate = t + 1 - 2 * (t % 2)
    across = (t + 2) % tp
    mate_across = (mate + 2) % tp
    tokens = gate_ref.shape[0]
    quarter, width = res_ref.shape
    piece = quarter // pieces
    half = cap // 2
    units = 2 * planes
    after, before = (s + 1) % n, (s + n - 1) % n
    f32, bf16 = jnp.float32, jnp.bfloat16

    loads = [
        pltpu.make_async_copy(src, dst, local_sem.at[i])
        for i, (src, dst) in enumerate(
            [
                (gate_hbm, gate_ref), (value_hbm, value_ref), (out_gate_hbm, out_gate_ref),
                (proj_hbm, proj_ref), (res_hbm, res_ref),
                (wg_hbm, gate_w), (wu_hbm, up_w), (wd_hbm, down_w),
            ]
        )
    ]
    for copy in loads[:5]:
        copy.start()

    barrier = pltpu.get_barrier_semaphore()

    @pl.loop(1, n)
    def _(k):
        pl.semaphore_signal(barrier, inc=1, device_id=((s + k) % n, t), device_id_type=MESH)

    for peer in (mate, across):
        pl.semaphore_signal(barrier, inc=1, device_id=(s, peer), device_id_type=MESH)

    def remote(src, dst, send_sem, recv_sem, device):
        return pltpu.make_async_remote_copy(
            src_ref=src, dst_ref=dst, send_sem=send_sem, recv_sem=recv_sem,
            device_id=device, device_id_type=MESH,
        )

    own_at = pl.ds(pl.multiple_of(t * quarter, quarter), quarter)
    named = [routes_ref[k:k + 1, own_at] for k in range(2)]
    expert_ids = lax.broadcasted_iota(jnp.int32, (n, quarter), 0)
    one_hot = [(expert_ids == name).astype(f32) for name in named]
    earlier = (
        lax.broadcasted_iota(jnp.int32, (quarter, quarter), 0)
        < lax.broadcasted_iota(jnp.int32, (quarter, quarter), 1)
    ).astype(bf16)
    count = jnp.dot(
        (one_hot[0] + one_hot[1]).astype(bf16), earlier, preferred_element_type=f32
    )
    picks = [
        name.astype(f32) * cap + jnp.sum(count * hot, axis=0, keepdims=True)
        for name, hot in zip(named, one_hot)
    ]
    info[z] = jnp.concatenate(picks + [jnp.zeros((6, quarter), f32)], axis=0)

    for copy in loads[:2]:
        copy.wait()
    tail = pl.ds(tokens - halo, halo)
    edges = [
        remote(ref.at[tail], edge.at[i], msend.at[i], mgot.at[i], (after, t))
        for i, ref in enumerate((gate_ref, value_ref))
    ]
    pl.semaphore_wait(barrier, n + 1)
    for copy in edges:
        copy.start()

    def tell(k):
        to = (z + k) % planes
        return remote(info.at[z], info.at[z], isend.at[k], igot.at[z], (to * 2 + y, t))

    def told(k):
        origin = (z + k) % planes
        return remote(info.at[origin], info.at[origin], isend.at[k], igot.at[origin], (s, mate))

    @pl.loop(1, planes)
    def _(k):
        tell(k).start()

    for copy in loads[5:]:
        copy.start()

    body_rows = pl.ds(halo, tokens)
    product[body_rows] = gate_ref[...].astype(f32) * value_ref[...].astype(f32)
    for copy in edges:
        copy.wait_recv()
    prior = edge[0].astype(f32) * edge[1].astype(f32)
    product[pl.ds(0, halo)] = jnp.where(s == 0, 0.0, prior)
    conv_sum = (
        taps_ref[0:1] * product[pl.ds(halo - 2, tokens)]
        + taps_ref[1:2] * product[pl.ds(halo - 1, tokens)]
        + taps_ref[2:3] * product[body_rows]
    )
    loads[2].wait()
    mixed[...] = (out_gate_ref[...].astype(f32) * conv_sum).astype(bf16)
    loads[3].wait()

    def project(block, p):
        first = pl.multiple_of(block * quarter + p * piece, piece)
        y_block = jnp.dot(mixed[pl.ds(first, piece)], proj_ref[...], preferred_element_type=f32)
        mpart[block, p] = y_block.astype(bf16)

    def lane(kind, p):
        return 2 + kind * pieces + p

    def to_mate(kind, block, p):
        at = lane(kind, p)
        return remote(mpart.at[block, p], mmate.at[kind, p], msend.at[at], mgot.at[at], (s, mate))

    def to_across(p):
        at = lane(2, p)
        return remote(msum.at[p], mfar.at[p], msend.at[at], mgot.at[at], (s, across))

    for p in range(pieces):
        project(mate_across, p)
        to_mate(0, mate_across, p).start()
    for p in range(pieces):
        project(across, p)
        to_mate(0, mate_across, p).wait_recv()
        msum[p] = (mpart[across, p].astype(f32) + mmate[0, p].astype(f32)).astype(bf16)
        to_across(p).start()
    for p in range(pieces):
        project(mate, p)
        to_mate(1, mate, p).start()
    for p in range(pieces):
        project(t, p)

    slot_ids = lax.broadcasted_iota(jnp.int32, (n * cap, quarter), 0).astype(f32)
    share = jnp.where(slot_ids == picks[0], weights_ref[0:1, own_at], 0.0) + jnp.where(
        slot_ids == picks[1], weights_ref[1:2, own_at], 0.0
    )
    share = jnp.transpose(share)
    high = share.astype(bf16)
    spread[0] = high
    spread[1] = (share - high.astype(f32)).astype(bf16)

    loads[4].wait()
    for p in range(pieces):
        to_mate(1, mate, p).wait_recv()
        to_across(p).wait_recv()
        at = pl.ds(p * piece, piece)
        summed = (
            mpart[t, p].astype(f32) + mmate[1, p].astype(f32) + mfar[p].astype(f32)
        )
        hidden_rows = res_ref[at].astype(f32) + summed
        inverse = lax.rsqrt(jnp.mean(hidden_rows * hidden_rows, axis=-1, keepdims=True) + 1e-05)
        rows[at] = hidden_rows
        raw[z, at] = (hidden_rows * inverse * gain_ref[...]).astype(bf16)

    def along(block, up):
        to = jnp.where(up == 1, z + 1, z - 1)
        return remote(raw.at[block], raw.at[block], rsend.at[up, block], rgot.at[block], (to * 2 + y, t))

    def has_up(block):
        return (block <= z) & (z < planes - 1)

    def has_down(block):
        return (block >= z) & (z > 0)

    def pass_on(block):
        @pl.when(has_up(block))
        def _():
            along(block, 1).start()

        @pl.when(has_down(block))
        def _():
            along(block, 0).start()

    def beside(j, h):
        return remote(
            ysend.at[j, h], recv.at[j, h, t, y], ysem.at[j, h], ygot.at[j, h], (z * 2 + other_y, t)
        )

    def over(j, h, source):
        ref = recv.at[j, h, t, source]
        return remote(ref, ref, dsend.at[0, j, h, source], dgot.at[0, j, h, source], (s, across))

    def pair_own(j, h, source):
        ref = recv.at[j, h, t, source]
        return remote(ref, ref, dsend.at[1, j, h, source], dgot.at[1, j, h, source], (s, mate))

    def pair_far(j, h, source):
        ref = recv.at[j, h, across, source]
        return remote(ref, ref, dsend.at[2, j, h, source], dgot.at[2, j, h, source], (s, mate))

    wide = min(512, width)

    def select(j, block, expert, put):
        place = lax.broadcasted_iota(jnp.int32, (cap, quarter), 0).astype(f32) + (
            expert * cap
        ).astype(f32)
        table = info[block]
        chosen = ((place == table[0:1]) | (place == table[1:2])).astype(f32).astype(bf16)

        @pl.loop(0, width // wide)
        def _(c):
            at = pl.ds(pl.multiple_of(c * wide, wide), wide)
            taken = jnp.dot(chosen, raw[block, :, at], preferred_element_type=f32).astype(bf16)
            for h in range(2):
                put(h, at, taken[h * half:(h + 1) * half])

    def dispatch(j):
        block = plane_of(j, z, planes)

        @pl.when(j > 0)
        def _():
            along(block, 1).wait_recv()

        pass_on(block)

        @pl.when(j > 0)
        def _():
            told((block + planes - z) % planes).wait_recv()

        def put_own(h, at, value):
            recv[j, h, t, y, :, at] = value

        def put_other(h, at, value):
            ysend[j, h, :, at] = value

        select(j, block, s, put_own)
        for h in (1, 0):
            over(j, h, y).start()
        select(j, block, z * 2 + other_y, put_other)
        for h in (1, 0):
            beside(j, h).start()
        for h in (1, 0):
            pair_own(j, h, y).start()

    def dispatch_beside(j):
        for h in (1, 0):
            beside(j, h).wait_recv()
            over(j, h, other_y).start()
            pair_own(j, h, other_y).start()

    def dispatch_far(j):
        for source in (y, other_y):
            for h in (1, 0):
                over(j, h, source).wait_recv()
                pair_far(j, h, source).start()

    def group(u):
        return (u + 1) // 2 % planes, (u + 1) % 2

    def part_near(u):
        return remote(part.at[u, mate], mrecv.at[u, 0], psend.at[0, u], pgot.at[0, u], (s, mate))

    def part_far(u):
        return remote(part.at[u, mate_across], mrecv.at[u, 1], psend.at[1, u], pgot.at[1, u], (s, mate))

    def sum_over(u):
        return remote(psum.at[u], xrecv.at[u], psend.at[2, u], pgot.at[2, u], (s, across))

    def ffn(u):
        j, h = group(u)
        for source in range(2):
            pair_own(j, h, source).wait_recv()
            pair_far(j, h, source).wait_recv()
        count = gate_w.shape[1]
        cols = min(256, count)

        @pl.loop(0, count // cols)
        def _(c):
            at = pl.ds(pl.multiple_of(c * cols, cols), cols)
            x = recv[j, h].reshape(tp * cap, width)
            gate = jnp.dot(x, gate_w[:, at], preferred_element_type=f32)
            up = jnp.dot(x, up_w[:, at], preferred_element_type=f32)
            hid[:, at] = (gate / (1.0 + jnp.exp(-gate)) * up).astype(bf16)

        @pl.loop(0, width // wide)
        def _(c):
            at = pl.ds(pl.multiple_of(c * wide, wide), wide)
            out = jnp.dot(hid[...], down_w[:, at], preferred_element_type=f32)
            part[u, :, :, :, at] = out.reshape(tp, 2, half, wide).astype(bf16)

        part_far(u).start()
        part_near(u).start()

    def homeward(u, source):
        j, h = group(u)
        to = plane_of(j, z, planes) * 2 + source
        return remote(fin.at[u, source], ret.at[s, h], hsend.at[u, source], hgot.at[s, h], (to, t))

    def returned(origin, h):
        return remote(ret.at[origin, h], ret.at[origin, h], hsend.at[0, 0], hgot.at[origin, h], (s, mate))

    def sum_far(u):
        part_far(u).wait_recv()
        psum[u] = (part[u, across].astype(f32) + mrecv[u, 1].astype(f32)).astype(bf16)
        sum_over(u).start()

    def send_home(u):
        j, h = group(u)
        part_near(u).wait_recv()
        sum_over(u).wait_recv()
        total = (
            part[u, t].astype(f32) + mrecv[u, 0].astype(f32) + xrecv[u].astype(f32)
        ).astype(bf16)
        fin[u] = total

        @pl.when(j == 0)
        def _():
            ret[s, h] = fin[u, y]
            homeward(u, other_y).start()

        @pl.when(j > 0)
        def _():
            for source in range(2):
                homeward(u, source).start()

    dispatch(0)
    dispatch_beside(0)
    for copy in loads[5:]:
        copy.wait()

    @pl.loop(0, planes + 1)
    def _(j):
        @pl.when(j + 1 < planes)
        def _():
            dispatch(j + 1)

        @pl.when(j < planes)
        def _():
            dispatch_far(j)

        first = 2 * j - 1

        @pl.when(j > 0)
        def _():
            ffn(first)

        @pl.when(j + 1 < planes)
        def _():
            dispatch_beside(j + 1)

        @pl.when(j < planes)
        def _():
            ffn(2 * j)

        @pl.when(j > 0)
        def _():
            sum_far(first)

        @pl.when(j > 1)
        def _():
            send_home(first - 2)

        @pl.when(j > 0)
        def _():
            send_home(first - 1)

        @pl.when(j < planes)
        def _():
            sum_far(2 * j)

    send_home(units - 1)

    def gather(plane, put):
        for source in range(2):
            for h in range(2):
                origin = plane * 2 + source

                @pl.when(origin != s)
                def _():
                    returned(origin, h).wait_recv()

        slots = pl.ds(pl.multiple_of(plane * 2 * cap, 2 * cap), 2 * cap)

        @pl.loop(0, width // wide)
        def _(c):
            at = pl.ds(pl.multiple_of(c * wide, wide), wide)
            got = ret[pl.ds(plane * 2, 2), :, :, at].reshape(2 * cap, wide)
            put(
                at,
                rows[:, at]
                + jnp.dot(spread[0, :, slots], got, preferred_element_type=f32)
                + jnp.dot(spread[1, :, slots], got, preferred_element_type=f32),
            )

    def keep(at, value):
        rows[:, at] = value

    def finish(at, value):
        out_ref[:, at] = value.astype(bf16)

    @pl.loop(1, planes)
    def _(j):
        gather(plane_of(j, z, planes), keep)

    gather(z, finish)

    for copy in edges:
        copy.wait_send()
    for p in range(pieces):
        to_mate(0, mate_across, p).wait_send()
        to_mate(1, mate, p).wait_send()
        to_across(p).wait_send()

    @pl.loop(0, planes)
    def _(j):
        @pl.when(j > 0)
        def _():
            tell(j).wait_send()

        @pl.when(has_up(j))
        def _():
            along(j, 1).wait_send()

        @pl.when(has_down(j))
        def _():
            along(j, 0).wait_send()

        for h in range(2):
            beside(j, h).wait_send()
            for source in range(2):
                over(j, h, source).wait_send()
                pair_own(j, h, source).wait_send()
                pair_far(j, h, source).wait_send()

    @pl.loop(0, units)
    def _(u):
        part_near(u).wait_send()
        part_far(u).wait_send()
        sum_over(u).wait_send()
        j, h = group(u)
        homeward(u, other_y).wait_send()

        @pl.when(j > 0)
        def _():
            homeward(u, y).wait_send()


def relay_body(
    gate_in, value_in, gate_out, conv_taps, proj_weight, residual, norm_gain,
    routes, route_weight, expert_gate, expert_up, expert_down,
):
    n, tp = lax.axis_size("sp"), lax.axis_size("tp")
    tokens, channels = gate_in.shape
    quarter, width = residual.shape
    cap = 2 * quarter * routes.shape[1] // n
    units_hidden = expert_gate.shape[2]
    planes, half = n // 2, cap // 2
    units = 2 * planes
    halo, pieces = 16, 4
    piece = quarter // pieces
    vmem = pl.BlockSpec(memory_space=pltpu.VMEM)
    hbm = pl.BlockSpec(memory_space=pl.ANY)
    bf16, f32 = jnp.bfloat16, jnp.float32
    dma = pltpu.SemaphoreType.DMA
    rows = (2, half, width)
    return pl.pallas_call(
        functools.partial(layer_kernel, n, tp, halo, pieces, cap),
        out_shape=jax.ShapeDtypeStruct((quarter, width), bf16),
        in_specs=[vmem] * 4 + [hbm] * 8,
        out_specs=vmem,
        scratch_shapes=[
            pltpu.VMEM((tokens, channels), bf16),
            pltpu.VMEM((tokens, channels), bf16),
            pltpu.VMEM((tokens, channels), bf16),
            pltpu.VMEM(proj_weight.shape, bf16),
            pltpu.VMEM((quarter, width), bf16),
            pltpu.VMEM((width, units_hidden), bf16),
            pltpu.VMEM((width, units_hidden), bf16),
            pltpu.VMEM((units_hidden, width), bf16),
            pltpu.VMEM((2, halo, channels), bf16),
            pltpu.VMEM((halo + tokens, channels), f32),
            pltpu.VMEM((tokens, channels), bf16),
            pltpu.VMEM((tp, pieces, piece, width), bf16),
            pltpu.VMEM((2, pieces, piece, width), bf16),
            pltpu.VMEM((pieces, piece, width), bf16),
            pltpu.VMEM((pieces, piece, width), bf16),
            pltpu.VMEM((quarter, width), f32),
            pltpu.VMEM((planes, 8, quarter), f32),
            pltpu.VMEM((2, quarter, n * cap), bf16),
            pltpu.VMEM((planes, quarter, width), bf16),
            pltpu.VMEM((planes,) + rows, bf16),
            pltpu.VMEM((planes, 2, tp) + rows, bf16),
            pltpu.VMEM((units, tp) + rows, bf16),
            pltpu.VMEM((units, 2) + rows, bf16),
            pltpu.VMEM((units,) + rows, bf16),
            pltpu.VMEM((units,) + rows, bf16),
            pltpu.VMEM((units,) + rows, bf16),
            pltpu.VMEM((n,) + rows, bf16),
            pltpu.VMEM((tp * cap, units_hidden), bf16),
            dma((8,)),
            dma((2 + 3 * pieces,)),
            dma((2 + 3 * pieces,)),
            dma((planes,)),
            dma((planes,)),
            dma((2, planes)),
            dma((planes,)),
            dma((planes, 2)),
            dma((planes, 2)),
            dma((3, planes, 2, 2)),
            dma((3, planes, 2, 2)),
            dma((3, units)),
            dma((3, units)),
            dma((units, 2)),
            dma((n, 2)),
        ],
        compiler_params=pltpu.CompilerParams(
            collective_id=3, has_side_effects=True, vmem_limit_bytes=60 * 1024 * 1024
        ),
    )(
        routes.T, route_weight.T, conv_taps, norm_gain.reshape(1, width),
        gate_in, value_in, gate_out, proj_weight, residual,
        expert_gate[0], expert_up[0], expert_down[0],
    )


def body(*args):
    residual, routes = args[5], args[7]
    n, tp = lax.axis_size("sp"), lax.axis_size("tp")
    quarter = residual.shape[0]
    capacity = 2 * quarter * routes.shape[1] // n
    relay = n % 2 == 0 and tp == 4 and capacity % 32 == 0 and quarter % 128 == 0
    if relay and (n // 2) * quarter <= n * capacity:
        return relay_body(*args)
    return exchange_body(*args)


def solution(mesh):
    placed = (
        P("sp", "tp"),
        P("sp", "tp"),
        P("sp", "tp"),
        P(None, "tp"),
        P("tp", None),
        P(("sp", "tp"), None),
        P(),
        P("sp", None),
        P("sp", None),
        P("sp", None, "tp"),
        P("sp", None, "tp"),
        P("sp", "tp", None),
    )
    return jax.shard_map(
        body, mesh=mesh, in_specs=placed, out_specs=P(("sp", "tp"), None), check_vma=False
    )
```

```python
import functools

import jax
import jax.numpy as jnp
from jax import lax
from jax.experimental import pallas as pl
from jax.experimental.pallas import tpu as pltpu
from jax.sharding import PartitionSpec as P


def slot_numbers(route_ids, block_rows, expert_count):
    block_count = route_ids.shape[0] // block_rows
    flat_ids = route_ids.reshape(block_count, block_rows * route_ids.shape[1])
    one_hot = (
        flat_ids[:, :, None] == jnp.arange(expert_count, dtype=jnp.int32)[None, None, :]
    ).astype(jnp.int32)
    before = jnp.cumsum(one_hot, axis=1) - one_hot
    return jnp.sum(before * one_hot, axis=2).reshape(route_ids.shape)


def dispatch_rows(normed, flat_pick, slot_count):
    slot_ids = jnp.arange(slot_count, dtype=jnp.int32)
    chosen = jnp.any(flat_pick[None, :, :] == slot_ids[:, None, None], axis=2)
    return jnp.dot(
        chosen.astype(jnp.bfloat16), normed, preferred_element_type=jnp.float32
    ).astype(jnp.bfloat16)


MESH = pl.DeviceIdType.MESH


def mixer_kernel(
    n, tp, halo, pieces, gate_ref, value_ref, out_gate_ref, taps_ref, proj_ref, res_ref, gain_ref,
    rows_ref, normed_ref, edge, product, mixed, part, mrecv, psum, xrecv, send, got,
):
    s = lax.axis_index("sp")
    t = lax.axis_index("tp")
    mate = t + 1 - 2 * (t % 2)
    across = (t + 2) % tp
    mate_across = (mate + 2) % tp
    tokens = gate_ref.shape[0]
    quarter, width = res_ref.shape
    piece = quarter // pieces
    after, before = (s + 1) % n, (s + n - 1) % n

    barrier = pltpu.get_barrier_semaphore()
    for peer in ((s, mate), (s, across), (after, t), (before, t)):
        pl.semaphore_signal(barrier, inc=1, device_id=peer, device_id_type=MESH)

    def remote(src, dst, lane, device):
        return pltpu.make_async_remote_copy(
            src_ref=src,
            dst_ref=dst,
            send_sem=send.at[lane],
            recv_sem=got.at[lane],
            device_id=device,
            device_id_type=MESH,
        )

    tail = pl.ds(tokens - halo, halo)
    edges = [
        remote(ref.at[tail], edge.at[i], i, (after, t))
        for i, ref in enumerate((gate_ref, value_ref))
    ]
    pl.semaphore_wait(barrier, 4)
    for copy in edges:
        copy.start()

    body_rows = pl.ds(halo, tokens)
    product[body_rows] = gate_ref[...].astype(jnp.float32) * value_ref[...].astype(jnp.float32)
    for copy in edges:
        copy.wait_recv()
    prior = edge[0].astype(jnp.float32) * edge[1].astype(jnp.float32)
    product[pl.ds(0, halo)] = jnp.where(s == 0, 0.0, prior)
    conv_sum = (
        taps_ref[0:1] * product[pl.ds(halo - 2, tokens)]
        + taps_ref[1:2] * product[pl.ds(halo - 1, tokens)]
        + taps_ref[2:3] * product[body_rows]
    )
    mixed[...] = (out_gate_ref[...].astype(jnp.float32) * conv_sum).astype(jnp.bfloat16)

    def project(block, p):
        first = pl.multiple_of(block * quarter + p * piece, piece)
        y = jnp.dot(
            mixed[pl.ds(first, piece)], proj_ref[...], preferred_element_type=jnp.float32
        )
        part[block, p] = y.astype(jnp.bfloat16)

    def lane(kind, p):
        return 2 + kind * pieces + p

    def to_mate(kind, block, p):
        return remote(part.at[block, p], mrecv.at[kind, p], lane(kind, p), (s, mate))

    def over(p):
        return remote(psum.at[p], xrecv.at[p], lane(2, p), (s, across))

    def wide(block):
        return block.astype(jnp.float32)

    for p in range(pieces):
        project(mate_across, p)
        to_mate(0, mate_across, p).start()
    for p in range(pieces):
        project(across, p)
        to_mate(0, mate_across, p).wait_recv()
        psum[p] = (wide(part[across, p]) + wide(mrecv[0, p])).astype(jnp.bfloat16)
        over(p).start()
    for p in range(pieces):
        project(mate, p)
        to_mate(1, mate, p).start()
    for p in range(pieces):
        project(t, p)
    for p in range(pieces):
        to_mate(1, mate, p).wait_recv()
        over(p).wait_recv()
        at = pl.ds(p * piece, piece)
        summed = wide(part[t, p]) + wide(mrecv[1, p]) + wide(xrecv[p])
        hidden_rows = wide(res_ref[at]) + summed
        inverse = lax.rsqrt(jnp.mean(hidden_rows * hidden_rows, axis=-1, keepdims=True) + 1e-05)
        rows_ref[at] = hidden_rows
        normed_ref[at] = (hidden_rows * inverse * gain_ref[...]).astype(jnp.bfloat16)
    for copy in edges:
        copy.wait_send()
    for p in range(pieces):
        to_mate(0, mate_across, p).wait_send()
        to_mate(1, mate, p).wait_send()
        over(p).wait_send()


def run_mixer(gate_in, value_in, gate_out, conv_taps, proj_weight, residual, norm_gain):
    n, tp = lax.axis_size("sp"), lax.axis_size("tp")
    tokens, channels = gate_in.shape
    quarter, width = residual.shape
    halo, pieces = 16, 4
    piece = quarter // pieces
    vmem = pl.BlockSpec(memory_space=pltpu.VMEM)
    bf16, f32 = jnp.bfloat16, jnp.float32
    return pl.pallas_call(
        functools.partial(mixer_kernel, n, tp, halo, pieces),
        out_shape=(
            jax.ShapeDtypeStruct((quarter, width), f32),
            jax.ShapeDtypeStruct((quarter, width), bf16),
        ),
        in_specs=[vmem] * 7,
        out_specs=(vmem, vmem),
        scratch_shapes=[
            pltpu.VMEM((2, halo, channels), bf16),
            pltpu.VMEM((halo + tokens, channels), f32),
            pltpu.VMEM((tokens, channels), bf16),
            pltpu.VMEM((tp, pieces, piece, width), bf16),
            pltpu.VMEM((2, pieces, piece, width), bf16),
            pltpu.VMEM((pieces, piece, width), bf16),
            pltpu.VMEM((pieces, piece, width), bf16),
            pltpu.SemaphoreType.DMA((2 + 3 * pieces,)),
            pltpu.SemaphoreType.DMA((2 + 3 * pieces,)),
        ],
        compiler_params=pltpu.CompilerParams(
            collective_id=2, has_side_effects=True, vmem_limit_bytes=60 * 1024 * 1024
        ),
    )(gate_in, value_in, gate_out, conv_taps, proj_weight, residual, norm_gain.reshape(1, width))


def expert_kernel(
    n, tp, halves, out_ref, gate_hbm, up_hbm, down_hbm, ret_ref,
    recv, part, mrecv, psum, xrecv, fin, gate_w, up_w, down_w, hid, local_sem, send, got,
):
    s = lax.axis_index("sp")
    t = lax.axis_index("tp")
    mate = t + 1 - 2 * (t % 2)
    across = (t + 2) % tp
    mate_across = (mate + 2) % tp
    cap, width = out_ref.shape[1], out_ref.shape[2]
    units = gate_w.shape[1]
    rows = tp * cap
    steps = n * halves

    weight_copies = [
        pltpu.make_async_copy(src, dst, local_sem.at[i])
        for i, (src, dst) in enumerate(
            [(gate_hbm, gate_w), (up_hbm, up_w), (down_hbm, down_w)]
        )
    ]
    for copy in weight_copies:
        copy.start()

    barrier = pltpu.get_barrier_semaphore()

    @pl.loop(1, n)
    def _(k):
        pl.semaphore_signal(barrier, inc=1, device_id=((s + k) % n, t), device_id_type=MESH)

    for peer in (mate, across):
        pl.semaphore_signal(barrier, inc=1, device_id=(s, peer), device_id_type=MESH)
    pl.semaphore_wait(barrier, n + 1)

    def remote(src, dst, lane, k, device):
        return pltpu.make_async_remote_copy(
            src_ref=src,
            dst_ref=dst,
            send_sem=send.at[lane, k],
            recv_sem=got.at[lane, k],
            device_id=device,
            device_id_type=MESH,
        )

    def outward(k):
        to = (s + k // halves) % n
        return remote(out_ref.at[to * halves + k % halves], recv.at[k, t], 0, k, (to, t))

    def over(k, block):
        return remote(recv.at[k, block], recv.at[k, block], 1, k, (s, across))

    def pair_own(k, block):
        return remote(recv.at[k, block], recv.at[k, block], 2, k, (s, mate))

    def pair_far(k, block):
        return remote(recv.at[k, block], recv.at[k, block], 3, k, (s, mate))

    def part_near(k):
        return remote(part.at[k, mate], mrecv.at[k, 0], 4, k, (s, mate))

    def part_far(k):
        return remote(part.at[k, mate_across], mrecv.at[k, 1], 5, k, (s, mate))

    def sum_over(k):
        return remote(psum.at[k], xrecv.at[k], 6, k, (s, across))

    def homeward(k):
        to = (s + n - k // halves) % n
        return remote(fin.at[k], ret_ref.at[s * halves + k % halves], 7, k, (to, t))

    own = [
        pltpu.make_async_copy(out_ref.at[s * halves + h], recv.at[h, t], local_sem.at[3 + h])
        for h in range(halves)
    ]
    for copy in own:
        copy.start()

    @pl.loop(halves, steps)
    def _(k):
        outward(k).start()

    for copy in own:
        copy.wait()

    def ffn(k):
        def load():
            block = recv[k]
            if cap % 16:
                return block.astype(jnp.float32).reshape(rows, width).astype(jnp.bfloat16)
            return block.reshape(rows, width)

        cols = min(256, units)

        @pl.loop(0, units // cols)
        def _(c):
            at = pl.ds(pl.multiple_of(c * cols, cols), cols)
            x = load()
            gate = jnp.dot(x, gate_w[:, at], preferred_element_type=jnp.float32)
            up = jnp.dot(x, up_w[:, at], preferred_element_type=jnp.float32)
            hid[:, at] = (gate / (1.0 + jnp.exp(-gate)) * up).astype(jnp.bfloat16)

        wide = min(512, width)

        @pl.loop(0, width // wide)
        def _(c):
            at = pl.ds(pl.multiple_of(c * wide, wide), wide)
            y = jnp.dot(hid[...], down_w[:, at], preferred_element_type=jnp.float32)
            part[k, :, :, at] = y.reshape(tp, cap, wide).astype(jnp.bfloat16)

    def wide_sum(*blocks):
        total = blocks[0].astype(jnp.float32)
        for block in blocks[1:]:
            total = total + block.astype(jnp.float32)
        return total

    @pl.loop(0, steps + 4)
    def _(i):
        @pl.when(i < steps)
        def _():
            @pl.when(i >= halves)
            def _():
                outward(i).wait_recv()

            over(i, t).start()
            pair_own(i, t).start()

        @pl.when((i >= 1) & (i < steps + 1))
        def _():
            k = i - 1
            over(k, across).wait_recv()
            pair_far(k, across).start()

        @pl.when((i >= 3) & (i < steps + 3))
        def _():
            k = i - 3
            part_far(k).wait_recv()
            psum[k] = wide_sum(part[k, across], mrecv[k, 1]).astype(jnp.bfloat16)
            sum_over(k).start()

        @pl.when(i >= 4)
        def _():
            k = i - 4
            part_near(k).wait_recv()
            sum_over(k).wait_recv()
            total = wide_sum(part[k, t], mrecv[k, 0], xrecv[k]).astype(jnp.bfloat16)

            @pl.when(k < halves)
            def _():
                ret_ref[s * halves + k] = total

            @pl.when(k >= halves)
            def _():
                fin[k] = total
                homeward(k).start()

        @pl.when(i == 2)
        def _():
            for copy in weight_copies:
                copy.wait()

        @pl.when((i >= 2) & (i < steps + 2))
        def _():
            k = i - 2
            pair_own(k, mate).wait_recv()
            pair_far(k, mate_across).wait_recv()
            ffn(k)
            part_far(k).start()
            part_near(k).start()

    @pl.loop(0, steps)
    def _(k):
        over(k, t).wait_send()
        pair_own(k, t).wait_send()
        pair_far(k, across).wait_send()
        part_near(k).wait_send()
        part_far(k).wait_send()
        sum_over(k).wait_send()

        @pl.when(k >= halves)
        def _():
            outward(k).wait_send()
            homeward(k).wait_send()
            homeward(k).wait_recv()


def run_experts(outgoing, gate_weight, up_weight, down_weight):
    n, cap, width = outgoing.shape
    tp = lax.axis_size("tp")
    units = gate_weight.shape[1]
    halves = 2 if cap % 32 == 0 else 1
    steps, cap = n * halves, cap // halves
    vmem = pl.BlockSpec(memory_space=pltpu.VMEM)
    hbm = pl.BlockSpec(memory_space=pl.ANY)
    bf16 = jnp.bfloat16
    return pl.pallas_call(
        functools.partial(expert_kernel, n, tp, halves),
        out_shape=jax.ShapeDtypeStruct((steps, cap, width), bf16),
        in_specs=[vmem, hbm, hbm, hbm],
        out_specs=vmem,
        scratch_shapes=[
            pltpu.VMEM((steps, tp, cap, width), bf16),
            pltpu.VMEM((steps, tp, cap, width), bf16),
            pltpu.VMEM((steps, 2, cap, width), bf16),
            pltpu.VMEM((steps, cap, width), bf16),
            pltpu.VMEM((steps, cap, width), bf16),
            pltpu.VMEM((steps, cap, width), bf16),
            pltpu.VMEM(gate_weight.shape, bf16),
            pltpu.VMEM(up_weight.shape, bf16),
            pltpu.VMEM(down_weight.shape, bf16),
            pltpu.VMEM((tp * cap, units), bf16),
            pltpu.SemaphoreType.DMA((3 + halves,)),
            pltpu.SemaphoreType.DMA((8, steps)),
            pltpu.SemaphoreType.DMA((8, steps)),
        ],
        compiler_params=pltpu.CompilerParams(
            collective_id=1, has_side_effects=True, vmem_limit_bytes=60 * 1024 * 1024
        ),
    )(outgoing.reshape(steps, cap, width), gate_weight, up_weight, down_weight)


def exchange_body(
    gate_in,
    value_in,
    gate_out,
    conv_taps,
    proj_weight,
    residual,
    norm_gain,
    routes,
    route_weight,
    expert_gate,
    expert_up,
    expert_down,
):
    model_width = residual.shape[1]
    tp_count = lax.axis_size("tp")
    groups = lax.axis_size("sp")
    quarter = residual.shape[0]
    top_count = routes.shape[1]
    capacity = 2 * quarter * top_count // groups
    tp_index = lax.axis_index("tp")
    first_own = tp_index * quarter
    own_routes = lax.dynamic_slice_in_dim(routes, first_own, quarter, 0)
    own_weights = lax.dynamic_slice_in_dim(route_weight, first_own, quarter, 0)
    my_rows, normed = run_mixer(
        gate_in, value_in, gate_out, conv_taps, proj_weight, residual, norm_gain
    )
    own_slots = slot_numbers(own_routes, quarter, groups)
    flat_pick = own_routes * capacity + own_slots
    slot_count = groups * capacity
    outgoing = dispatch_rows(normed, flat_pick, slot_count)
    returned = run_experts(
        outgoing.reshape(groups, capacity, model_width),
        expert_gate[0],
        expert_up[0],
        expert_down[0],
    ).reshape(slot_count, model_width)
    total = my_rows
    for k in range(top_count):
        pick = flat_pick[:, k, None] == jnp.arange(slot_count, dtype=jnp.int32)
        picked = jnp.dot(
            pick.astype(jnp.bfloat16), returned, preferred_element_type=jnp.float32
        )
        total = total + own_weights[:, k, None] * picked
    return total.astype(jnp.bfloat16)


def plane_of(j, z, planes):
    return jnp.where(z < planes // 2, z + j, z + planes - j) % planes


def layer_kernel(
    n, tp, halo, pieces, cap,
    routes_ref, weights_ref, taps_ref, gain_ref,
    gate_hbm, value_hbm, out_gate_hbm, proj_hbm, res_hbm, wg_hbm, wu_hbm, wd_hbm,
    out_ref,
    gate_ref, value_ref, out_gate_ref, proj_ref, res_ref, gate_w, up_w, down_w,
    edge, product, mixed, mpart, mmate, msum, mfar,
    rows, info, spread, raw, ysend, recv, part, mrecv, psum, xrecv, fin, ret, hid,
    local_sem, msend, mgot, isend, igot, rsend, rgot, ysem, ygot, dsend, dgot, psend, pgot, hsend, hgot,
):
    s = lax.axis_index("sp")
    t = lax.axis_index("tp")
    planes = n // 2
    z, y = s // 2, s % 2
    other_y = 1 - y
    mate = t + 1 - 2 * (t % 2)
    across = (t + 2) % tp
    mate_across = (mate + 2) % tp
    tokens = gate_ref.shape[0]
    quarter, width = res_ref.shape
    half = cap // 2
    units = 2 * planes
    after, before = (s + 1) % n, (s + n - 1) % n
    f32, bf16 = jnp.float32, jnp.bfloat16

    loads = [
        pltpu.make_async_copy(src, dst, local_sem.at[i])
        for i, (src, dst) in enumerate(
            [
                (gate_hbm, gate_ref), (value_hbm, value_ref), (out_gate_hbm, out_gate_ref),
                (proj_hbm, proj_ref), (res_hbm, res_ref),
                (wg_hbm, gate_w), (wu_hbm, up_w), (wd_hbm, down_w),
            ]
        )
    ]
    for copy in loads[:5]:
        copy.start()

    barrier = pltpu.get_barrier_semaphore()

    @pl.loop(1, n)
    def _(k):
        pl.semaphore_signal(barrier, inc=1, device_id=((s + k) % n, t), device_id_type=MESH)

    for peer in (mate, across):
        pl.semaphore_signal(barrier, inc=1, device_id=(s, peer), device_id_type=MESH)

    def remote(src, dst, send_sem, recv_sem, device):
        return pltpu.make_async_remote_copy(
            src_ref=src, dst_ref=dst, send_sem=send_sem, recv_sem=recv_sem,
            device_id=device, device_id_type=MESH,
        )

    own_at = pl.ds(pl.multiple_of(t * quarter, quarter), quarter)
    named = [routes_ref[k:k + 1, own_at] for k in range(2)]
    expert_ids = lax.broadcasted_iota(jnp.int32, (n, quarter), 0)
    one_hot = [(expert_ids == name).astype(f32) for name in named]
    earlier = (
        lax.broadcasted_iota(jnp.int32, (quarter, quarter), 0)
        < lax.broadcasted_iota(jnp.int32, (quarter, quarter), 1)
    ).astype(bf16)
    count = jnp.dot(
        (one_hot[0] + one_hot[1]).astype(bf16), earlier, preferred_element_type=f32
    )
    picks = [
        name.astype(f32) * cap + jnp.sum(count * hot, axis=0, keepdims=True)
        for name, hot in zip(named, one_hot)
    ]
    for copy in loads[:2]:
        copy.wait()
    tail = pl.ds(tokens - halo, halo)
    edges = [
        remote(ref.at[tail], edge.at[i], msend.at[i], mgot.at[i], (after, t))
        for i, ref in enumerate((gate_ref, value_ref))
    ]
    pl.semaphore_wait(barrier, n + 1)
    for copy in edges:
        copy.start()

    def tell(k):
        to = (z + k) % planes
        return remote(info.at[z], info.at[z], isend.at[k], igot.at[z], (to * 2 + y, t))

    def told(k):
        origin = (z + k) % planes
        return remote(info.at[origin], info.at[origin], isend.at[k], igot.at[origin], (s, mate))

    for copy in loads[5:]:
        copy.start()

    product[pl.ds(halo, tokens)] = gate_ref[...].astype(f32) * value_ref[...].astype(f32)
    loads[2].wait()
    part_width = width // pieces

    def mix(block):
        @pl.when(block == 0)
        def _():
            for copy in edges:
                copy.wait_recv()
            prior = edge[0].astype(f32) * edge[1].astype(f32)
            product[pl.ds(0, halo)] = jnp.where(s == 0, 0.0, prior)

        at = pl.ds(pl.multiple_of(block * quarter, quarter), quarter)
        window = product[pl.ds(pl.multiple_of(block * quarter, quarter), halo + quarter)]
        conv_sum = (
            taps_ref[0:1] * window[halo - 2:halo - 2 + quarter]
            + taps_ref[1:2] * window[halo - 1:halo - 1 + quarter]
            + taps_ref[2:3] * window[halo:]
        )
        mixed[at] = (out_gate_ref[at].astype(f32) * conv_sum).astype(bf16)

    def columns(p):
        return pl.ds(p * part_width, part_width)

    def project(block, p):
        at = pl.ds(pl.multiple_of(block * quarter, quarter), quarter)
        y_block = jnp.dot(mixed[at], proj_ref[:, columns(p)], preferred_element_type=f32)
        mpart[block, p] = y_block.astype(bf16)

    def lane(kind, p):
        return 2 + kind * pieces + p

    def to_mate(kind, block, p):
        at = lane(kind, p)
        return remote(mpart.at[block, p], mmate.at[kind, p], msend.at[at], mgot.at[at], (s, mate))

    def to_across(p):
        at = lane(2, p)
        return remote(msum.at[p], mfar.at[p], msend.at[at], mgot.at[at], (s, across))

    mix(mate_across)
    loads[3].wait()
    for p in range(min(2, pieces)):
        project(mate_across, p)
        to_mate(0, mate_across, p).start()
    mix(across)
    for p in range(pieces):
        project(across, p)
        to_mate(0, mate_across, p).wait_recv()
        msum[p] = (mpart[across, p].astype(f32) + mmate[0, p].astype(f32)).astype(bf16)
        to_across(p).start()
        if p + 2 < pieces:
            project(mate_across, p + 2)
            to_mate(0, mate_across, p + 2).start()
    mix(mate)
    for p in range(pieces):
        project(mate, p)
        to_mate(1, mate, p).start()
    mix(t)
    for p in range(pieces):
        project(t, p)

    slot_ids = lax.broadcasted_iota(jnp.int32, (n * cap, quarter), 0).astype(f32)
    share = jnp.where(slot_ids == picks[0], weights_ref[0:1, own_at], 0.0) + jnp.where(
        slot_ids == picks[1], weights_ref[1:2, own_at], 0.0
    )
    share = jnp.transpose(share)
    high = share.astype(bf16)
    spread[0] = high
    spread[1] = (share - high.astype(f32)).astype(bf16)

    def along(block, up, at=slice(None)):
        to = jnp.where(up == 1, z + 1, z - 1)
        ref = raw.at[block, :, at]
        return remote(ref, ref, rsend.at[up, block], rgot.at[block], (to * 2 + y, t))

    def has_up(block):
        return (block <= z) & (z < planes - 1)

    def has_down(block):
        return (block >= z) & (z > 0)

    def pass_on(block):
        @pl.when(has_up(block))
        def _():
            along(block, 1).start()

        @pl.when(has_down(block))
        def _():
            along(block, 0).start()

    loads[4].wait()
    square = jnp.zeros((quarter, 1), f32)
    for p in range(pieces):
        at = columns(p)
        to_mate(1, mate, p).wait_recv()
        to_across(p).wait_recv()
        summed = mpart[t, p].astype(f32) + mmate[1, p].astype(f32) + mfar[p].astype(f32)
        hidden_rows = res_ref[:, at].astype(f32) + summed
        rows[:, at] = hidden_rows
        raw[z, :, at] = (hidden_rows * gain_ref[:, at]).astype(bf16)
        for up, has in ((1, has_up), (0, has_down)):
            @pl.when(has(z))
            def _():
                along(z, up, at).start()

        square = square + jnp.sum(hidden_rows * hidden_rows, axis=-1, keepdims=True)
    inverse = lax.rsqrt(square / width + 1e-05)
    scale = jnp.transpose(jnp.broadcast_to(inverse, (quarter, quarter)))[0:1]
    info[z] = jnp.concatenate(picks + [scale, jnp.zeros((5, quarter), f32)], axis=0)

    @pl.loop(1, planes)
    def _(k):
        tell(k).start()

    def beside(j, h):
        return remote(
            ysend.at[j, h], recv.at[j, h, t, y], ysem.at[j, h], ygot.at[j, h], (z * 2 + other_y, t)
        )

    def over(j, h, source):
        ref = recv.at[j, h, t, source]
        return remote(ref, ref, dsend.at[0, j, h, source], dgot.at[0, j, h, source], (s, across))

    def pair_own(j, h, source):
        ref = recv.at[j, h, t, source]
        return remote(ref, ref, dsend.at[1, j, h, source], dgot.at[1, j, h, source], (s, mate))

    def pair_far(j, h, source):
        ref = recv.at[j, h, across, source]
        return remote(ref, ref, dsend.at[2, j, h, source], dgot.at[2, j, h, source], (s, mate))

    wide = min(512, width)

    def select(j, block, expert, put):
        place = lax.broadcasted_iota(jnp.int32, (cap, quarter), 0).astype(f32) + (
            expert * cap
        ).astype(f32)
        table = info[block]
        named = (place == table[0:1]) | (place == table[1:2])
        chosen = named.astype(f32).astype(bf16)
        scale = jnp.sum(jnp.where(named, table[2:3], 0.0), axis=1, keepdims=True)

        @pl.loop(0, width // wide)
        def _(c):
            at = pl.ds(pl.multiple_of(c * wide, wide), wide)
            taken = jnp.dot(chosen, raw[block, :, at], preferred_element_type=f32)
            taken = (taken * scale).astype(bf16)
            for h in range(2):
                put(h, at, taken[h * half:(h + 1) * half])

    def arrive(j):
        block = plane_of(j, z, planes)
        along(block, 1).wait_recv()
        pass_on(block)

    def dispatch(j):
        block = plane_of(j, z, planes)

        @pl.when(j > 0)
        def _():
            told((block + planes - z) % planes).wait_recv()

        def put_own(h, at, value):
            recv[j, h, t, y, :, at] = value

        def put_other(h, at, value):
            ysend[j, h, :, at] = value

        select(j, block, s, put_own)
        for h in (1, 0):
            over(j, h, y).start()
        select(j, block, z * 2 + other_y, put_other)
        for h in (1, 0):
            beside(j, h).start()
        for h in (1, 0):
            pair_own(j, h, y).start()

    def dispatch_beside(j):
        for h in (1, 0):
            beside(j, h).wait_recv()
            over(j, h, other_y).start()
            pair_own(j, h, other_y).start()

    def dispatch_far(j, source):
        for h in (1, 0):
            over(j, h, source).wait_recv()
            pair_far(j, h, source).start()

    def part_near(u):
        return remote(part.at[u, mate], mrecv.at[u, 0], psend.at[0, u], pgot.at[0, u], (s, mate))

    def part_far(u):
        return remote(part.at[u, mate_across], mrecv.at[u, 1], psend.at[1, u], pgot.at[1, u], (s, mate))

    def sum_over(u):
        return remote(psum.at[u], xrecv.at[u], psend.at[2, u], pgot.at[2, u], (s, across))

    def ffn(j, h):
        u = 2 * j + h
        for source in range(2):
            pair_own(j, h, source).wait_recv()
            pair_far(j, h, source).wait_recv()
        count = gate_w.shape[1]
        cols = min(256, count)

        @pl.loop(0, count // cols)
        def _(c):
            at = pl.ds(pl.multiple_of(c * cols, cols), cols)
            x = recv[j, h].reshape(tp * cap, width)
            gate = jnp.dot(x, gate_w[:, at], preferred_element_type=f32)
            up = jnp.dot(x, up_w[:, at], preferred_element_type=f32)
            hid[:, at] = (gate / (1.0 + jnp.exp(-gate)) * up).astype(bf16)

        @pl.loop(0, width // wide)
        def _(c):
            at = pl.ds(pl.multiple_of(c * wide, wide), wide)
            out = jnp.dot(hid[...], down_w[:, at], preferred_element_type=f32)
            part[u, :, :, :, at] = out.reshape(tp, 2, half, wide).astype(bf16)

        part_far(u).start()
        part_near(u).start()

    def homeward(j, h, source):
        u = 2 * j + h
        to = plane_of(j, z, planes) * 2 + source
        return remote(fin.at[u, source], ret.at[s, h], hsend.at[u, source], hgot.at[s, h], (to, t))

    def returned(origin, h):
        return remote(ret.at[origin, h], ret.at[origin, h], hsend.at[0, 0], hgot.at[origin, h], (s, mate))

    def sum_far(j, h):
        u = 2 * j + h
        part_far(u).wait_recv()
        psum[u] = (part[u, across].astype(f32) + mrecv[u, 1].astype(f32)).astype(bf16)
        sum_over(u).start()

    def send_home(j, h):
        u = 2 * j + h
        part_near(u).wait_recv()
        sum_over(u).wait_recv()
        total = (
            part[u, t].astype(f32) + mrecv[u, 0].astype(f32) + xrecv[u].astype(f32)
        ).astype(bf16)
        fin[u] = total

        @pl.when(j == 0)
        def _():
            ret[s, h] = fin[u, y]
            homeward(j, h, other_y).start()

        @pl.when(j > 0)
        def _():
            for source in range(2):
                homeward(j, h, source).start()

    def gather(plane, put):
        for source in range(2):
            for h in range(2):
                origin = plane * 2 + source

                @pl.when(origin != s)
                def _():
                    returned(origin, h).wait_recv()

        slots = pl.ds(pl.multiple_of(plane * 2 * cap, 2 * cap), 2 * cap)

        @pl.loop(0, width // wide)
        def _(c):
            at = pl.ds(pl.multiple_of(c * wide, wide), wide)
            got = ret[pl.ds(plane * 2, 2), :, :, at].reshape(2 * cap, wide)
            put(
                at,
                rows[:, at]
                + jnp.dot(spread[0, :, slots], got, preferred_element_type=f32)
                + jnp.dot(spread[1, :, slots], got, preferred_element_type=f32),
            )

    def keep(at, value):
        rows[:, at] = value

    def finish(at, value):
        out_ref[:, at] = value.astype(bf16)

    at_end = (z == 0) | (z == planes - 1)
    late = jnp.where(at_end, 1, 0)

    dispatch(0)
    arrive(1)

    @pl.when(late == 0)
    def _():
        arrive(planes - 1)

    dispatch_beside(0)
    for copy in loads[5:]:
        copy.wait()

    @pl.loop(0, planes)
    def _(j):
        @pl.when((j > 0) & (late == 1) & (j + 1 < planes))
        def _():
            arrive(j + 1)

        @pl.when(j + 1 < planes)
        def _():
            dispatch(j + 1)

        dispatch_far(j, y)

        @pl.when(j > 1 + late)
        def _():
            send_home(j - 1, 0)

        dispatch_far(j, other_y)
        ffn(j, 0)

        @pl.when(j > late)
        def _():
            sum_far(j, 0)

        @pl.when(j == 0)
        def _():
            dispatch_beside(1)

        @pl.when((j == 0) & (late == 0))
        def _():
            arrive(2)

        ffn(j, 1)

        @pl.when(j > 1 + late)
        def _():
            send_home(j - 1, 1)

        @pl.when((j > 0) & (j + 1 < planes))
        def _():
            dispatch_beside(j + 1)

        @pl.when(j > late)
        def _():
            sum_far(j, 1)

    @pl.when(late == 1)
    def _():
        sum_far(1, 0)
        sum_far(1, 1)

    sum_far(0, 0)
    sum_far(0, 1)
    send_home(planes - 1, 0)
    send_home(planes - 1, 1)

    @pl.when(late == 1)
    def _():
        send_home(1, 0)
        send_home(1, 1)

    @pl.loop(1, planes - 1)
    def _(j):
        gather(plane_of(j + late, z, planes), keep)

    send_home(0, 0)
    send_home(0, 1)
    gather(plane_of(jnp.where(late == 1, 1, planes - 1), z, planes), keep)
    gather(z, finish)

    for copy in edges:
        copy.wait_send()
    for p in range(pieces):
        to_mate(0, mate_across, p).wait_send()
        to_mate(1, mate, p).wait_send()
        to_across(p).wait_send()

    @pl.loop(0, planes)
    def _(j):
        @pl.when(j > 0)
        def _():
            tell(j).wait_send()

        @pl.when(has_up(j))
        def _():
            along(j, 1).wait_send()

        @pl.when(has_down(j))
        def _():
            along(j, 0).wait_send()

        for h in range(2):
            beside(j, h).wait_send()
            for source in range(2):
                over(j, h, source).wait_send()
                pair_own(j, h, source).wait_send()
                pair_far(j, h, source).wait_send()

    @pl.loop(0, units)
    def _(u):
        part_near(u).wait_send()
        part_far(u).wait_send()
        sum_over(u).wait_send()
        homeward(u // 2, u % 2, other_y).wait_send()

        @pl.when(u > 1)
        def _():
            homeward(u // 2, u % 2, y).wait_send()


def relay_body(
    gate_in, value_in, gate_out, conv_taps, proj_weight, residual, norm_gain,
    routes, route_weight, expert_gate, expert_up, expert_down,
):
    n, tp = lax.axis_size("sp"), lax.axis_size("tp")
    tokens, channels = gate_in.shape
    quarter, width = residual.shape
    cap = 2 * quarter * routes.shape[1] // n
    units_hidden = expert_gate.shape[2]
    planes, half = n // 2, cap // 2
    units = 2 * planes
    halo, pieces = 16, 4
    part_width = width // pieces
    vmem = pl.BlockSpec(memory_space=pltpu.VMEM)
    hbm = pl.BlockSpec(memory_space=pl.ANY)
    bf16, f32 = jnp.bfloat16, jnp.float32
    dma = pltpu.SemaphoreType.DMA
    rows = (2, half, width)
    return pl.pallas_call(
        functools.partial(layer_kernel, n, tp, halo, pieces, cap),
        out_shape=jax.ShapeDtypeStruct((quarter, width), bf16),
        in_specs=[vmem] * 4 + [hbm] * 8,
        out_specs=vmem,
        scratch_shapes=[
            pltpu.VMEM((tokens, channels), bf16),
            pltpu.VMEM((tokens, channels), bf16),
            pltpu.VMEM((tokens, channels), bf16),
            pltpu.VMEM(proj_weight.shape, bf16),
            pltpu.VMEM((quarter, width), bf16),
            pltpu.VMEM((width, units_hidden), bf16),
            pltpu.VMEM((width, units_hidden), bf16),
            pltpu.VMEM((units_hidden, width), bf16),
            pltpu.VMEM((2, halo, channels), bf16),
            pltpu.VMEM((halo + tokens, channels), f32),
            pltpu.VMEM((tokens, channels), bf16),
            pltpu.VMEM((tp, pieces, quarter, part_width), bf16),
            pltpu.VMEM((2, pieces, quarter, part_width), bf16),
            pltpu.VMEM((pieces, quarter, part_width), bf16),
            pltpu.VMEM((pieces, quarter, part_width), bf16),
            pltpu.VMEM((quarter, width), f32),
            pltpu.VMEM((planes, 8, quarter), f32),
            pltpu.VMEM((2, quarter, n * cap), bf16),
            pltpu.VMEM((planes, quarter, width), bf16),
            pltpu.VMEM((planes,) + rows, bf16),
            pltpu.VMEM((planes, 2, tp) + rows, bf16),
            pltpu.VMEM((units, tp) + rows, bf16),
            pltpu.VMEM((units, 2) + rows, bf16),
            pltpu.VMEM((units,) + rows, bf16),
            pltpu.VMEM((units,) + rows, bf16),
            pltpu.VMEM((units,) + rows, bf16),
            pltpu.VMEM((n,) + rows, bf16),
            pltpu.VMEM((tp * cap, units_hidden), bf16),
            dma((8,)),
            dma((2 + 3 * pieces,)),
            dma((2 + 3 * pieces,)),
            dma((planes,)),
            dma((planes,)),
            dma((2, planes)),
            dma((planes,)),
            dma((planes, 2)),
            dma((planes, 2)),
            dma((3, planes, 2, 2)),
            dma((3, planes, 2, 2)),
            dma((3, units)),
            dma((3, units)),
            dma((units, 2)),
            dma((n, 2)),
        ],
        compiler_params=pltpu.CompilerParams(
            collective_id=3, has_side_effects=True, vmem_limit_bytes=60 * 1024 * 1024
        ),
    )(
        routes.T, route_weight.T, conv_taps, norm_gain.reshape(1, width),
        gate_in, value_in, gate_out, proj_weight, residual,
        expert_gate[0], expert_up[0], expert_down[0],
    )


def body(*args):
    residual, routes = args[5], args[7]
    n, tp = lax.axis_size("sp"), lax.axis_size("tp")
    quarter = residual.shape[0]
    capacity = 2 * quarter * routes.shape[1] // n
    relay = n == 2 * tp and tp == 4 and capacity % 32 == 0 and quarter % 128 == 0
    if relay and (n // 2) * quarter <= n * capacity:
        return relay_body(*args)
    return exchange_body(*args)


def solution(mesh):
    placed = (
        P("sp", "tp"),
        P("sp", "tp"),
        P("sp", "tp"),
        P(None, "tp"),
        P("tp", None),
        P(("sp", "tp"), None),
        P(),
        P("sp", None),
        P("sp", None),
        P("sp", None, "tp"),
        P("sp", None, "tp"),
        P("sp", "tp", None),
    )
    return jax.shard_map(
        body, mesh=mesh, in_specs=placed, out_specs=P(("sp", "tp"), None), check_vma=False
    )
```

```python
import functools

import jax
import jax.numpy as jnp
from jax import lax
from jax.experimental import pallas as pl
from jax.experimental.pallas import tpu as pltpu
from jax.sharding import PartitionSpec as P


def slot_numbers(route_ids, block_rows, expert_count):
    block_count = route_ids.shape[0] // block_rows
    flat_ids = route_ids.reshape(block_count, block_rows * route_ids.shape[1])
    one_hot = (
        flat_ids[:, :, None] == jnp.arange(expert_count, dtype=jnp.int32)[None, None, :]
    ).astype(jnp.int32)
    before = jnp.cumsum(one_hot, axis=1) - one_hot
    return jnp.sum(before * one_hot, axis=2).reshape(route_ids.shape)


def dispatch_rows(normed, flat_pick, slot_count):
    slot_ids = jnp.arange(slot_count, dtype=jnp.int32)
    chosen = jnp.any(flat_pick[None, :, :] == slot_ids[:, None, None], axis=2)
    return jnp.dot(
        chosen.astype(jnp.bfloat16), normed, preferred_element_type=jnp.float32
    ).astype(jnp.bfloat16)


MESH = pl.DeviceIdType.MESH


def mixer_kernel(
    n, tp, halo, pieces, gate_ref, value_ref, out_gate_ref, taps_ref, proj_ref, res_ref, gain_ref,
    rows_ref, normed_ref, edge, product, mixed, part, mrecv, psum, xrecv, send, got,
):
    s = lax.axis_index("sp")
    t = lax.axis_index("tp")
    mate = t + 1 - 2 * (t % 2)
    across = (t + 2) % tp
    mate_across = (mate + 2) % tp
    tokens = gate_ref.shape[0]
    quarter, width = res_ref.shape
    piece = quarter // pieces
    after, before = (s + 1) % n, (s + n - 1) % n

    barrier = pltpu.get_barrier_semaphore()
    for peer in ((s, mate), (s, across), (after, t), (before, t)):
        pl.semaphore_signal(barrier, inc=1, device_id=peer, device_id_type=MESH)

    def remote(src, dst, lane, device):
        return pltpu.make_async_remote_copy(
            src_ref=src,
            dst_ref=dst,
            send_sem=send.at[lane],
            recv_sem=got.at[lane],
            device_id=device,
            device_id_type=MESH,
        )

    tail = pl.ds(tokens - halo, halo)
    edges = [
        remote(ref.at[tail], edge.at[i], i, (after, t))
        for i, ref in enumerate((gate_ref, value_ref))
    ]
    pl.semaphore_wait(barrier, 4)
    for copy in edges:
        copy.start()

    body_rows = pl.ds(halo, tokens)
    product[body_rows] = gate_ref[...].astype(jnp.float32) * value_ref[...].astype(jnp.float32)
    for copy in edges:
        copy.wait_recv()
    prior = edge[0].astype(jnp.float32) * edge[1].astype(jnp.float32)
    product[pl.ds(0, halo)] = jnp.where(s == 0, 0.0, prior)
    conv_sum = (
        taps_ref[0:1] * product[pl.ds(halo - 2, tokens)]
        + taps_ref[1:2] * product[pl.ds(halo - 1, tokens)]
        + taps_ref[2:3] * product[body_rows]
    )
    mixed[...] = (out_gate_ref[...].astype(jnp.float32) * conv_sum).astype(jnp.bfloat16)

    def project(block, p):
        first = pl.multiple_of(block * quarter + p * piece, piece)
        y = jnp.dot(
            mixed[pl.ds(first, piece)], proj_ref[...], preferred_element_type=jnp.float32
        )
        part[block, p] = y.astype(jnp.bfloat16)

    def lane(kind, p):
        return 2 + kind * pieces + p

    def to_mate(kind, block, p):
        return remote(part.at[block, p], mrecv.at[kind, p], lane(kind, p), (s, mate))

    def over(p):
        return remote(psum.at[p], xrecv.at[p], lane(2, p), (s, across))

    def wide(block):
        return block.astype(jnp.float32)

    for p in range(pieces):
        project(mate_across, p)
        to_mate(0, mate_across, p).start()
    for p in range(pieces):
        project(across, p)
        to_mate(0, mate_across, p).wait_recv()
        psum[p] = (wide(part[across, p]) + wide(mrecv[0, p])).astype(jnp.bfloat16)
        over(p).start()
    for p in range(pieces):
        project(mate, p)
        to_mate(1, mate, p).start()
    for p in range(pieces):
        project(t, p)
    for p in range(pieces):
        to_mate(1, mate, p).wait_recv()
        over(p).wait_recv()
        at = pl.ds(p * piece, piece)
        summed = wide(part[t, p]) + wide(mrecv[1, p]) + wide(xrecv[p])
        hidden_rows = wide(res_ref[at]) + summed
        inverse = lax.rsqrt(jnp.mean(hidden_rows * hidden_rows, axis=-1, keepdims=True) + 1e-05)
        rows_ref[at] = hidden_rows
        normed_ref[at] = (hidden_rows * inverse * gain_ref[...]).astype(jnp.bfloat16)
    for copy in edges:
        copy.wait_send()
    for p in range(pieces):
        to_mate(0, mate_across, p).wait_send()
        to_mate(1, mate, p).wait_send()
        over(p).wait_send()


def run_mixer(gate_in, value_in, gate_out, conv_taps, proj_weight, residual, norm_gain):
    n, tp = lax.axis_size("sp"), lax.axis_size("tp")
    tokens, channels = gate_in.shape
    quarter, width = residual.shape
    halo, pieces = 16, 4
    piece = quarter // pieces
    vmem = pl.BlockSpec(memory_space=pltpu.VMEM)
    bf16, f32 = jnp.bfloat16, jnp.float32
    return pl.pallas_call(
        functools.partial(mixer_kernel, n, tp, halo, pieces),
        out_shape=(
            jax.ShapeDtypeStruct((quarter, width), f32),
            jax.ShapeDtypeStruct((quarter, width), bf16),
        ),
        in_specs=[vmem] * 7,
        out_specs=(vmem, vmem),
        scratch_shapes=[
            pltpu.VMEM((2, halo, channels), bf16),
            pltpu.VMEM((halo + tokens, channels), f32),
            pltpu.VMEM((tokens, channels), bf16),
            pltpu.VMEM((tp, pieces, piece, width), bf16),
            pltpu.VMEM((2, pieces, piece, width), bf16),
            pltpu.VMEM((pieces, piece, width), bf16),
            pltpu.VMEM((pieces, piece, width), bf16),
            pltpu.SemaphoreType.DMA((2 + 3 * pieces,)),
            pltpu.SemaphoreType.DMA((2 + 3 * pieces,)),
        ],
        compiler_params=pltpu.CompilerParams(
            collective_id=2, has_side_effects=True, vmem_limit_bytes=60 * 1024 * 1024
        ),
    )(gate_in, value_in, gate_out, conv_taps, proj_weight, residual, norm_gain.reshape(1, width))


def expert_kernel(
    n, tp, halves, out_ref, gate_hbm, up_hbm, down_hbm, ret_ref,
    recv, part, mrecv, psum, xrecv, fin, gate_w, up_w, down_w, hid, local_sem, send, got,
):
    s = lax.axis_index("sp")
    t = lax.axis_index("tp")
    mate = t + 1 - 2 * (t % 2)
    across = (t + 2) % tp
    mate_across = (mate + 2) % tp
    cap, width = out_ref.shape[1], out_ref.shape[2]
    units = gate_w.shape[1]
    rows = tp * cap
    steps = n * halves

    weight_copies = [
        pltpu.make_async_copy(src, dst, local_sem.at[i])
        for i, (src, dst) in enumerate(
            [(gate_hbm, gate_w), (up_hbm, up_w), (down_hbm, down_w)]
        )
    ]
    for copy in weight_copies:
        copy.start()

    barrier = pltpu.get_barrier_semaphore()

    @pl.loop(1, n)
    def _(k):
        pl.semaphore_signal(barrier, inc=1, device_id=((s + k) % n, t), device_id_type=MESH)

    for peer in (mate, across):
        pl.semaphore_signal(barrier, inc=1, device_id=(s, peer), device_id_type=MESH)
    pl.semaphore_wait(barrier, n + 1)

    def remote(src, dst, lane, k, device):
        return pltpu.make_async_remote_copy(
            src_ref=src,
            dst_ref=dst,
            send_sem=send.at[lane, k],
            recv_sem=got.at[lane, k],
            device_id=device,
            device_id_type=MESH,
        )

    def outward(k):
        to = (s + k // halves) % n
        return remote(out_ref.at[to * halves + k % halves], recv.at[k, t], 0, k, (to, t))

    def over(k, block):
        return remote(recv.at[k, block], recv.at[k, block], 1, k, (s, across))

    def pair_own(k, block):
        return remote(recv.at[k, block], recv.at[k, block], 2, k, (s, mate))

    def pair_far(k, block):
        return remote(recv.at[k, block], recv.at[k, block], 3, k, (s, mate))

    def part_near(k):
        return remote(part.at[k, mate], mrecv.at[k, 0], 4, k, (s, mate))

    def part_far(k):
        return remote(part.at[k, mate_across], mrecv.at[k, 1], 5, k, (s, mate))

    def sum_over(k):
        return remote(psum.at[k], xrecv.at[k], 6, k, (s, across))

    def homeward(k):
        to = (s + n - k // halves) % n
        return remote(fin.at[k], ret_ref.at[s * halves + k % halves], 7, k, (to, t))

    own = [
        pltpu.make_async_copy(out_ref.at[s * halves + h], recv.at[h, t], local_sem.at[3 + h])
        for h in range(halves)
    ]
    for copy in own:
        copy.start()

    @pl.loop(halves, steps)
    def _(k):
        outward(k).start()

    for copy in own:
        copy.wait()

    def ffn(k):
        def load():
            block = recv[k]
            if cap % 16:
                return block.astype(jnp.float32).reshape(rows, width).astype(jnp.bfloat16)
            return block.reshape(rows, width)

        cols = min(256, units)

        @pl.loop(0, units // cols)
        def _(c):
            at = pl.ds(pl.multiple_of(c * cols, cols), cols)
            x = load()
            gate = jnp.dot(x, gate_w[:, at], preferred_element_type=jnp.float32)
            up = jnp.dot(x, up_w[:, at], preferred_element_type=jnp.float32)
            hid[:, at] = (gate / (1.0 + jnp.exp(-gate)) * up).astype(jnp.bfloat16)

        wide = min(512, width)

        @pl.loop(0, width // wide)
        def _(c):
            at = pl.ds(pl.multiple_of(c * wide, wide), wide)
            y = jnp.dot(hid[...], down_w[:, at], preferred_element_type=jnp.float32)
            part[k, :, :, at] = y.reshape(tp, cap, wide).astype(jnp.bfloat16)

    def wide_sum(*blocks):
        total = blocks[0].astype(jnp.float32)
        for block in blocks[1:]:
            total = total + block.astype(jnp.float32)
        return total

    @pl.loop(0, steps + 4)
    def _(i):
        @pl.when(i < steps)
        def _():
            @pl.when(i >= halves)
            def _():
                outward(i).wait_recv()

            over(i, t).start()
            pair_own(i, t).start()

        @pl.when((i >= 1) & (i < steps + 1))
        def _():
            k = i - 1
            over(k, across).wait_recv()
            pair_far(k, across).start()

        @pl.when((i >= 3) & (i < steps + 3))
        def _():
            k = i - 3
            part_far(k).wait_recv()
            psum[k] = wide_sum(part[k, across], mrecv[k, 1]).astype(jnp.bfloat16)
            sum_over(k).start()

        @pl.when(i >= 4)
        def _():
            k = i - 4
            part_near(k).wait_recv()
            sum_over(k).wait_recv()
            total = wide_sum(part[k, t], mrecv[k, 0], xrecv[k]).astype(jnp.bfloat16)

            @pl.when(k < halves)
            def _():
                ret_ref[s * halves + k] = total

            @pl.when(k >= halves)
            def _():
                fin[k] = total
                homeward(k).start()

        @pl.when(i == 2)
        def _():
            for copy in weight_copies:
                copy.wait()

        @pl.when((i >= 2) & (i < steps + 2))
        def _():
            k = i - 2
            pair_own(k, mate).wait_recv()
            pair_far(k, mate_across).wait_recv()
            ffn(k)
            part_far(k).start()
            part_near(k).start()

    @pl.loop(0, steps)
    def _(k):
        over(k, t).wait_send()
        pair_own(k, t).wait_send()
        pair_far(k, across).wait_send()
        part_near(k).wait_send()
        part_far(k).wait_send()
        sum_over(k).wait_send()

        @pl.when(k >= halves)
        def _():
            outward(k).wait_send()
            homeward(k).wait_send()
            homeward(k).wait_recv()


def run_experts(outgoing, gate_weight, up_weight, down_weight):
    n, cap, width = outgoing.shape
    tp = lax.axis_size("tp")
    units = gate_weight.shape[1]
    halves = 2 if cap % 32 == 0 else 1
    steps, cap = n * halves, cap // halves
    vmem = pl.BlockSpec(memory_space=pltpu.VMEM)
    hbm = pl.BlockSpec(memory_space=pl.ANY)
    bf16 = jnp.bfloat16
    return pl.pallas_call(
        functools.partial(expert_kernel, n, tp, halves),
        out_shape=jax.ShapeDtypeStruct((steps, cap, width), bf16),
        in_specs=[vmem, hbm, hbm, hbm],
        out_specs=vmem,
        scratch_shapes=[
            pltpu.VMEM((steps, tp, cap, width), bf16),
            pltpu.VMEM((steps, tp, cap, width), bf16),
            pltpu.VMEM((steps, 2, cap, width), bf16),
            pltpu.VMEM((steps, cap, width), bf16),
            pltpu.VMEM((steps, cap, width), bf16),
            pltpu.VMEM((steps, cap, width), bf16),
            pltpu.VMEM(gate_weight.shape, bf16),
            pltpu.VMEM(up_weight.shape, bf16),
            pltpu.VMEM(down_weight.shape, bf16),
            pltpu.VMEM((tp * cap, units), bf16),
            pltpu.SemaphoreType.DMA((3 + halves,)),
            pltpu.SemaphoreType.DMA((8, steps)),
            pltpu.SemaphoreType.DMA((8, steps)),
        ],
        compiler_params=pltpu.CompilerParams(
            collective_id=1, has_side_effects=True, vmem_limit_bytes=60 * 1024 * 1024
        ),
    )(outgoing.reshape(steps, cap, width), gate_weight, up_weight, down_weight)


def exchange_body(
    gate_in,
    value_in,
    gate_out,
    conv_taps,
    proj_weight,
    residual,
    norm_gain,
    routes,
    route_weight,
    expert_gate,
    expert_up,
    expert_down,
):
    model_width = residual.shape[1]
    tp_count = lax.axis_size("tp")
    groups = lax.axis_size("sp")
    quarter = residual.shape[0]
    top_count = routes.shape[1]
    capacity = 2 * quarter * top_count // groups
    tp_index = lax.axis_index("tp")
    first_own = tp_index * quarter
    own_routes = lax.dynamic_slice_in_dim(routes, first_own, quarter, 0)
    own_weights = lax.dynamic_slice_in_dim(route_weight, first_own, quarter, 0)
    my_rows, normed = run_mixer(
        gate_in, value_in, gate_out, conv_taps, proj_weight, residual, norm_gain
    )
    own_slots = slot_numbers(own_routes, quarter, groups)
    flat_pick = own_routes * capacity + own_slots
    slot_count = groups * capacity
    outgoing = dispatch_rows(normed, flat_pick, slot_count)
    returned = run_experts(
        outgoing.reshape(groups, capacity, model_width),
        expert_gate[0],
        expert_up[0],
        expert_down[0],
    ).reshape(slot_count, model_width)
    total = my_rows
    for k in range(top_count):
        pick = flat_pick[:, k, None] == jnp.arange(slot_count, dtype=jnp.int32)
        picked = jnp.dot(
            pick.astype(jnp.bfloat16), returned, preferred_element_type=jnp.float32
        )
        total = total + own_weights[:, k, None] * picked
    return total.astype(jnp.bfloat16)


def plane_of(j, z, planes):
    return jnp.where(z < planes // 2, z + j, z + planes - j) % planes


def layer_kernel(
    n, tp, halo, pieces, cap, early,
    routes_ref, weights_ref, taps_ref, gain_ref,
    gate_hbm, value_hbm, out_gate_hbm, proj_hbm, res_hbm, wg_hbm, wu_hbm, wd_hbm,
    out_ref,
    gate_ref, value_ref, out_gate_ref, proj_ref, res_ref, gate_w, up_w, down_w,
    edge, product, mixed, mpart, mmate, msum, mfar,
    rows, info, far_info, spread, raw, far_raw, ysend, far_ysend, recv, part, mrecv, psum, xrecv, fin, ret, hid,
    local_sem, msend, mgot, isend, igot, rsend, rgot, ysem, ygot, dsend, dgot, psend, pgot, hsend, hgot,
    csend, fisend, figot, frsend, frgot, fysem, fygot,
):
    s = lax.axis_index("sp")
    t = lax.axis_index("tp")
    planes = n // 2
    z, y = s // 2, s % 2
    other_y = 1 - y
    mate = t + 1 - 2 * (t % 2)
    across = (t + 2) % tp
    mate_across = (mate + 2) % tp
    tokens = gate_ref.shape[0]
    quarter, width = res_ref.shape
    half = cap // 2
    units = 2 * planes
    after, before = (s + 1) % n, (s + n - 1) % n
    f32, bf16 = jnp.float32, jnp.bfloat16

    loads = [
        pltpu.make_async_copy(src, dst, local_sem.at[i])
        for i, (src, dst) in enumerate(
            [
                (gate_hbm, gate_ref), (value_hbm, value_ref), (out_gate_hbm, out_gate_ref),
                (proj_hbm, proj_ref), (res_hbm, res_ref),
                (wg_hbm, gate_w), (wu_hbm, up_w), (wd_hbm, down_w),
            ]
        )
    ]
    for copy in loads[:5]:
        copy.start()

    barrier = pltpu.get_barrier_semaphore()

    @pl.loop(1, n)
    def _(k):
        pl.semaphore_signal(barrier, inc=1, device_id=((s + k) % n, t), device_id_type=MESH)

    @pl.loop(1, planes)
    def _(k):
        to = (z + k) % planes * 2 + y
        pl.semaphore_signal(barrier, inc=1, device_id=(to, across), device_id_type=MESH)

    for peer in (mate, across):
        pl.semaphore_signal(barrier, inc=1, device_id=(s, peer), device_id_type=MESH)

    def remote(src, dst, send_sem, recv_sem, device):
        return pltpu.make_async_remote_copy(
            src_ref=src, dst_ref=dst, send_sem=send_sem, recv_sem=recv_sem,
            device_id=device, device_id_type=MESH,
        )

    own_at = pl.ds(pl.multiple_of(t * quarter, quarter), quarter)
    named = [routes_ref[k:k + 1, own_at] for k in range(2)]
    expert_ids = lax.broadcasted_iota(jnp.int32, (n, quarter), 0)
    one_hot = [(expert_ids == name).astype(f32) for name in named]
    earlier = (
        lax.broadcasted_iota(jnp.int32, (quarter, quarter), 0)
        < lax.broadcasted_iota(jnp.int32, (quarter, quarter), 1)
    ).astype(bf16)
    count = jnp.dot(
        (one_hot[0] + one_hot[1]).astype(bf16), earlier, preferred_element_type=f32
    )
    picks = [
        name.astype(f32) * cap + jnp.sum(count * hot, axis=0, keepdims=True)
        for name, hot in zip(named, one_hot)
    ]
    def tell(k):
        to = (z + k) % planes
        return remote(info.at[z], info.at[z], isend.at[k], igot.at[z], (to * 2 + y, t))

    def told(k):
        origin = (z + k) % planes
        return remote(info.at[origin], info.at[origin], isend.at[k], igot.at[origin], (s, mate))

    for copy in loads[5:]:
        copy.start()

    def tell_far(k):
        to = (z + k) % planes
        return remote(info.at[z], far_info.at[z], fisend.at[k], figot.at[z], (to * 2 + y, across))

    def told_far(origin):
        ref = far_info.at[origin]
        return remote(ref, ref, fisend.at[0], figot.at[origin], (s, mate))

    for copy in loads[:2]:
        copy.wait()
    product[pl.ds(halo, tokens)] = gate_ref[...].astype(f32) * value_ref[...].astype(f32)
    loads[2].wait()
    part_width = width // pieces

    def mix(block):
        at = pl.ds(pl.multiple_of(block * quarter, quarter), quarter)
        window = product[pl.ds(pl.multiple_of(block * quarter, quarter), halo + quarter)]
        conv_sum = (
            taps_ref[0:1] * window[halo - 2:halo - 2 + quarter]
            + taps_ref[1:2] * window[halo - 1:halo - 1 + quarter]
            + taps_ref[2:3] * window[halo:]
        )
        mixed[at] = (out_gate_ref[at].astype(f32) * conv_sum).astype(bf16)

    @pl.loop(1, tp)
    def _(block):
        mix(block)

    def columns(p):
        return pl.ds(p * part_width, part_width)

    def project(block, p):
        at = pl.ds(pl.multiple_of(block * quarter, quarter), quarter)
        y_block = jnp.dot(mixed[at], proj_ref[:, columns(p)], preferred_element_type=f32)
        mpart[block, p] = y_block.astype(bf16)

    loads[3].wait()
    opens = mate_across == 0
    ahead = jnp.where(opens, across, mate_across)
    for p in range(pieces):
        project(ahead, p)

    tail = pl.ds(tokens - halo, halo)
    edges = [
        remote(ref.at[tail], edge.at[i], msend.at[i], mgot.at[i], (after, t))
        for i, ref in enumerate((gate_ref, value_ref))
    ]
    pl.semaphore_wait(barrier, n + planes)
    for copy in edges:
        copy.start()


    def first_block(block):
        @pl.when(block == 0)
        def _():
            for copy in edges:
                copy.wait_recv()
            prior = edge[0].astype(f32) * edge[1].astype(f32)
            product[pl.ds(0, halo)] = jnp.where(s == 0, 0.0, prior)
            mix(block)

    def lane(kind, p):
        return 2 + kind * pieces + p

    def to_mate(kind, block, p):
        at = lane(kind, p)
        return remote(mpart.at[block, p], mmate.at[kind, p], msend.at[at], mgot.at[at], (s, mate))

    def to_across(p):
        at = lane(2, p)
        return remote(msum.at[p], mfar.at[p], msend.at[at], mgot.at[at], (s, across))

    def cross_sum(p):
        to_mate(0, mate_across, p).wait_recv()
        msum[p] = (mpart[across, p].astype(f32) + mmate[0, p].astype(f32)).astype(bf16)
        to_across(p).start()

    @pl.when(opens)
    def _():
        for p in range(pieces):
            cross_sum(p)
        first_block(mate_across)
        for p in range(pieces):
            project(mate_across, p)
            to_mate(0, mate_across, p).start()

    @pl.when(jnp.logical_not(opens))
    def _():
        for p in range(pieces):
            to_mate(0, mate_across, p).start()
        first_block(across)
        for p in range(pieces):
            project(across, p)
            cross_sum(p)

    first_block(mate)
    for p in range(pieces):
        project(mate, p)
        to_mate(1, mate, p).start()
    first_block(t)
    for p in range(pieces):
        project(t, p)

    slot_ids = lax.broadcasted_iota(jnp.int32, (n * cap, quarter), 0).astype(f32)
    share = jnp.where(slot_ids == picks[0], weights_ref[0:1, own_at], 0.0) + jnp.where(
        slot_ids == picks[1], weights_ref[1:2, own_at], 0.0
    )
    share = jnp.transpose(share)
    high = share.astype(bf16)
    spread[0] = high
    spread[1] = (share - high.astype(f32)).astype(bf16)

    def along(block, up, at=slice(None)):
        to = jnp.where(up == 1, z + 1, z - 1)
        ref = raw.at[block, :, at]
        return remote(ref, ref, rsend.at[up, block], rgot.at[block], (to * 2 + y, t))

    def has_up(block):
        return (block <= z) & (z < planes - 1)

    def has_down(block):
        return (block >= z) & (z > 0)

    def pass_on(block):
        @pl.when(has_up(block))
        def _():
            along(block, 1).start()

        @pl.when(has_down(block))
        def _():
            along(block, 0).start()

    first_columns, last_columns = pl.ds(0, early), pl.ds(early, width - early)

    def cross():
        return remote(
            raw.at[z, :, first_columns], far_raw.at[z], csend.at[0], frgot.at[z], (s, across)
        )

    def along_far(block, up):
        to = jnp.where(up == 1, z + 1, z - 1)
        ref = far_raw.at[block]
        return remote(ref, ref, frsend.at[up, block], frgot.at[block], (to * 2 + y, t))

    loads[4].wait()
    square = jnp.zeros((quarter, 1), f32)
    for p in range(pieces):
        at = columns(p)
        to_mate(1, mate, p).wait_recv()
        to_across(p).wait_recv()
        summed = mpart[t, p].astype(f32) + mmate[1, p].astype(f32) + mfar[p].astype(f32)
        hidden_rows = res_ref[:, at].astype(f32) + summed
        rows[:, at] = hidden_rows
        raw[z, :, at] = (hidden_rows * gain_ref[:, at]).astype(bf16)
        for up, has in ((1, has_up), (0, has_down)):
            @pl.when(has(z))
            def _():
                along(z, up, at).start()

        if p == (early - 1) // part_width:
            cross().start()
        square = square + jnp.sum(hidden_rows * hidden_rows, axis=-1, keepdims=True)
    inverse = lax.rsqrt(square / width + 1e-05)
    scale = jnp.transpose(jnp.broadcast_to(inverse, (quarter, quarter)))[0:1]
    info[z] = jnp.concatenate(picks + [scale, jnp.zeros((5, quarter), f32)], axis=0)

    @pl.loop(1, planes)
    def _(k):
        tell(k).start()

    @pl.loop(0, planes)
    def _(k):
        tell_far(k).start()

    def beside(j, h):
        return remote(
            ysend.at[j, h], recv.at[j, h, t, y], ysem.at[j, h], ygot.at[j, h], (z * 2 + other_y, t)
        )

    def beside_far(j, h):
        return remote(
            far_ysend.at[j, h], recv.at[j, h, across, y, :, first_columns],
            fysem.at[j, h], fygot.at[j, h], (z * 2 + other_y, t),
        )

    def over(j, h, source):
        ref = recv.at[j, h, t, source, :, last_columns]
        return remote(ref, ref, dsend.at[0, j, h, source], dgot.at[0, j, h, source], (s, across))

    def pair_own(j, h, source):
        ref = recv.at[j, h, t, source]
        return remote(ref, ref, dsend.at[1, j, h, source], dgot.at[1, j, h, source], (s, mate))

    def pair_far(j, h, source):
        ref = recv.at[j, h, across, source]
        return remote(ref, ref, dsend.at[2, j, h, source], dgot.at[2, j, h, source], (s, mate))

    wide = min(512, width)

    def select(raw, info, block, expert, put):
        place = lax.broadcasted_iota(jnp.int32, (cap, quarter), 0).astype(f32) + (
            expert * cap
        ).astype(f32)
        table = info[block]
        named = (place == table[0:1]) | (place == table[1:2])
        chosen = named.astype(f32).astype(bf16)
        scale = jnp.sum(jnp.where(named, table[2:3], 0.0), axis=1, keepdims=True)

        step = raw.shape[2] if raw.shape[2] % wide else wide

        @pl.loop(0, raw.shape[2] // step)
        def _(c):
            at = pl.ds(pl.multiple_of(c * step, step), step)
            taken = jnp.dot(chosen, raw[block, :, at], preferred_element_type=f32)
            taken = (taken * scale).astype(bf16)
            for h in range(2):
                put(h, at, taken[h * half:(h + 1) * half])

    def arrive_far(j):
        block = plane_of(j, z, planes)
        along_far(block, 1).wait_recv()

        @pl.when(has_up(block))
        def _():
            along_far(block, 1).start()

        @pl.when(has_down(block))
        def _():
            along_far(block, 0).start()

    def dispatch_early(j):
        block = plane_of(j, z, planes)
        told_far(block).wait_recv()

        def put_own(h, at, value):
            recv[j, h, across, y, :, at] = value

        def put_other(h, at, value):
            far_ysend[j, h, :, at] = value

        select(far_raw, far_info, block, z * 2 + other_y, put_other)
        for h in range(2):
            beside_far(j, h).start()
        select(far_raw, far_info, block, s, put_own)

    def arrive(j):
        block = plane_of(j, z, planes)
        along(block, 1).wait_recv()
        pass_on(block)

    def hear(j):
        @pl.when(j > 0)
        def _():
            told((plane_of(j, z, planes) + planes - z) % planes).wait_recv()

    def dispatch_own(j):
        def put(h, at, value):
            recv[j, h, t, y, :, at] = value

        select(raw, info, plane_of(j, z, planes), s, put)
        for h in range(2):
            over(j, h, y).start()
            pair_own(j, h, y).start()

    def dispatch_other(j):
        def put(h, at, value):
            ysend[j, h, :, at] = value

        select(raw, info, plane_of(j, z, planes), z * 2 + other_y, put)
        for h in range(2):
            beside(j, h).start()

    def dispatch_beside(j):
        for h in range(2):
            beside(j, h).wait_recv()
            over(j, h, other_y).start()
            pair_own(j, h, other_y).start()

    def dispatch_far(j, source, crossed):
        for h in range(2):
            over(j, h, source).wait_recv()
            if crossed:
                beside_far(j, h).wait_recv()
            pair_far(j, h, source).start()

    def part_near(u):
        return remote(part.at[u, mate], mrecv.at[u, 0], psend.at[0, u], pgot.at[0, u], (s, mate))

    def part_far(u):
        return remote(part.at[u, mate_across], mrecv.at[u, 1], psend.at[1, u], pgot.at[1, u], (s, mate))

    def sum_over(u):
        return remote(psum.at[u], xrecv.at[u], psend.at[2, u], pgot.at[2, u], (s, across))

    def ffn(j, h):
        u = 2 * j + h
        for source in range(2):
            pair_own(j, h, source).wait_recv()
            pair_far(j, h, source).wait_recv()
        count = gate_w.shape[1]
        cols = min(256, count)

        @pl.loop(0, count // cols)
        def _(c):
            at = pl.ds(pl.multiple_of(c * cols, cols), cols)
            x = recv[j, h].reshape(tp * cap, width)
            gate = jnp.dot(x, gate_w[:, at], preferred_element_type=f32)
            up = jnp.dot(x, up_w[:, at], preferred_element_type=f32)
            hid[:, at] = (gate / (1.0 + jnp.exp(-gate)) * up).astype(bf16)

        @pl.loop(0, width // wide)
        def _(c):
            at = pl.ds(pl.multiple_of(c * wide, wide), wide)
            out = jnp.dot(hid[...], down_w[:, at], preferred_element_type=f32)
            part[u, :, :, :, at] = out.reshape(tp, 2, half, wide).astype(bf16)

        part_far(u).start()
        part_near(u).start()

    def homeward(j, h, source):
        u = 2 * j + h
        to = plane_of(j, z, planes) * 2 + source
        return remote(fin.at[u, source], ret.at[s, h], hsend.at[u, source], hgot.at[s, h], (to, t))

    def returned(origin, h):
        return remote(ret.at[origin, h], ret.at[origin, h], hsend.at[0, 0], hgot.at[origin, h], (s, mate))

    def sum_far(j, h):
        u = 2 * j + h
        part_far(u).wait_recv()
        psum[u] = (part[u, across].astype(f32) + mrecv[u, 1].astype(f32)).astype(bf16)
        sum_over(u).start()

    def send_home(j, h):
        u = 2 * j + h
        part_near(u).wait_recv()
        sum_over(u).wait_recv()
        total = (
            part[u, t].astype(f32) + mrecv[u, 0].astype(f32) + xrecv[u].astype(f32)
        ).astype(bf16)
        fin[u] = total

        @pl.when(j == 0)
        def _():
            ret[s, h] = fin[u, y]
            homeward(j, h, other_y).start()

        @pl.when(j > 0)
        def _():
            for source in range(2):
                homeward(j, h, source).start()

    def gather(plane, put):
        for source in range(2):
            for h in range(2):
                origin = plane * 2 + source

                @pl.when(origin != s)
                def _():
                    returned(origin, h).wait_recv()

        slots = pl.ds(pl.multiple_of(plane * 2 * cap, 2 * cap), 2 * cap)

        @pl.loop(0, width // wide)
        def _(c):
            at = pl.ds(pl.multiple_of(c * wide, wide), wide)
            got = ret[pl.ds(plane * 2, 2), :, :, at].reshape(2 * cap, wide)
            put(
                at,
                rows[:, at]
                + jnp.dot(spread[0, :, slots], got, preferred_element_type=f32)
                + jnp.dot(spread[1, :, slots], got, preferred_element_type=f32),
            )

    def keep(at, value):
        rows[:, at] = value

    def finish(at, value):
        out_ref[:, at] = value.astype(bf16)

    at_end = (z == 0) | (z == planes - 1)
    late = jnp.where(at_end, 1, 0)

    def far_near(j):
        dispatch_far(j, y, False)

    def far_other(j):
        dispatch_far(j, other_y, True)

    def home_pair(j):
        send_home(j, 0)
        send_home(j, 1)

    def take(j):
        hear(j)
        dispatch_own(j)
        dispatch_other(j)

    last = planes - 1
    middle_start = [
        (dispatch_own, 0), (arrive_far, 0), (arrive, 1), (arrive, last), (hear, 1),
        (dispatch_other, 1), (dispatch_own, 1), (arrive_far, 1), (arrive_far, last),
        (dispatch_early, 1), (hear, last), (dispatch_other, last), (dispatch_early, last),
        (far_near, 1), (dispatch_beside, 1), (dispatch_own, last), (dispatch_other, 0),
        (dispatch_early, 0), (far_other, 1),
    ]
    middle_after = [
        [
            (arrive, 2), (sum_far, 1, 0), (dispatch_beside, last), (take, 2), (arrive_far, 2),
            (dispatch_early, 2),
        ],
        [(sum_far, 1, 1), (send_home, 1, 0), (far_near, last), (far_other, last), (dispatch_beside, 2)],
        [(sum_far, last, 0), (far_near, 2), (send_home, 1, 1), (far_other, 2)],
        [(sum_far, 2, 0), (send_home, last, 0)],
        [(sum_far, last, 1), (dispatch_beside, 0)],
        [
            (send_home, 2, 0), (sum_far, 2, 1), (far_near, 0), (send_home, last, 1),
            (far_other, 0),
        ],
        [(sum_far, 0, 0)],
        [(sum_far, 0, 1), (send_home, 2, 1)],
    ]
    end_start = [
        (dispatch_own, 0), (dispatch_other, 0), (arrive_far, 0), (arrive, 1), (dispatch_early, 0),
        (dispatch_beside, 0), (take, 1), (arrive_far, 1), (dispatch_early, 1),
        (far_near, 0), (far_other, 0),
    ]
    end_after = [
        [(sum_far, 0, 0), (dispatch_beside, 1)],
        [
            (arrive, 2), (take, 2), (arrive_far, 2), (dispatch_early, 2),
            (far_near, 1), (far_other, 1),
        ],
        [(dispatch_beside, 2)],
        [
            (sum_far, 1, 0), (arrive, last), (take, last), (arrive_far, last),
            (dispatch_early, last), (far_near, 2), (far_other, 2),
        ],
        [(sum_far, 2, 0), (send_home, 1, 0), (dispatch_beside, last)],
        [(sum_far, 2, 1), (far_near, last), (send_home, 2, 0), (far_other, last)],
        [(sum_far, last, 0)],
        [
            (send_home, 2, 1), (sum_far, last, 1), (sum_far, 1, 1), (sum_far, 0, 1),
            (send_home, 0, 0), (send_home, last, 0), (send_home, last, 1), (send_home, 1, 1),
        ],
    ]

    def carry_out(actions):
        for act, *where in actions:
            act(*[jnp.int32(place) for place in where])

    @pl.when(late == 0)
    def _():
        carry_out(middle_start)

    @pl.when(late == 1)
    def _():
        carry_out(end_start)

    for copy in loads[5:]:
        copy.wait()

    @pl.loop(0, units)
    def _(k):
        woven = (k > 1) & (k < units - 2)
        middle_plane = jnp.where(k < 2, 1, jnp.where(woven, jnp.where(k % 2 == 0, last, 2), 0))
        middle_half = jnp.where(woven, k // planes, k % 2)
        ffn(jnp.where(late == 1, k // 2, middle_plane), jnp.where(late == 1, k % 2, middle_half))
        for step in range(units):
            @pl.when((k == step) & (late == 0))
            def _():
                carry_out(middle_after[step])

            @pl.when((k == step) & (late == 1))
            def _():
                carry_out(end_after[step])

    @pl.when(late == 1)
    def _():
        send_home(jnp.int32(0), jnp.int32(1))

    @pl.loop(1, planes - 1)
    def _(j):
        gather(plane_of(j + late, z, planes), keep)

    @pl.when(late == 0)
    def _():
        send_home(jnp.int32(0), jnp.int32(0))
        send_home(jnp.int32(0), jnp.int32(1))

    gather(plane_of(jnp.where(late == 1, 1, planes - 1), z, planes), keep)
    for copy in edges:
        copy.wait_send()
    for p in range(pieces):
        to_mate(0, mate_across, p).wait_send()
        to_mate(1, mate, p).wait_send()
        to_across(p).wait_send()

    @pl.loop(0, planes)
    def _(j):
        @pl.when(j > 0)
        def _():
            tell(j).wait_send()

        tell_far(j).wait_send()

        @pl.when(has_up(j))
        def _():
            along(j, 1).wait_send()
            along_far(j, 1).wait_send()

        @pl.when(has_down(j))
        def _():
            along(j, 0).wait_send()
            along_far(j, 0).wait_send()

        for h in range(2):
            beside(j, h).wait_send()
            beside_far(j, h).wait_send()
            for source in range(2):
                over(j, h, source).wait_send()
                pair_own(j, h, source).wait_send()
                pair_far(j, h, source).wait_send()

    cross().wait_send()

    @pl.loop(0, units)
    def _(u):
        part_near(u).wait_send()
        part_far(u).wait_send()
        sum_over(u).wait_send()

    gather(z, finish)

    @pl.loop(0, units)
    def _(u):
        homeward(u // 2, u % 2, other_y).wait_send()

        @pl.when(u > 1)
        def _():
            homeward(u // 2, u % 2, y).wait_send()


def relay_body(
    gate_in, value_in, gate_out, conv_taps, proj_weight, residual, norm_gain,
    routes, route_weight, expert_gate, expert_up, expert_down,
):
    n, tp = lax.axis_size("sp"), lax.axis_size("tp")
    tokens, channels = gate_in.shape
    quarter, width = residual.shape
    cap = 2 * quarter * routes.shape[1] // n
    units_hidden = expert_gate.shape[2]
    planes, half = n // 2, cap // 2
    units = 2 * planes
    halo, pieces = 16, 4
    early = width // 1024 * 384
    part_width = width // pieces
    vmem = pl.BlockSpec(memory_space=pltpu.VMEM)
    hbm = pl.BlockSpec(memory_space=pl.ANY)
    bf16, f32 = jnp.bfloat16, jnp.float32
    dma = pltpu.SemaphoreType.DMA
    rows = (2, half, width)
    return pl.pallas_call(
        functools.partial(layer_kernel, n, tp, halo, pieces, cap, early),
        out_shape=jax.ShapeDtypeStruct((quarter, width), bf16),
        in_specs=[vmem] * 4 + [hbm] * 8,
        out_specs=vmem,
        scratch_shapes=[
            pltpu.VMEM((tokens, channels), bf16),
            pltpu.VMEM((tokens, channels), bf16),
            pltpu.VMEM((tokens, channels), bf16),
            pltpu.VMEM(proj_weight.shape, bf16),
            pltpu.VMEM((quarter, width), bf16),
            pltpu.VMEM((width, units_hidden), bf16),
            pltpu.VMEM((width, units_hidden), bf16),
            pltpu.VMEM((units_hidden, width), bf16),
            pltpu.VMEM((2, halo, channels), bf16),
            pltpu.VMEM((halo + tokens, channels), f32),
            pltpu.VMEM((tokens, channels), bf16),
            pltpu.VMEM((tp, pieces, quarter, part_width), bf16),
            pltpu.VMEM((2, pieces, quarter, part_width), bf16),
            pltpu.VMEM((pieces, quarter, part_width), bf16),
            pltpu.VMEM((pieces, quarter, part_width), bf16),
            pltpu.VMEM((quarter, width), f32),
            pltpu.VMEM((planes, 8, quarter), f32),
            pltpu.VMEM((planes, 8, quarter), f32),
            pltpu.VMEM((2, quarter, n * cap), bf16),
            pltpu.VMEM((planes, quarter, width), bf16),
            pltpu.VMEM((planes, quarter, early), bf16),
            pltpu.VMEM((planes,) + rows, bf16),
            pltpu.VMEM((planes, 2, half, early), bf16),
            pltpu.VMEM((planes, 2, tp) + rows, bf16),
            pltpu.VMEM((units, tp) + rows, bf16),
            pltpu.VMEM((units, 2) + rows, bf16),
            pltpu.VMEM((units,) + rows, bf16),
            pltpu.VMEM((units,) + rows, bf16),
            pltpu.VMEM((units,) + rows, bf16),
            pltpu.VMEM((n,) + rows, bf16),
            pltpu.VMEM((tp * cap, units_hidden), bf16),
            dma((8,)),
            dma((2 + 3 * pieces,)),
            dma((2 + 3 * pieces,)),
            dma((planes,)),
            dma((planes,)),
            dma((2, planes)),
            dma((planes,)),
            dma((planes, 2)),
            dma((planes, 2)),
            dma((3, planes, 2, 2)),
            dma((3, planes, 2, 2)),
            dma((3, units)),
            dma((3, units)),
            dma((units, 2)),
            dma((n, 2)),
            dma((1,)),
            dma((planes,)),
            dma((planes,)),
            dma((2, planes)),
            dma((planes,)),
            dma((planes, 2)),
            dma((planes, 2)),
        ],
        compiler_params=pltpu.CompilerParams(
            collective_id=3, has_side_effects=True, vmem_limit_bytes=60 * 1024 * 1024
        ),
    )(
        routes.T, route_weight.T, conv_taps, norm_gain.reshape(1, width),
        gate_in, value_in, gate_out, proj_weight, residual,
        expert_gate[0], expert_up[0], expert_down[0],
    )


def body(*args):
    residual, routes = args[5], args[7]
    n, tp = lax.axis_size("sp"), lax.axis_size("tp")
    quarter = residual.shape[0]
    capacity = 2 * quarter * routes.shape[1] // n
    relay = n == 2 * tp and tp == 4 and capacity % 32 == 0 and quarter % 128 == 0 and residual.shape[1] % 1024 == 0
    if relay and (n // 2) * quarter <= n * capacity:
        return relay_body(*args)
    return exchange_body(*args)


def solution(mesh):
    placed = (
        P("sp", "tp"),
        P("sp", "tp"),
        P("sp", "tp"),
        P(None, "tp"),
        P("tp", None),
        P(("sp", "tp"), None),
        P(),
        P("sp", None),
        P("sp", None),
        P("sp", None, "tp"),
        P("sp", None, "tp"),
        P("sp", "tp", None),
    )
    return jax.shard_map(
        body, mesh=mesh, in_specs=placed, out_specs=P(("sp", "tp"), None), check_vma=False
    )
```

```python
import functools

import jax
import jax.numpy as jnp
from jax import lax
from jax.experimental import pallas as pl
from jax.experimental.pallas import tpu as pltpu
from jax.sharding import PartitionSpec as P


def slot_numbers(route_ids, block_rows, expert_count):
    block_count = route_ids.shape[0] // block_rows
    flat_ids = route_ids.reshape(block_count, block_rows * route_ids.shape[1])
    one_hot = (
        flat_ids[:, :, None] == jnp.arange(expert_count, dtype=jnp.int32)[None, None, :]
    ).astype(jnp.int32)
    before = jnp.cumsum(one_hot, axis=1) - one_hot
    return jnp.sum(before * one_hot, axis=2).reshape(route_ids.shape)


def dispatch_rows(normed, flat_pick, slot_count):
    slot_ids = jnp.arange(slot_count, dtype=jnp.int32)
    chosen = jnp.any(flat_pick[None, :, :] == slot_ids[:, None, None], axis=2)
    return jnp.dot(
        chosen.astype(jnp.bfloat16), normed, preferred_element_type=jnp.float32
    ).astype(jnp.bfloat16)


MESH = pl.DeviceIdType.MESH


def mixer_kernel(
    n, tp, halo, pieces, gate_ref, value_ref, out_gate_ref, taps_ref, proj_ref, res_ref, gain_ref,
    rows_ref, normed_ref, edge, product, mixed, part, mrecv, psum, xrecv, send, got,
):
    s = lax.axis_index("sp")
    t = lax.axis_index("tp")
    mate = t + 1 - 2 * (t % 2)
    across = (t + 2) % tp
    mate_across = (mate + 2) % tp
    tokens = gate_ref.shape[0]
    quarter, width = res_ref.shape
    piece = quarter // pieces
    after, before = (s + 1) % n, (s + n - 1) % n

    barrier = pltpu.get_barrier_semaphore()
    for peer in ((s, mate), (s, across), (after, t), (before, t)):
        pl.semaphore_signal(barrier, inc=1, device_id=peer, device_id_type=MESH)

    def remote(src, dst, lane, device):
        return pltpu.make_async_remote_copy(
            src_ref=src,
            dst_ref=dst,
            send_sem=send.at[lane],
            recv_sem=got.at[lane],
            device_id=device,
            device_id_type=MESH,
        )

    tail = pl.ds(tokens - halo, halo)
    edges = [
        remote(ref.at[tail], edge.at[i], i, (after, t))
        for i, ref in enumerate((gate_ref, value_ref))
    ]
    pl.semaphore_wait(barrier, 4)
    for copy in edges:
        copy.start()

    body_rows = pl.ds(halo, tokens)
    product[body_rows] = gate_ref[...].astype(jnp.float32) * value_ref[...].astype(jnp.float32)
    for copy in edges:
        copy.wait_recv()
    prior = edge[0].astype(jnp.float32) * edge[1].astype(jnp.float32)
    product[pl.ds(0, halo)] = jnp.where(s == 0, 0.0, prior)
    conv_sum = (
        taps_ref[0:1] * product[pl.ds(halo - 2, tokens)]
        + taps_ref[1:2] * product[pl.ds(halo - 1, tokens)]
        + taps_ref[2:3] * product[body_rows]
    )
    mixed[...] = (out_gate_ref[...].astype(jnp.float32) * conv_sum).astype(jnp.bfloat16)

    def project(block, p):
        first = pl.multiple_of(block * quarter + p * piece, piece)
        y = jnp.dot(
            mixed[pl.ds(first, piece)], proj_ref[...], preferred_element_type=jnp.float32
        )
        part[block, p] = y.astype(jnp.bfloat16)

    def lane(kind, p):
        return 2 + kind * pieces + p

    def to_mate(kind, block, p):
        return remote(part.at[block, p], mrecv.at[kind, p], lane(kind, p), (s, mate))

    def over(p):
        return remote(psum.at[p], xrecv.at[p], lane(2, p), (s, across))

    def wide(block):
        return block.astype(jnp.float32)

    for p in range(pieces):
        project(mate_across, p)
        to_mate(0, mate_across, p).start()
    for p in range(pieces):
        project(across, p)
        to_mate(0, mate_across, p).wait_recv()
        psum[p] = (wide(part[across, p]) + wide(mrecv[0, p])).astype(jnp.bfloat16)
        over(p).start()
    for p in range(pieces):
        project(mate, p)
        to_mate(1, mate, p).start()
    for p in range(pieces):
        project(t, p)
    for p in range(pieces):
        to_mate(1, mate, p).wait_recv()
        over(p).wait_recv()
        at = pl.ds(p * piece, piece)
        summed = wide(part[t, p]) + wide(mrecv[1, p]) + wide(xrecv[p])
        hidden_rows = wide(res_ref[at]) + summed
        inverse = lax.rsqrt(jnp.mean(hidden_rows * hidden_rows, axis=-1, keepdims=True) + 1e-05)
        rows_ref[at] = hidden_rows
        normed_ref[at] = (hidden_rows * inverse * gain_ref[...]).astype(jnp.bfloat16)
    for copy in edges:
        copy.wait_send()
    for p in range(pieces):
        to_mate(0, mate_across, p).wait_send()
        to_mate(1, mate, p).wait_send()
        over(p).wait_send()


def run_mixer(gate_in, value_in, gate_out, conv_taps, proj_weight, residual, norm_gain):
    n, tp = lax.axis_size("sp"), lax.axis_size("tp")
    tokens, channels = gate_in.shape
    quarter, width = residual.shape
    halo, pieces = 16, 4
    piece = quarter // pieces
    vmem = pl.BlockSpec(memory_space=pltpu.VMEM)
    bf16, f32 = jnp.bfloat16, jnp.float32
    return pl.pallas_call(
        functools.partial(mixer_kernel, n, tp, halo, pieces),
        out_shape=(
            jax.ShapeDtypeStruct((quarter, width), f32),
            jax.ShapeDtypeStruct((quarter, width), bf16),
        ),
        in_specs=[vmem] * 7,
        out_specs=(vmem, vmem),
        scratch_shapes=[
            pltpu.VMEM((2, halo, channels), bf16),
            pltpu.VMEM((halo + tokens, channels), f32),
            pltpu.VMEM((tokens, channels), bf16),
            pltpu.VMEM((tp, pieces, piece, width), bf16),
            pltpu.VMEM((2, pieces, piece, width), bf16),
            pltpu.VMEM((pieces, piece, width), bf16),
            pltpu.VMEM((pieces, piece, width), bf16),
            pltpu.SemaphoreType.DMA((2 + 3 * pieces,)),
            pltpu.SemaphoreType.DMA((2 + 3 * pieces,)),
        ],
        compiler_params=pltpu.CompilerParams(
            collective_id=2, has_side_effects=True, vmem_limit_bytes=60 * 1024 * 1024
        ),
    )(gate_in, value_in, gate_out, conv_taps, proj_weight, residual, norm_gain.reshape(1, width))


def expert_kernel(
    n, tp, halves, out_ref, gate_hbm, up_hbm, down_hbm, ret_ref,
    recv, part, mrecv, psum, xrecv, fin, gate_w, up_w, down_w, hid, local_sem, send, got,
):
    s = lax.axis_index("sp")
    t = lax.axis_index("tp")
    mate = t + 1 - 2 * (t % 2)
    across = (t + 2) % tp
    mate_across = (mate + 2) % tp
    cap, width = out_ref.shape[1], out_ref.shape[2]
    units = gate_w.shape[1]
    rows = tp * cap
    steps = n * halves

    weight_copies = [
        pltpu.make_async_copy(src, dst, local_sem.at[i])
        for i, (src, dst) in enumerate(
            [(gate_hbm, gate_w), (up_hbm, up_w), (down_hbm, down_w)]
        )
    ]
    for copy in weight_copies:
        copy.start()

    barrier = pltpu.get_barrier_semaphore()

    @pl.loop(1, n)
    def _(k):
        pl.semaphore_signal(barrier, inc=1, device_id=((s + k) % n, t), device_id_type=MESH)

    for peer in (mate, across):
        pl.semaphore_signal(barrier, inc=1, device_id=(s, peer), device_id_type=MESH)
    pl.semaphore_wait(barrier, n + 1)

    def remote(src, dst, lane, k, device):
        return pltpu.make_async_remote_copy(
            src_ref=src,
            dst_ref=dst,
            send_sem=send.at[lane, k],
            recv_sem=got.at[lane, k],
            device_id=device,
            device_id_type=MESH,
        )

    def outward(k):
        to = (s + k // halves) % n
        return remote(out_ref.at[to * halves + k % halves], recv.at[k, t], 0, k, (to, t))

    def over(k, block):
        return remote(recv.at[k, block], recv.at[k, block], 1, k, (s, across))

    def pair_own(k, block):
        return remote(recv.at[k, block], recv.at[k, block], 2, k, (s, mate))

    def pair_far(k, block):
        return remote(recv.at[k, block], recv.at[k, block], 3, k, (s, mate))

    def part_near(k):
        return remote(part.at[k, mate], mrecv.at[k, 0], 4, k, (s, mate))

    def part_far(k):
        return remote(part.at[k, mate_across], mrecv.at[k, 1], 5, k, (s, mate))

    def sum_over(k):
        return remote(psum.at[k], xrecv.at[k], 6, k, (s, across))

    def homeward(k):
        to = (s + n - k // halves) % n
        return remote(fin.at[k], ret_ref.at[s * halves + k % halves], 7, k, (to, t))

    own = [
        pltpu.make_async_copy(out_ref.at[s * halves + h], recv.at[h, t], local_sem.at[3 + h])
        for h in range(halves)
    ]
    for copy in own:
        copy.start()

    @pl.loop(halves, steps)
    def _(k):
        outward(k).start()

    for copy in own:
        copy.wait()

    def ffn(k):
        def load():
            block = recv[k]
            if cap % 16:
                return block.astype(jnp.float32).reshape(rows, width).astype(jnp.bfloat16)
            return block.reshape(rows, width)

        cols = min(256, units)

        @pl.loop(0, units // cols)
        def _(c):
            at = pl.ds(pl.multiple_of(c * cols, cols), cols)
            x = load()
            gate = jnp.dot(x, gate_w[:, at], preferred_element_type=jnp.float32)
            up = jnp.dot(x, up_w[:, at], preferred_element_type=jnp.float32)
            hid[:, at] = (gate / (1.0 + jnp.exp(-gate)) * up).astype(jnp.bfloat16)

        wide = min(512, width)

        @pl.loop(0, width // wide)
        def _(c):
            at = pl.ds(pl.multiple_of(c * wide, wide), wide)
            y = jnp.dot(hid[...], down_w[:, at], preferred_element_type=jnp.float32)
            part[k, :, :, at] = y.reshape(tp, cap, wide).astype(jnp.bfloat16)

    def wide_sum(*blocks):
        total = blocks[0].astype(jnp.float32)
        for block in blocks[1:]:
            total = total + block.astype(jnp.float32)
        return total

    @pl.loop(0, steps + 4)
    def _(i):
        @pl.when(i < steps)
        def _():
            @pl.when(i >= halves)
            def _():
                outward(i).wait_recv()

            over(i, t).start()
            pair_own(i, t).start()

        @pl.when((i >= 1) & (i < steps + 1))
        def _():
            k = i - 1
            over(k, across).wait_recv()
            pair_far(k, across).start()

        @pl.when((i >= 3) & (i < steps + 3))
        def _():
            k = i - 3
            part_far(k).wait_recv()
            psum[k] = wide_sum(part[k, across], mrecv[k, 1]).astype(jnp.bfloat16)
            sum_over(k).start()

        @pl.when(i >= 4)
        def _():
            k = i - 4
            part_near(k).wait_recv()
            sum_over(k).wait_recv()
            total = wide_sum(part[k, t], mrecv[k, 0], xrecv[k]).astype(jnp.bfloat16)

            @pl.when(k < halves)
            def _():
                ret_ref[s * halves + k] = total

            @pl.when(k >= halves)
            def _():
                fin[k] = total
                homeward(k).start()

        @pl.when(i == 2)
        def _():
            for copy in weight_copies:
                copy.wait()

        @pl.when((i >= 2) & (i < steps + 2))
        def _():
            k = i - 2
            pair_own(k, mate).wait_recv()
            pair_far(k, mate_across).wait_recv()
            ffn(k)
            part_far(k).start()
            part_near(k).start()

    @pl.loop(0, steps)
    def _(k):
        over(k, t).wait_send()
        pair_own(k, t).wait_send()
        pair_far(k, across).wait_send()
        part_near(k).wait_send()
        part_far(k).wait_send()
        sum_over(k).wait_send()

        @pl.when(k >= halves)
        def _():
            outward(k).wait_send()
            homeward(k).wait_send()
            homeward(k).wait_recv()


def run_experts(outgoing, gate_weight, up_weight, down_weight):
    n, cap, width = outgoing.shape
    tp = lax.axis_size("tp")
    units = gate_weight.shape[1]
    halves = 2 if cap % 32 == 0 else 1
    steps, cap = n * halves, cap // halves
    vmem = pl.BlockSpec(memory_space=pltpu.VMEM)
    hbm = pl.BlockSpec(memory_space=pl.ANY)
    bf16 = jnp.bfloat16
    return pl.pallas_call(
        functools.partial(expert_kernel, n, tp, halves),
        out_shape=jax.ShapeDtypeStruct((steps, cap, width), bf16),
        in_specs=[vmem, hbm, hbm, hbm],
        out_specs=vmem,
        scratch_shapes=[
            pltpu.VMEM((steps, tp, cap, width), bf16),
            pltpu.VMEM((steps, tp, cap, width), bf16),
            pltpu.VMEM((steps, 2, cap, width), bf16),
            pltpu.VMEM((steps, cap, width), bf16),
            pltpu.VMEM((steps, cap, width), bf16),
            pltpu.VMEM((steps, cap, width), bf16),
            pltpu.VMEM(gate_weight.shape, bf16),
            pltpu.VMEM(up_weight.shape, bf16),
            pltpu.VMEM(down_weight.shape, bf16),
            pltpu.VMEM((tp * cap, units), bf16),
            pltpu.SemaphoreType.DMA((3 + halves,)),
            pltpu.SemaphoreType.DMA((8, steps)),
            pltpu.SemaphoreType.DMA((8, steps)),
        ],
        compiler_params=pltpu.CompilerParams(
            collective_id=1, has_side_effects=True, vmem_limit_bytes=60 * 1024 * 1024
        ),
    )(outgoing.reshape(steps, cap, width), gate_weight, up_weight, down_weight)


def exchange_body(
    gate_in,
    value_in,
    gate_out,
    conv_taps,
    proj_weight,
    residual,
    norm_gain,
    routes,
    route_weight,
    expert_gate,
    expert_up,
    expert_down,
):
    model_width = residual.shape[1]
    tp_count = lax.axis_size("tp")
    groups = lax.axis_size("sp")
    quarter = residual.shape[0]
    top_count = routes.shape[1]
    capacity = 2 * quarter * top_count // groups
    tp_index = lax.axis_index("tp")
    first_own = tp_index * quarter
    own_routes = lax.dynamic_slice_in_dim(routes, first_own, quarter, 0)
    own_weights = lax.dynamic_slice_in_dim(route_weight, first_own, quarter, 0)
    my_rows, normed = run_mixer(
        gate_in, value_in, gate_out, conv_taps, proj_weight, residual, norm_gain
    )
    own_slots = slot_numbers(own_routes, quarter, groups)
    flat_pick = own_routes * capacity + own_slots
    slot_count = groups * capacity
    outgoing = dispatch_rows(normed, flat_pick, slot_count)
    returned = run_experts(
        outgoing.reshape(groups, capacity, model_width),
        expert_gate[0],
        expert_up[0],
        expert_down[0],
    ).reshape(slot_count, model_width)
    total = my_rows
    for k in range(top_count):
        pick = flat_pick[:, k, None] == jnp.arange(slot_count, dtype=jnp.int32)
        picked = jnp.dot(
            pick.astype(jnp.bfloat16), returned, preferred_element_type=jnp.float32
        )
        total = total + own_weights[:, k, None] * picked
    return total.astype(jnp.bfloat16)


def plane_of(j, z, planes):
    return jnp.where(z < planes // 2, z + j, z + planes - j) % planes


def layer_kernel(
    n, tp, halo, pieces, cap, early,
    routes_ref, weights_ref, taps_ref, gain_ref,
    gate_hbm, value_hbm, out_gate_hbm, proj_hbm, res_hbm, wg_hbm, wu_hbm, wd_hbm,
    out_ref,
    gate_ref, value_ref, out_gate_ref, proj_ref, res_ref, gate_w, up_w, down_w,
    edge, product, mixed, mpart, mmate, msum, mfar,
    rows, info, far_info, spread, raw, far_raw, ysend, far_ysend, recv, part, mrecv, psum, xrecv,
    fin, ret, hid,
    local_sem, msend, mgot, isend, igot, rsend, rgot, ysem, ygot, dsend, dgot, psend, pgot, hsend, hgot,
    csend, fisend, figot, frsend, frgot, fysem, fygot,
):
    s = lax.axis_index("sp")
    t = lax.axis_index("tp")
    planes = n // 2
    z, y = s // 2, s % 2
    other_y = 1 - y
    mate = t + 1 - 2 * (t % 2)
    across = (t + 2) % tp
    mate_across = (mate + 2) % tp
    tokens = gate_ref.shape[0]
    quarter, width = res_ref.shape
    half = cap // 2
    units = 2 * planes
    after, before = (s + 1) % n, (s + n - 1) % n
    f32, bf16 = jnp.float32, jnp.bfloat16

    loads = [
        pltpu.make_async_copy(src, dst, local_sem.at[i])
        for i, (src, dst) in enumerate(
            [
                (gate_hbm, gate_ref), (value_hbm, value_ref), (out_gate_hbm, out_gate_ref),
                (proj_hbm, proj_ref), (res_hbm, res_ref),
                (wg_hbm, gate_w), (wu_hbm, up_w), (wd_hbm, down_w),
            ]
        )
    ]
    for copy in loads[:5]:
        copy.start()

    barrier = pltpu.get_barrier_semaphore()

    @pl.loop(1, n)
    def _(k):
        pl.semaphore_signal(barrier, inc=1, device_id=((s + k) % n, t), device_id_type=MESH)

    @pl.loop(1, planes)
    def _(k):
        to = (z + k) % planes * 2 + y
        pl.semaphore_signal(barrier, inc=1, device_id=(to, across), device_id_type=MESH)

    for peer in (mate, across):
        pl.semaphore_signal(barrier, inc=1, device_id=(s, peer), device_id_type=MESH)

    def remote(src, dst, send_sem, recv_sem, device):
        return pltpu.make_async_remote_copy(
            src_ref=src, dst_ref=dst, send_sem=send_sem, recv_sem=recv_sem,
            device_id=device, device_id_type=MESH,
        )

    own_at = pl.ds(pl.multiple_of(t * quarter, quarter), quarter)
    named = [routes_ref[k:k + 1, own_at] for k in range(2)]
    expert_ids = lax.broadcasted_iota(jnp.int32, (n, quarter), 0)
    one_hot = [(expert_ids == name).astype(f32) for name in named]
    earlier = (
        lax.broadcasted_iota(jnp.int32, (quarter, quarter), 0)
        < lax.broadcasted_iota(jnp.int32, (quarter, quarter), 1)
    ).astype(bf16)
    count = jnp.dot(
        (one_hot[0] + one_hot[1]).astype(bf16), earlier, preferred_element_type=f32
    )
    picks = [
        name.astype(f32) * cap + jnp.sum(count * hot, axis=0, keepdims=True)
        for name, hot in zip(named, one_hot)
    ]
    def tell(k):
        to = (z + k) % planes
        return remote(info.at[z], info.at[z], isend.at[k], igot.at[z], (to * 2 + y, t))

    def told(k):
        origin = (z + k) % planes
        return remote(info.at[origin], info.at[origin], isend.at[k], igot.at[origin], (s, mate))

    for copy in loads[5:]:
        copy.start()

    def tell_far(k):
        to = (z + k) % planes
        return remote(info.at[z], far_info.at[z], fisend.at[k], figot.at[z], (to * 2 + y, across))

    def told_far(origin):
        ref = far_info.at[origin]
        return remote(ref, ref, fisend.at[0], figot.at[origin], (s, mate))

    for copy in loads[:2]:
        copy.wait()
    product[pl.ds(halo, tokens)] = gate_ref[...].astype(f32) * value_ref[...].astype(f32)
    loads[2].wait()
    part_width = width // pieces

    def mix(block):
        at = pl.ds(pl.multiple_of(block * quarter, quarter), quarter)
        window = product[pl.ds(pl.multiple_of(block * quarter, quarter), halo + quarter)]
        conv_sum = (
            taps_ref[0:1] * window[halo - 2:halo - 2 + quarter]
            + taps_ref[1:2] * window[halo - 1:halo - 1 + quarter]
            + taps_ref[2:3] * window[halo:]
        )
        mixed[at] = (out_gate_ref[at].astype(f32) * conv_sum).astype(bf16)

    @pl.loop(1, tp)
    def _(block):
        mix(block)

    def columns(p):
        return pl.ds(p * part_width, part_width)

    def project(block, p):
        at = pl.ds(pl.multiple_of(block * quarter, quarter), quarter)
        y_block = jnp.dot(mixed[at], proj_ref[:, columns(p)], preferred_element_type=f32)
        mpart[block, p] = y_block.astype(bf16)

    loads[3].wait()
    opens = mate_across == 0
    ahead = jnp.where(opens, across, mate_across)
    for p in range(pieces):
        project(ahead, p)

    tail = pl.ds(tokens - halo, halo)
    edges = [
        remote(ref.at[tail], edge.at[i], msend.at[i], mgot.at[i], (after, t))
        for i, ref in enumerate((gate_ref, value_ref))
    ]
    pl.semaphore_wait(barrier, n + planes)
    for copy in edges:
        copy.start()


    def first_block(block):
        @pl.when(block == 0)
        def _():
            for copy in edges:
                copy.wait_recv()
            prior = edge[0].astype(f32) * edge[1].astype(f32)
            product[pl.ds(0, halo)] = jnp.where(s == 0, 0.0, prior)
            mix(block)

    def lane(kind, p):
        return 2 + kind * pieces + p

    def to_mate(kind, block, p):
        at = lane(kind, p)
        return remote(mpart.at[block, p], mmate.at[kind, p], msend.at[at], mgot.at[at], (s, mate))

    def to_across(p):
        at = lane(2, p)
        return remote(msum.at[p], mfar.at[p], msend.at[at], mgot.at[at], (s, across))

    def cross_sum(p):
        to_mate(0, mate_across, p).wait_recv()
        msum[p] = (mpart[across, p].astype(f32) + mmate[0, p].astype(f32)).astype(bf16)
        to_across(p).start()

    @pl.when(opens)
    def _():
        for p in range(pieces):
            cross_sum(p)
        first_block(mate_across)
        for p in range(pieces):
            project(mate_across, p)
            to_mate(0, mate_across, p).start()

    @pl.when(jnp.logical_not(opens))
    def _():
        for p in range(pieces):
            to_mate(0, mate_across, p).start()
        first_block(across)
        for p in range(pieces):
            project(across, p)
            cross_sum(p)

    first_block(mate)
    for p in range(pieces):
        project(mate, p)
        to_mate(1, mate, p).start()
    first_block(t)
    for p in range(pieces):
        project(t, p)

    slot_ids = lax.broadcasted_iota(jnp.int32, (n * cap, quarter), 0).astype(f32)
    share = jnp.where(slot_ids == picks[0], weights_ref[0:1, own_at], 0.0) + jnp.where(
        slot_ids == picks[1], weights_ref[1:2, own_at], 0.0
    )
    share = jnp.transpose(share)
    high = share.astype(bf16)
    spread[0] = high
    spread[1] = (share - high.astype(f32)).astype(bf16)

    def along(block, up, at=slice(None)):
        to = jnp.where(up == 1, z + 1, z - 1)
        ref = raw.at[block, :, at]
        return remote(ref, ref, rsend.at[up, block], rgot.at[block], (to * 2 + y, t))

    def has_up(block):
        return (block <= z) & (z < planes - 1)

    def has_down(block):
        return (block >= z) & (z > 0)

    def pass_on(block):
        @pl.when(has_up(block))
        def _():
            along(block, 1).start()

        @pl.when(has_down(block))
        def _():
            along(block, 0).start()

    first_columns, last_columns = pl.ds(0, early), pl.ds(early, width - early)

    def cross():
        return remote(
            raw.at[z, :, first_columns], far_raw.at[z], csend.at[0], frgot.at[z], (s, across)
        )

    def along_far(block, up):
        to = jnp.where(up == 1, z + 1, z - 1)
        ref = far_raw.at[block]
        return remote(ref, ref, frsend.at[up, block], frgot.at[block], (to * 2 + y, t))

    loads[4].wait()
    square = jnp.zeros((quarter, 1), f32)
    for p in range(pieces):
        at = columns(p)
        to_mate(1, mate, p).wait_recv()
        to_across(p).wait_recv()
        summed = mpart[t, p].astype(f32) + mmate[1, p].astype(f32) + mfar[p].astype(f32)
        hidden_rows = res_ref[:, at].astype(f32) + summed
        rows[:, at] = hidden_rows
        raw[z, :, at] = (hidden_rows * gain_ref[:, at]).astype(bf16)
        for up, has in ((1, has_up), (0, has_down)):
            @pl.when(has(z))
            def _():
                along(z, up, at).start()

        if p == (early - 1) // part_width:
            cross().start()
        square = square + jnp.sum(hidden_rows * hidden_rows, axis=-1, keepdims=True)
    inverse = lax.rsqrt(square / width + 1e-05)
    scale = jnp.transpose(jnp.broadcast_to(inverse, (quarter, quarter)))[0:1]
    info[z] = jnp.concatenate(picks + [scale, jnp.zeros((5, quarter), f32)], axis=0)

    @pl.loop(1, planes)
    def _(k):
        tell(k).start()

    @pl.loop(0, planes)
    def _(k):
        tell_far(k).start()

    def beside(j, h):
        return remote(
            ysend.at[j, h], recv.at[j, h, t, y], ysem.at[0], ygot.at[j, h], (z * 2 + other_y, t)
        )

    def beside_far(j, h):
        return remote(
            far_ysend.at[j, h], recv.at[j, h, across, y, :, first_columns],
            fysem.at[0], fygot.at[j, h], (z * 2 + other_y, t),
        )

    def over(j, h, source):
        ref = recv.at[j, h, t, source, :, last_columns]
        return remote(ref, ref, dsend.at[0], dgot.at[0, j, h, source], (s, across))

    def pair_own(j, h, source):
        ref = recv.at[j, h, t, source]
        return remote(ref, ref, dsend.at[1], dgot.at[1, j, h, source], (s, mate))

    def pair_far(j, h, source):
        ref = recv.at[j, h, across, source]
        return remote(ref, ref, dsend.at[2], dgot.at[2, j, h, source], (s, mate))

    wide = min(512, width)

    def select(raw, info, block, expert, put):
        place = lax.broadcasted_iota(jnp.int32, (cap, quarter), 0).astype(f32) + (
            expert * cap
        ).astype(f32)
        table = info[block]
        named = (place == table[0:1]) | (place == table[1:2])
        chosen = named.astype(f32).astype(bf16)
        scale = jnp.sum(jnp.where(named, table[2:3], 0.0), axis=1, keepdims=True)

        step = raw.shape[2] if raw.shape[2] % wide else wide

        @pl.loop(0, raw.shape[2] // step)
        def _(c):
            at = pl.ds(pl.multiple_of(c * step, step), step)
            taken = jnp.dot(chosen, raw[block, :, at], preferred_element_type=f32)
            taken = (taken * scale).astype(bf16)
            for h in range(2):
                put(h, at, taken[h * half:(h + 1) * half])

    def arrive_far(j):
        block = plane_of(j, z, planes)
        along_far(block, 1).wait_recv()

        @pl.when(has_up(block))
        def _():
            along_far(block, 1).start()

        @pl.when(has_down(block))
        def _():
            along_far(block, 0).start()

    def dispatch_early(j):
        block = plane_of(j, z, planes)
        told_far(block).wait_recv()

        def put_own(h, at, value):
            recv[j, h, across, y, :, at] = value

        def put_other(h, at, value):
            far_ysend[j, h, :, at] = value

        select(far_raw, far_info, block, z * 2 + other_y, put_other)
        for h in range(2):
            beside_far(j, h).start()
        select(far_raw, far_info, block, s, put_own)

    def arrive(j):
        block = plane_of(j, z, planes)
        along(block, 1).wait_recv()
        pass_on(block)

    def hear(j):
        @pl.when(j > 0)
        def _():
            told((plane_of(j, z, planes) + planes - z) % planes).wait_recv()

    def dispatch_own(j):
        def put(h, at, value):
            recv[j, h, t, y, :, at] = value

        select(raw, info, plane_of(j, z, planes), s, put)
        for h in range(2):
            over(j, h, y).start()
            pair_own(j, h, y).start()

    def dispatch_other(j):
        def put(h, at, value):
            ysend[j, h, :, at] = value

        select(raw, info, plane_of(j, z, planes), z * 2 + other_y, put)
        for h in range(2):
            beside(j, h).start()

    def dispatch_beside(j):
        for h in range(2):
            beside(j, h).wait_recv()
            over(j, h, other_y).start()
            pair_own(j, h, other_y).start()

    def dispatch_far(j, source, crossed):
        for h in range(2):
            over(j, h, source).wait_recv()
            if crossed:
                beside_far(j, h).wait_recv()
            pair_far(j, h, source).start()

    def part_near(u):
        return remote(part.at[u, mate], mrecv.at[u, 0], psend.at[0], pgot.at[0, u], (s, mate))

    def part_far(u):
        return remote(part.at[u, mate_across], mrecv.at[u, 1], psend.at[1], pgot.at[1, u], (s, mate))

    def sum_over(u):
        return remote(psum.at[u], xrecv.at[u], psend.at[2], pgot.at[2, u], (s, across))

    def ffn(j, h):
        u = 2 * j + h
        for source in range(2):
            pair_own(j, h, source).wait_recv()
            pair_far(j, h, source).wait_recv()
        count = gate_w.shape[1]
        cols = min(512, count)

        @pl.loop(0, count // cols)
        def _(c):
            at = pl.ds(pl.multiple_of(c * cols, cols), cols)
            x = recv[j, h].reshape(tp * cap, width)
            gate = jnp.dot(x, gate_w[:, at], preferred_element_type=f32)
            up = jnp.dot(x, up_w[:, at], preferred_element_type=f32)
            hid[:, at] = (gate / (1.0 + jnp.exp(-gate)) * up).astype(bf16)

        @pl.loop(0, width // wide)
        def _(c):
            at = pl.ds(pl.multiple_of(c * wide, wide), wide)
            out = jnp.dot(hid[...], down_w[:, at], preferred_element_type=f32)
            part[u, :, :, :, at] = out.reshape(tp, 2, half, wide).astype(bf16)

        part_far(u).start()
        part_near(u).start()

    def homeward(j, h, source):
        u = 2 * j + h
        to = plane_of(j, z, planes) * 2 + source
        return remote(fin.at[u, source], ret.at[s, h], hsend.at[0], hgot.at[s, h], (to, t))

    def returned(origin, h):
        return remote(ret.at[origin, h], ret.at[origin, h], hsend.at[0], hgot.at[origin, h], (s, mate))

    def sum_far(j, h):
        u = 2 * j + h
        part_far(u).wait_recv()
        psum[u] = (part[u, across].astype(f32) + mrecv[u, 1].astype(f32)).astype(bf16)
        sum_over(u).start()

    def send_home(j, h):
        u = 2 * j + h
        part_near(u).wait_recv()
        sum_over(u).wait_recv()
        total = (
            part[u, t].astype(f32) + mrecv[u, 0].astype(f32) + xrecv[u].astype(f32)
        ).astype(bf16)
        fin[u] = total

        @pl.when(j == 0)
        def _():
            ret[s, h] = fin[u, y]
            homeward(j, h, other_y).start()

        @pl.when(j > 0)
        def _():
            for source in range(2):
                homeward(j, h, source).start()

    def gather(plane, put):
        for source in range(2):
            for h in range(2):
                origin = plane * 2 + source

                @pl.when(origin != s)
                def _():
                    returned(origin, h).wait_recv()

        slots = pl.ds(pl.multiple_of(plane * 2 * cap, 2 * cap), 2 * cap)

        @pl.loop(0, width // wide)
        def _(c):
            at = pl.ds(pl.multiple_of(c * wide, wide), wide)
            got = ret[pl.ds(plane * 2, 2), :, :, at].reshape(2 * cap, wide)
            put(
                at,
                rows[:, at]
                + jnp.dot(spread[0, :, slots], got, preferred_element_type=f32)
                + jnp.dot(spread[1, :, slots], got, preferred_element_type=f32),
            )

    def keep(at, value):
        rows[:, at] = value

    def finish(at, value):
        out_ref[:, at] = value.astype(bf16)

    at_end = (z == 0) | (z == planes - 1)
    late = jnp.where(at_end, 1, 0)

    def far_near(j):
        dispatch_far(j, y, False)

    def far_other(j):
        dispatch_far(j, other_y, True)

    def home_pair(j):
        send_home(j, 0)
        send_home(j, 1)

    def take(j):
        hear(j)
        dispatch_own(j)
        dispatch_other(j)

    last = planes - 1
    middle_start = [
        (dispatch_own, 0), (arrive_far, 0), (arrive, 1), (arrive, last), (hear, 1),
        (dispatch_other, 1), (dispatch_own, 1), (arrive_far, 1), (arrive_far, last),
        (dispatch_early, 1), (hear, last), (dispatch_other, last), (dispatch_early, last),
        (far_near, 1), (dispatch_beside, 1), (dispatch_own, last), (dispatch_other, 0),
        (dispatch_early, 0), (far_other, 1),
    ]
    middle_after = [
        [
            (arrive, 2), (sum_far, 1, 0), (dispatch_beside, last), (take, 2), (arrive_far, 2),
            (dispatch_early, 2),
        ],
        [(sum_far, 1, 1), (send_home, 1, 0), (far_near, last), (far_other, last), (dispatch_beside, 2)],
        [(sum_far, last, 0), (far_near, 2), (send_home, 1, 1), (far_other, 2)],
        [(sum_far, 2, 0), (send_home, last, 0)],
        [(sum_far, last, 1), (dispatch_beside, 0)],
        [
            (send_home, 2, 0), (sum_far, 2, 1), (far_near, 0), (send_home, last, 1),
            (far_other, 0),
        ],
        [(sum_far, 0, 0)],
        [(sum_far, 0, 1), (send_home, 2, 1)],
    ]
    end_start = [
        (dispatch_own, 0), (dispatch_other, 0), (arrive_far, 0), (arrive, 1), (dispatch_early, 0),
        (dispatch_beside, 0), (take, 1), (arrive_far, 1), (dispatch_early, 1),
        (far_near, 0), (far_other, 0),
    ]
    end_after = [
        [(sum_far, 0, 0), (dispatch_beside, 1)],
        [
            (arrive, 2), (take, 2), (arrive_far, 2), (dispatch_early, 2),
            (far_near, 1), (far_other, 1),
        ],
        [(dispatch_beside, 2)],
        [
            (sum_far, 1, 0), (arrive, last), (take, last), (arrive_far, last),
            (dispatch_early, last), (far_near, 2), (far_other, 2),
        ],
        [(sum_far, 2, 0), (send_home, 1, 0), (dispatch_beside, last)],
        [(sum_far, 2, 1), (far_near, last), (send_home, 2, 0), (far_other, last)],
        [(sum_far, last, 0)],
        [
            (send_home, 2, 1), (sum_far, last, 1), (sum_far, 1, 1), (sum_far, 0, 1),
            (send_home, 0, 0), (send_home, last, 0), (send_home, last, 1), (send_home, 1, 1),
        ],
    ]

    def carry_out(actions):
        for act, *where in actions:
            act(*[jnp.int32(place) for place in where])

    @pl.when(late == 0)
    def _():
        carry_out(middle_start)

    @pl.when(late == 1)
    def _():
        carry_out(end_start)

    for copy in loads[5:]:
        copy.wait()

    @pl.loop(0, units)
    def _(k):
        woven = (k > 1) & (k < units - 2)
        middle_plane = jnp.where(k < 2, 1, jnp.where(woven, jnp.where(k % 2 == 0, last, 2), 0))
        middle_half = jnp.where(woven, k // planes, k % 2)
        ffn(jnp.where(late == 1, k // 2, middle_plane), jnp.where(late == 1, k % 2, middle_half))
        for step in range(units):
            @pl.when((k == step) & (late == 0))
            def _():
                carry_out(middle_after[step])

            @pl.when((k == step) & (late == 1))
            def _():
                carry_out(end_after[step])

    @pl.when(late == 1)
    def _():
        send_home(jnp.int32(0), jnp.int32(1))

    @pl.loop(1, planes - 1)
    def _(j):
        gather(plane_of(j + late, z, planes), keep)

    @pl.when(late == 0)
    def _():
        send_home(jnp.int32(0), jnp.int32(0))
        send_home(jnp.int32(0), jnp.int32(1))

    gather(plane_of(jnp.where(late == 1, 1, planes - 1), z, planes), keep)
    for copy in edges:
        copy.wait_send()
    for p in range(pieces):
        to_mate(0, mate_across, p).wait_send()
        to_mate(1, mate, p).wait_send()
        to_across(p).wait_send()

    @pl.loop(0, planes)
    def _(j):
        @pl.when(j > 0)
        def _():
            tell(j).wait_send()

        tell_far(j).wait_send()

        @pl.when(has_up(j))
        def _():
            along(j, 1).wait_send()
            along_far(j, 1).wait_send()

        @pl.when(has_down(j))
        def _():
            along(j, 0).wait_send()
            along_far(j, 0).wait_send()

    cross().wait_send()

    def sent(ref, sem):
        remote(ref, ref, sem, rgot.at[z], (s, mate)).wait_send()

    sent(ysend, ysem.at[0])
    sent(far_ysend, fysem.at[0])
    sent(recv.at[:, :, t, :, :, last_columns], dsend.at[0])
    sent(recv.at[:, :, t], dsend.at[1])
    sent(recv.at[:, :, across], dsend.at[2])
    sent(part.at[:, mate], psend.at[0])
    sent(part.at[:, mate_across], psend.at[1])
    sent(psum, psend.at[2])
    gather(z, finish)
    sent(fin.at[pl.ds(0, units - 1)], hsend.at[0])


def relay_body(
    gate_in, value_in, gate_out, conv_taps, proj_weight, residual, norm_gain,
    routes, route_weight, expert_gate, expert_up, expert_down,
):
    n, tp = lax.axis_size("sp"), lax.axis_size("tp")
    tokens, channels = gate_in.shape
    quarter, width = residual.shape
    cap = 2 * quarter * routes.shape[1] // n
    units_hidden = expert_gate.shape[2]
    planes, half = n // 2, cap // 2
    units = 2 * planes
    halo, pieces = 16, 8
    early = width // 1024 * 384
    part_width = width // pieces
    vmem = pl.BlockSpec(memory_space=pltpu.VMEM)
    hbm = pl.BlockSpec(memory_space=pl.ANY)
    bf16, f32 = jnp.bfloat16, jnp.float32
    dma = pltpu.SemaphoreType.DMA
    rows = (2, half, width)
    return pl.pallas_call(
        functools.partial(layer_kernel, n, tp, halo, pieces, cap, early),
        out_shape=jax.ShapeDtypeStruct((quarter, width), bf16),
        in_specs=[vmem] * 4 + [hbm] * 8,
        out_specs=vmem,
        scratch_shapes=[
            pltpu.VMEM((tokens, channels), bf16),
            pltpu.VMEM((tokens, channels), bf16),
            pltpu.VMEM((tokens, channels), bf16),
            pltpu.VMEM(proj_weight.shape, bf16),
            pltpu.VMEM((quarter, width), bf16),
            pltpu.VMEM((width, units_hidden), bf16),
            pltpu.VMEM((width, units_hidden), bf16),
            pltpu.VMEM((units_hidden, width), bf16),
            pltpu.VMEM((2, halo, channels), bf16),
            pltpu.VMEM((halo + tokens, channels), f32),
            pltpu.VMEM((tokens, channels), bf16),
            pltpu.VMEM((tp, pieces, quarter, part_width), bf16),
            pltpu.VMEM((2, pieces, quarter, part_width), bf16),
            pltpu.VMEM((pieces, quarter, part_width), bf16),
            pltpu.VMEM((pieces, quarter, part_width), bf16),
            pltpu.VMEM((quarter, width), f32),
            pltpu.VMEM((planes, 8, quarter), f32),
            pltpu.VMEM((planes, 8, quarter), f32),
            pltpu.VMEM((2, quarter, n * cap), bf16),
            pltpu.VMEM((planes, quarter, width), bf16),
            pltpu.VMEM((planes, quarter, early), bf16),
            pltpu.VMEM((planes,) + rows, bf16),
            pltpu.VMEM((planes, 2, half, early), bf16),
            pltpu.VMEM((planes, 2, tp) + rows, bf16),
            pltpu.VMEM((units, tp) + rows, bf16),
            pltpu.VMEM((units, 2) + rows, bf16),
            pltpu.VMEM((units,) + rows, bf16),
            pltpu.VMEM((units,) + rows, bf16),
            pltpu.VMEM((units,) + rows, bf16),
            pltpu.VMEM((n,) + rows, bf16),
            pltpu.VMEM((tp * cap, units_hidden), bf16),
            dma((8,)),
            dma((2 + 3 * pieces,)),
            dma((2 + 3 * pieces,)),
            dma((planes,)),
            dma((planes,)),
            dma((2, planes)),
            dma((planes,)),
            dma((1,)),
            dma((planes, 2)),
            dma((3,)),
            dma((3, planes, 2, 2)),
            dma((3,)),
            dma((3, units)),
            dma((1,)),
            dma((n, 2)),
            dma((1,)),
            dma((planes,)),
            dma((planes,)),
            dma((2, planes)),
            dma((planes,)),
            dma((1,)),
            dma((planes, 2)),
        ],
        compiler_params=pltpu.CompilerParams(
            collective_id=3, has_side_effects=True, vmem_limit_bytes=60 * 1024 * 1024
        ),
    )(
        routes.T, route_weight.T, conv_taps, norm_gain.reshape(1, width),
        gate_in, value_in, gate_out, proj_weight, residual,
        expert_gate[0], expert_up[0], expert_down[0],
    )


def body(*args):
    residual, routes = args[5], args[7]
    n, tp = lax.axis_size("sp"), lax.axis_size("tp")
    quarter = residual.shape[0]
    capacity = 2 * quarter * routes.shape[1] // n
    relay = n == 2 * tp and tp == 4 and capacity % 32 == 0 and quarter % 128 == 0 and residual.shape[1] % 1024 == 0
    if relay and (n // 2) * quarter <= n * capacity:
        return relay_body(*args)
    return exchange_body(*args)


def solution(mesh):
    placed = (
        P("sp", "tp"),
        P("sp", "tp"),
        P("sp", "tp"),
        P(None, "tp"),
        P("tp", None),
        P(("sp", "tp"), None),
        P(),
        P("sp", None),
        P("sp", None),
        P("sp", None, "tp"),
        P("sp", None, "tp"),
        P("sp", "tp", None),
    )
    return jax.shard_map(
        body, mesh=mesh, in_specs=placed, out_specs=P(("sp", "tp"), None), check_vma=False
    )
```

```python
import functools

import jax
import jax.numpy as jnp
from jax import lax
from jax.experimental import pallas as pl
from jax.experimental.pallas import tpu as pltpu
from jax.sharding import PartitionSpec as P


def slot_numbers(route_ids, block_rows, expert_count):
    block_count = route_ids.shape[0] // block_rows
    flat_ids = route_ids.reshape(block_count, block_rows * route_ids.shape[1])
    one_hot = (
        flat_ids[:, :, None] == jnp.arange(expert_count, dtype=jnp.int32)[None, None, :]
    ).astype(jnp.int32)
    before = jnp.cumsum(one_hot, axis=1) - one_hot
    return jnp.sum(before * one_hot, axis=2).reshape(route_ids.shape)


def dispatch_rows(normed, flat_pick, slot_count):
    slot_ids = jnp.arange(slot_count, dtype=jnp.int32)
    chosen = jnp.any(flat_pick[None, :, :] == slot_ids[:, None, None], axis=2)
    return jnp.dot(
        chosen.astype(jnp.bfloat16), normed, preferred_element_type=jnp.float32
    ).astype(jnp.bfloat16)


MESH = pl.DeviceIdType.MESH


def mixer_kernel(
    n, tp, halo, pieces, gate_ref, value_ref, out_gate_ref, taps_ref, proj_ref, res_ref, gain_ref,
    rows_ref, normed_ref, edge, product, mixed, part, mrecv, psum, xrecv, send, got,
):
    s = lax.axis_index("sp")
    t = lax.axis_index("tp")
    mate = t + 1 - 2 * (t % 2)
    across = (t + 2) % tp
    mate_across = (mate + 2) % tp
    tokens = gate_ref.shape[0]
    quarter, width = res_ref.shape
    piece = quarter // pieces
    after, before = (s + 1) % n, (s + n - 1) % n

    barrier = pltpu.get_barrier_semaphore()
    for peer in ((s, mate), (s, across), (after, t), (before, t)):
        pl.semaphore_signal(barrier, inc=1, device_id=peer, device_id_type=MESH)

    def remote(src, dst, lane, device):
        return pltpu.make_async_remote_copy(
            src_ref=src,
            dst_ref=dst,
            send_sem=send.at[lane],
            recv_sem=got.at[lane],
            device_id=device,
            device_id_type=MESH,
        )

    tail = pl.ds(tokens - halo, halo)
    edges = [
        remote(ref.at[tail], edge.at[i], i, (after, t))
        for i, ref in enumerate((gate_ref, value_ref))
    ]
    pl.semaphore_wait(barrier, 4)
    for copy in edges:
        copy.start()

    body_rows = pl.ds(halo, tokens)
    product[body_rows] = gate_ref[...].astype(jnp.float32) * value_ref[...].astype(jnp.float32)
    for copy in edges:
        copy.wait_recv()
    prior = edge[0].astype(jnp.float32) * edge[1].astype(jnp.float32)
    product[pl.ds(0, halo)] = jnp.where(s == 0, 0.0, prior)
    conv_sum = (
        taps_ref[0:1] * product[pl.ds(halo - 2, tokens)]
        + taps_ref[1:2] * product[pl.ds(halo - 1, tokens)]
        + taps_ref[2:3] * product[body_rows]
    )
    mixed[...] = (out_gate_ref[...].astype(jnp.float32) * conv_sum).astype(jnp.bfloat16)

    def project(block, p):
        first = pl.multiple_of(block * quarter + p * piece, piece)
        y = jnp.dot(
            mixed[pl.ds(first, piece)], proj_ref[...], preferred_element_type=jnp.float32
        )
        part[block, p] = y.astype(jnp.bfloat16)

    def lane(kind, p):
        return 2 + kind * pieces + p

    def to_mate(kind, block, p):
        return remote(part.at[block, p], mrecv.at[kind, p], lane(kind, p), (s, mate))

    def over(p):
        return remote(psum.at[p], xrecv.at[p], lane(2, p), (s, across))

    def wide(block):
        return block.astype(jnp.float32)

    for p in range(pieces):
        project(mate_across, p)
        to_mate(0, mate_across, p).start()
    for p in range(pieces):
        project(across, p)
        to_mate(0, mate_across, p).wait_recv()
        psum[p] = (wide(part[across, p]) + wide(mrecv[0, p])).astype(jnp.bfloat16)
        over(p).start()
    for p in range(pieces):
        project(mate, p)
        to_mate(1, mate, p).start()
    for p in range(pieces):
        project(t, p)
    for p in range(pieces):
        to_mate(1, mate, p).wait_recv()
        over(p).wait_recv()
        at = pl.ds(p * piece, piece)
        summed = wide(part[t, p]) + wide(mrecv[1, p]) + wide(xrecv[p])
        hidden_rows = wide(res_ref[at]) + summed
        inverse = lax.rsqrt(jnp.mean(hidden_rows * hidden_rows, axis=-1, keepdims=True) + 1e-05)
        rows_ref[at] = hidden_rows
        normed_ref[at] = (hidden_rows * inverse * gain_ref[...]).astype(jnp.bfloat16)
    for copy in edges:
        copy.wait_send()
    for p in range(pieces):
        to_mate(0, mate_across, p).wait_send()
        to_mate(1, mate, p).wait_send()
        over(p).wait_send()


def run_mixer(gate_in, value_in, gate_out, conv_taps, proj_weight, residual, norm_gain):
    n, tp = lax.axis_size("sp"), lax.axis_size("tp")
    tokens, channels = gate_in.shape
    quarter, width = residual.shape
    halo, pieces = 16, 4
    piece = quarter // pieces
    vmem = pl.BlockSpec(memory_space=pltpu.VMEM)
    bf16, f32 = jnp.bfloat16, jnp.float32
    return pl.pallas_call(
        functools.partial(mixer_kernel, n, tp, halo, pieces),
        out_shape=(
            jax.ShapeDtypeStruct((quarter, width), f32),
            jax.ShapeDtypeStruct((quarter, width), bf16),
        ),
        in_specs=[vmem] * 7,
        out_specs=(vmem, vmem),
        scratch_shapes=[
            pltpu.VMEM((2, halo, channels), bf16),
            pltpu.VMEM((halo + tokens, channels), f32),
            pltpu.VMEM((tokens, channels), bf16),
            pltpu.VMEM((tp, pieces, piece, width), bf16),
            pltpu.VMEM((2, pieces, piece, width), bf16),
            pltpu.VMEM((pieces, piece, width), bf16),
            pltpu.VMEM((pieces, piece, width), bf16),
            pltpu.SemaphoreType.DMA((2 + 3 * pieces,)),
            pltpu.SemaphoreType.DMA((2 + 3 * pieces,)),
        ],
        compiler_params=pltpu.CompilerParams(
            collective_id=2, has_side_effects=True, vmem_limit_bytes=60 * 1024 * 1024
        ),
    )(gate_in, value_in, gate_out, conv_taps, proj_weight, residual, norm_gain.reshape(1, width))


def expert_kernel(
    n, tp, halves, out_ref, gate_hbm, up_hbm, down_hbm, ret_ref,
    recv, part, mrecv, psum, xrecv, fin, gate_w, up_w, down_w, hid, local_sem, send, got,
):
    s = lax.axis_index("sp")
    t = lax.axis_index("tp")
    mate = t + 1 - 2 * (t % 2)
    across = (t + 2) % tp
    mate_across = (mate + 2) % tp
    cap, width = out_ref.shape[1], out_ref.shape[2]
    units = gate_w.shape[1]
    rows = tp * cap
    steps = n * halves

    weight_copies = [
        pltpu.make_async_copy(src, dst, local_sem.at[i])
        for i, (src, dst) in enumerate(
            [(gate_hbm, gate_w), (up_hbm, up_w), (down_hbm, down_w)]
        )
    ]
    for copy in weight_copies:
        copy.start()

    barrier = pltpu.get_barrier_semaphore()

    @pl.loop(1, n)
    def _(k):
        pl.semaphore_signal(barrier, inc=1, device_id=((s + k) % n, t), device_id_type=MESH)

    for peer in (mate, across):
        pl.semaphore_signal(barrier, inc=1, device_id=(s, peer), device_id_type=MESH)
    pl.semaphore_wait(barrier, n + 1)

    def remote(src, dst, lane, k, device):
        return pltpu.make_async_remote_copy(
            src_ref=src,
            dst_ref=dst,
            send_sem=send.at[lane, k],
            recv_sem=got.at[lane, k],
            device_id=device,
            device_id_type=MESH,
        )

    def outward(k):
        to = (s + k // halves) % n
        return remote(out_ref.at[to * halves + k % halves], recv.at[k, t], 0, k, (to, t))

    def over(k, block):
        return remote(recv.at[k, block], recv.at[k, block], 1, k, (s, across))

    def pair_own(k, block):
        return remote(recv.at[k, block], recv.at[k, block], 2, k, (s, mate))

    def pair_far(k, block):
        return remote(recv.at[k, block], recv.at[k, block], 3, k, (s, mate))

    def part_near(k):
        return remote(part.at[k, mate], mrecv.at[k, 0], 4, k, (s, mate))

    def part_far(k):
        return remote(part.at[k, mate_across], mrecv.at[k, 1], 5, k, (s, mate))

    def sum_over(k):
        return remote(psum.at[k], xrecv.at[k], 6, k, (s, across))

    def homeward(k):
        to = (s + n - k // halves) % n
        return remote(fin.at[k], ret_ref.at[s * halves + k % halves], 7, k, (to, t))

    own = [
        pltpu.make_async_copy(out_ref.at[s * halves + h], recv.at[h, t], local_sem.at[3 + h])
        for h in range(halves)
    ]
    for copy in own:
        copy.start()

    @pl.loop(halves, steps)
    def _(k):
        outward(k).start()

    for copy in own:
        copy.wait()

    def ffn(k):
        def load():
            block = recv[k]
            if cap % 16:
                return block.astype(jnp.float32).reshape(rows, width).astype(jnp.bfloat16)
            return block.reshape(rows, width)

        cols = min(256, units)

        @pl.loop(0, units // cols)
        def _(c):
            at = pl.ds(pl.multiple_of(c * cols, cols), cols)
            x = load()
            gate = jnp.dot(x, gate_w[:, at], preferred_element_type=jnp.float32)
            up = jnp.dot(x, up_w[:, at], preferred_element_type=jnp.float32)
            hid[:, at] = (gate / (1.0 + jnp.exp(-gate)) * up).astype(jnp.bfloat16)

        wide = min(512, width)

        @pl.loop(0, width // wide)
        def _(c):
            at = pl.ds(pl.multiple_of(c * wide, wide), wide)
            y = jnp.dot(hid[...], down_w[:, at], preferred_element_type=jnp.float32)
            part[k, :, :, at] = y.reshape(tp, cap, wide).astype(jnp.bfloat16)

    def wide_sum(*blocks):
        total = blocks[0].astype(jnp.float32)
        for block in blocks[1:]:
            total = total + block.astype(jnp.float32)
        return total

    @pl.loop(0, steps + 4)
    def _(i):
        @pl.when(i < steps)
        def _():
            @pl.when(i >= halves)
            def _():
                outward(i).wait_recv()

            over(i, t).start()
            pair_own(i, t).start()

        @pl.when((i >= 1) & (i < steps + 1))
        def _():
            k = i - 1
            over(k, across).wait_recv()
            pair_far(k, across).start()

        @pl.when((i >= 3) & (i < steps + 3))
        def _():
            k = i - 3
            part_far(k).wait_recv()
            psum[k] = wide_sum(part[k, across], mrecv[k, 1]).astype(jnp.bfloat16)
            sum_over(k).start()

        @pl.when(i >= 4)
        def _():
            k = i - 4
            part_near(k).wait_recv()
            sum_over(k).wait_recv()
            total = wide_sum(part[k, t], mrecv[k, 0], xrecv[k]).astype(jnp.bfloat16)

            @pl.when(k < halves)
            def _():
                ret_ref[s * halves + k] = total

            @pl.when(k >= halves)
            def _():
                fin[k] = total
                homeward(k).start()

        @pl.when(i == 2)
        def _():
            for copy in weight_copies:
                copy.wait()

        @pl.when((i >= 2) & (i < steps + 2))
        def _():
            k = i - 2
            pair_own(k, mate).wait_recv()
            pair_far(k, mate_across).wait_recv()
            ffn(k)
            part_far(k).start()
            part_near(k).start()

    @pl.loop(0, steps)
    def _(k):
        over(k, t).wait_send()
        pair_own(k, t).wait_send()
        pair_far(k, across).wait_send()
        part_near(k).wait_send()
        part_far(k).wait_send()
        sum_over(k).wait_send()

        @pl.when(k >= halves)
        def _():
            outward(k).wait_send()
            homeward(k).wait_send()
            homeward(k).wait_recv()


def run_experts(outgoing, gate_weight, up_weight, down_weight):
    n, cap, width = outgoing.shape
    tp = lax.axis_size("tp")
    units = gate_weight.shape[1]
    halves = 2 if cap % 32 == 0 else 1
    steps, cap = n * halves, cap // halves
    vmem = pl.BlockSpec(memory_space=pltpu.VMEM)
    hbm = pl.BlockSpec(memory_space=pl.ANY)
    bf16 = jnp.bfloat16
    return pl.pallas_call(
        functools.partial(expert_kernel, n, tp, halves),
        out_shape=jax.ShapeDtypeStruct((steps, cap, width), bf16),
        in_specs=[vmem, hbm, hbm, hbm],
        out_specs=vmem,
        scratch_shapes=[
            pltpu.VMEM((steps, tp, cap, width), bf16),
            pltpu.VMEM((steps, tp, cap, width), bf16),
            pltpu.VMEM((steps, 2, cap, width), bf16),
            pltpu.VMEM((steps, cap, width), bf16),
            pltpu.VMEM((steps, cap, width), bf16),
            pltpu.VMEM((steps, cap, width), bf16),
            pltpu.VMEM(gate_weight.shape, bf16),
            pltpu.VMEM(up_weight.shape, bf16),
            pltpu.VMEM(down_weight.shape, bf16),
            pltpu.VMEM((tp * cap, units), bf16),
            pltpu.SemaphoreType.DMA((3 + halves,)),
            pltpu.SemaphoreType.DMA((8, steps)),
            pltpu.SemaphoreType.DMA((8, steps)),
        ],
        compiler_params=pltpu.CompilerParams(
            collective_id=1, has_side_effects=True, vmem_limit_bytes=60 * 1024 * 1024
        ),
    )(outgoing.reshape(steps, cap, width), gate_weight, up_weight, down_weight)


def exchange_body(
    gate_in,
    value_in,
    gate_out,
    conv_taps,
    proj_weight,
    residual,
    norm_gain,
    routes,
    route_weight,
    expert_gate,
    expert_up,
    expert_down,
):
    model_width = residual.shape[1]
    tp_count = lax.axis_size("tp")
    groups = lax.axis_size("sp")
    quarter = residual.shape[0]
    top_count = routes.shape[1]
    capacity = 2 * quarter * top_count // groups
    tp_index = lax.axis_index("tp")
    first_own = tp_index * quarter
    own_routes = lax.dynamic_slice_in_dim(routes, first_own, quarter, 0)
    own_weights = lax.dynamic_slice_in_dim(route_weight, first_own, quarter, 0)
    my_rows, normed = run_mixer(
        gate_in, value_in, gate_out, conv_taps, proj_weight, residual, norm_gain
    )
    own_slots = slot_numbers(own_routes, quarter, groups)
    flat_pick = own_routes * capacity + own_slots
    slot_count = groups * capacity
    outgoing = dispatch_rows(normed, flat_pick, slot_count)
    returned = run_experts(
        outgoing.reshape(groups, capacity, model_width),
        expert_gate[0],
        expert_up[0],
        expert_down[0],
    ).reshape(slot_count, model_width)
    total = my_rows
    for k in range(top_count):
        pick = flat_pick[:, k, None] == jnp.arange(slot_count, dtype=jnp.int32)
        picked = jnp.dot(
            pick.astype(jnp.bfloat16), returned, preferred_element_type=jnp.float32
        )
        total = total + own_weights[:, k, None] * picked
    return total.astype(jnp.bfloat16)


def plane_of(j, z, planes):
    return jnp.where(z < planes // 2, z + j, z + planes - j) % planes


def layer_kernel(
    n, tp, halo, pieces, cap, early,
    routes_ref, weights_ref, taps_ref, gain_ref,
    gate_hbm, value_hbm, out_gate_hbm, proj_hbm, res_hbm, wg_hbm, wu_hbm, wd_hbm,
    out_ref,
    gate_ref, value_ref, out_gate_ref, proj_ref, res_ref, gate_w, up_w, down_w,
    edge, product, mixed, mpart, mmate, msum, mfar,
    rows, info, far_info, spread, raw, far_raw, ysend, far_ysend, recv, part, mrecv, psum, xrecv,
    fin, ret, hid,
    local_sem, msend, mgot, isend, igot, rsend, rgot, ysem, ygot, dsend, dgot, psend, pgot, hsend, hgot,
    csend, fisend, figot, frsend, frgot, fysem, fygot,
):
    s = lax.axis_index("sp")
    t = lax.axis_index("tp")
    planes = n // 2
    z, y = s // 2, s % 2
    other_y = 1 - y
    mate = t + 1 - 2 * (t % 2)
    across = (t + 2) % tp
    mate_across = (mate + 2) % tp
    tokens = gate_ref.shape[0]
    quarter, width = res_ref.shape
    half = cap // 2
    units = 2 * planes
    after, before = (s + 1) % n, (s + n - 1) % n
    f32, bf16 = jnp.float32, jnp.bfloat16

    loads = [
        pltpu.make_async_copy(src, dst, local_sem.at[i])
        for i, (src, dst) in enumerate(
            [
                (gate_hbm, gate_ref), (value_hbm, value_ref), (out_gate_hbm, out_gate_ref),
                (proj_hbm, proj_ref), (res_hbm, res_ref),
                (wg_hbm, gate_w), (wu_hbm, up_w), (wd_hbm, down_w),
            ]
        )
    ]
    for copy in loads[:5]:
        copy.start()

    barrier = pltpu.get_barrier_semaphore()

    @pl.loop(1, n)
    def _(k):
        pl.semaphore_signal(barrier, inc=1, device_id=((s + k) % n, t), device_id_type=MESH)

    @pl.loop(1, planes)
    def _(k):
        to = (z + k) % planes * 2 + y
        pl.semaphore_signal(barrier, inc=1, device_id=(to, across), device_id_type=MESH)

    for peer in (mate, across):
        pl.semaphore_signal(barrier, inc=1, device_id=(s, peer), device_id_type=MESH)

    def remote(src, dst, send_sem, recv_sem, device):
        return pltpu.make_async_remote_copy(
            src_ref=src, dst_ref=dst, send_sem=send_sem, recv_sem=recv_sem,
            device_id=device, device_id_type=MESH,
        )

    own_at = pl.ds(pl.multiple_of(t * quarter, quarter), quarter)
    named = [routes_ref[k:k + 1, own_at] for k in range(2)]
    expert_ids = lax.broadcasted_iota(jnp.int32, (n, quarter), 0)
    one_hot = [(expert_ids == name).astype(f32) for name in named]
    earlier = (
        lax.broadcasted_iota(jnp.int32, (quarter, quarter), 0)
        < lax.broadcasted_iota(jnp.int32, (quarter, quarter), 1)
    ).astype(bf16)
    count = jnp.dot(
        (one_hot[0] + one_hot[1]).astype(bf16), earlier, preferred_element_type=f32
    )
    picks = [
        name.astype(f32) * cap + jnp.sum(count * hot, axis=0, keepdims=True)
        for name, hot in zip(named, one_hot)
    ]
    def tell(k):
        to = (z + k) % planes
        return remote(info.at[z], info.at[z], isend.at[k], igot.at[z], (to * 2 + y, t))

    def told(k):
        origin = (z + k) % planes
        return remote(info.at[origin], info.at[origin], isend.at[k], igot.at[origin], (s, mate))

    for copy in loads[5:]:
        copy.start()

    def tell_far(k):
        to = (z + k) % planes
        return remote(info.at[z], far_info.at[z], fisend.at[k], figot.at[z], (to * 2 + y, across))

    def told_far(origin):
        ref = far_info.at[origin]
        return remote(ref, ref, fisend.at[0], figot.at[origin], (s, mate))

    for copy in loads[:2]:
        copy.wait()
    product[pl.ds(halo, tokens)] = gate_ref[...].astype(f32) * value_ref[...].astype(f32)
    loads[2].wait()
    part_width = width // pieces

    def mix(block):
        at = pl.ds(pl.multiple_of(block * quarter, quarter), quarter)
        window = product[pl.ds(pl.multiple_of(block * quarter, quarter), halo + quarter)]
        conv_sum = (
            taps_ref[0:1] * window[halo - 2:halo - 2 + quarter]
            + taps_ref[1:2] * window[halo - 1:halo - 1 + quarter]
            + taps_ref[2:3] * window[halo:]
        )
        mixed[at] = (out_gate_ref[at].astype(f32) * conv_sum).astype(bf16)

    @pl.loop(1, tp)
    def _(block):
        mix(block)

    def columns(p):
        return pl.ds(p * part_width, part_width)

    def project(block, p):
        at = pl.ds(pl.multiple_of(block * quarter, quarter), quarter)
        y_block = jnp.dot(mixed[at], proj_ref[:, columns(p)], preferred_element_type=f32)
        mpart[block, p] = y_block.astype(bf16)

    loads[3].wait()
    opens = mate_across == 0
    ahead = jnp.where(opens, across, mate_across)
    for p in range(pieces):
        project(ahead, p)

    tail = pl.ds(tokens - halo, halo)
    edges = [
        remote(ref.at[tail], edge.at[i], msend.at[i], mgot.at[i], (after, t))
        for i, ref in enumerate((gate_ref, value_ref))
    ]
    pl.semaphore_wait(barrier, n + planes)
    for copy in edges:
        copy.start()


    def first_block(block):
        @pl.when(block == 0)
        def _():
            for copy in edges:
                copy.wait_recv()
            prior = edge[0].astype(f32) * edge[1].astype(f32)
            product[pl.ds(0, halo)] = jnp.where(s == 0, 0.0, prior)
            mix(block)

    def lane(kind, p):
        return 2 + kind * pieces + p

    def to_mate(kind, block, p):
        at = lane(kind, p)
        return remote(mpart.at[block, p], mmate.at[kind, p], msend.at[at], mgot.at[at], (s, mate))

    def to_across(p):
        at = lane(2, p)
        return remote(msum.at[p], mfar.at[p], msend.at[at], mgot.at[at], (s, across))

    def cross_sum(p):
        to_mate(0, mate_across, p).wait_recv()
        msum[p] = (mpart[across, p].astype(f32) + mmate[0, p].astype(f32)).astype(bf16)
        to_across(p).start()

    @pl.when(opens)
    def _():
        for p in range(pieces):
            cross_sum(p)
        first_block(mate_across)
        for p in range(pieces):
            project(mate_across, p)
            to_mate(0, mate_across, p).start()

    @pl.when(jnp.logical_not(opens))
    def _():
        for p in range(pieces):
            to_mate(0, mate_across, p).start()
        first_block(across)
        for p in range(pieces):
            project(across, p)
            cross_sum(p)

    first_block(mate)
    for p in range(pieces):
        project(mate, p)
        to_mate(1, mate, p).start()
    first_block(t)
    for p in range(pieces):
        project(t, p)

    slot_ids = lax.broadcasted_iota(jnp.int32, (n * cap, quarter), 0).astype(f32)
    share = jnp.where(slot_ids == picks[0], weights_ref[0:1, own_at], 0.0) + jnp.where(
        slot_ids == picks[1], weights_ref[1:2, own_at], 0.0
    )
    share = jnp.transpose(share)
    high = share.astype(bf16)
    spread[0] = high
    spread[1] = (share - high.astype(f32)).astype(bf16)

    def along(block, up, at=slice(None)):
        to = jnp.where(up == 1, z + 1, z - 1)
        ref = raw.at[block, :, at]
        return remote(ref, ref, rsend.at[up, block], rgot.at[block], (to * 2 + y, t))

    def has_up(block):
        return (block <= z) & (z < planes - 1)

    def has_down(block):
        return (block >= z) & (z > 0)

    def pass_on(block):
        @pl.when(has_up(block))
        def _():
            along(block, 1).start()

        @pl.when(has_down(block))
        def _():
            along(block, 0).start()

    first_columns, last_columns = pl.ds(0, early), pl.ds(early, width - early)

    def cross():
        return remote(
            raw.at[z, :, first_columns], far_raw.at[z], csend.at[0], frgot.at[z], (s, across)
        )

    def along_far(block, up):
        to = jnp.where(up == 1, z + 1, z - 1)
        ref = far_raw.at[block]
        return remote(ref, ref, frsend.at[up, block], frgot.at[block], (to * 2 + y, t))

    loads[4].wait()
    square = jnp.zeros((quarter, 1), f32)
    for p in range(pieces):
        at = columns(p)
        to_mate(1, mate, p).wait_recv()
        to_across(p).wait_recv()
        summed = mpart[t, p].astype(f32) + mmate[1, p].astype(f32) + mfar[p].astype(f32)
        hidden_rows = res_ref[:, at].astype(f32) + summed
        rows[:, at] = hidden_rows
        raw[z, :, at] = (hidden_rows * gain_ref[:, at]).astype(bf16)
        for up, has in ((1, has_up), (0, has_down)):
            @pl.when(has(z))
            def _():
                along(z, up, at).start()

        if p == (early - 1) // part_width:
            cross().start()
        square = square + jnp.sum(hidden_rows * hidden_rows, axis=-1, keepdims=True)
    inverse = lax.rsqrt(square / width + 1e-05)
    scale = jnp.transpose(jnp.broadcast_to(inverse, (quarter, quarter)))[0:1]
    info[z] = jnp.concatenate(picks + [scale, jnp.zeros((5, quarter), f32)], axis=0)

    @pl.loop(1, planes)
    def _(k):
        tell(k).start()

    @pl.loop(0, planes)
    def _(k):
        tell_far(k).start()

    def beside(j, h):
        return remote(
            ysend.at[j, h], recv.at[j, h, t, y], ysem.at[0], ygot.at[j, h], (z * 2 + other_y, t)
        )

    def beside_far(j, h):
        return remote(
            far_ysend.at[j, h], recv.at[j, h, across, y, :, first_columns],
            fysem.at[0], fygot.at[j, h], (z * 2 + other_y, t),
        )

    def over(j, h, source):
        ref = recv.at[j, h, t, source, :, last_columns]
        return remote(ref, ref, dsend.at[0], dgot.at[0, j, h, source], (s, across))

    def pair_own(j, h, source):
        ref = recv.at[j, h, t, source]
        return remote(ref, ref, dsend.at[1], dgot.at[1, j, h, source], (s, mate))

    def pair_far(j, h, source):
        ref = recv.at[j, h, across, source]
        return remote(ref, ref, dsend.at[2], dgot.at[2, j, h, source], (s, mate))

    wide = min(1024, width)

    def select(raw, info, block, expert, put):
        place = lax.broadcasted_iota(jnp.int32, (cap, quarter), 0).astype(f32) + (
            expert * cap
        ).astype(f32)
        table = info[block]
        named = (place == table[0:1]) | (place == table[1:2])
        chosen = named.astype(f32).astype(bf16)
        scale = jnp.sum(jnp.where(named, table[2:3], 0.0), axis=1, keepdims=True)

        step = raw.shape[2] if raw.shape[2] % wide else wide

        @pl.loop(0, raw.shape[2] // step)
        def _(c):
            at = pl.ds(pl.multiple_of(c * step, step), step)
            taken = jnp.dot(chosen, raw[block, :, at], preferred_element_type=f32)
            taken = (taken * scale).astype(bf16)
            for h in range(2):
                put(h, at, taken[h * half:(h + 1) * half])

    def arrive_far(j):
        block = plane_of(j, z, planes)
        along_far(block, 1).wait_recv()

        @pl.when(has_up(block))
        def _():
            along_far(block, 1).start()

        @pl.when(has_down(block))
        def _():
            along_far(block, 0).start()

    def dispatch_early(j):
        block = plane_of(j, z, planes)
        told_far(block).wait_recv()

        def put_own(h, at, value):
            recv[j, h, across, y, :, at] = value

        def put_other(h, at, value):
            far_ysend[j, h, :, at] = value

        select(far_raw, far_info, block, z * 2 + other_y, put_other)
        for h in range(2):
            beside_far(j, h).start()
        select(far_raw, far_info, block, s, put_own)

    def arrive(j):
        block = plane_of(j, z, planes)
        along(block, 1).wait_recv()
        pass_on(block)

    def hear(j):
        @pl.when(j > 0)
        def _():
            told((plane_of(j, z, planes) + planes - z) % planes).wait_recv()

    def dispatch_own(j):
        def put(h, at, value):
            recv[j, h, t, y, :, at] = value

        select(raw, info, plane_of(j, z, planes), s, put)
        for h in range(2):
            over(j, h, y).start()
            pair_own(j, h, y).start()

    def dispatch_other(j):
        def put(h, at, value):
            ysend[j, h, :, at] = value

        select(raw, info, plane_of(j, z, planes), z * 2 + other_y, put)
        for h in range(2):
            beside(j, h).start()

    def dispatch_beside(j):
        for h in range(2):
            beside(j, h).wait_recv()
            over(j, h, other_y).start()
            pair_own(j, h, other_y).start()

    def dispatch_far(j, source, crossed):
        for h in range(2):
            over(j, h, source).wait_recv()
            if crossed:
                beside_far(j, h).wait_recv()
            pair_far(j, h, source).start()

    def part_near(u):
        return remote(part.at[u, mate], mrecv.at[u, 0], psend.at[0], pgot.at[0, u], (s, mate))

    def part_far(u):
        return remote(part.at[u, mate_across], mrecv.at[u, 1], psend.at[1], pgot.at[1, u], (s, mate))

    def sum_over(u):
        return remote(psum.at[u], xrecv.at[u], psend.at[2], pgot.at[2, u], (s, across))

    def ffn(j, h):
        u = 2 * j + h
        for source in range(2):
            pair_own(j, h, source).wait_recv()
            pair_far(j, h, source).wait_recv()
        count = gate_w.shape[1]
        cols = min(512, count)

        @pl.loop(0, count // cols)
        def _(c):
            at = pl.ds(pl.multiple_of(c * cols, cols), cols)
            x = recv[j, h].reshape(tp * cap, width)
            gate = jnp.dot(x, gate_w[:, at], preferred_element_type=f32)
            up = jnp.dot(x, up_w[:, at], preferred_element_type=f32)
            hid[:, at] = (gate / (1.0 + jnp.exp(-gate)) * up).astype(bf16)

        @pl.loop(0, width // wide)
        def _(c):
            at = pl.ds(pl.multiple_of(c * wide, wide), wide)
            out = jnp.dot(hid[...], down_w[:, at], preferred_element_type=f32)
            part[u, :, :, :, at] = out.reshape(tp, 2, half, wide).astype(bf16)

        part_far(u).start()
        part_near(u).start()

    def homeward(j, h, source):
        u = 2 * j + h
        to = plane_of(j, z, planes) * 2 + source
        return remote(fin.at[u, source], ret.at[s, h], hsend.at[0], hgot.at[s, h], (to, t))

    def returned(origin, h):
        return remote(ret.at[origin, h], ret.at[origin, h], hsend.at[0], hgot.at[origin, h], (s, mate))

    def sum_far(j, h):
        u = 2 * j + h
        part_far(u).wait_recv()
        psum[u] = (part[u, across].astype(f32) + mrecv[u, 1].astype(f32)).astype(bf16)
        sum_over(u).start()

    def send_home(j, h):
        u = 2 * j + h
        part_near(u).wait_recv()
        sum_over(u).wait_recv()
        total = (
            part[u, t].astype(f32) + mrecv[u, 0].astype(f32) + xrecv[u].astype(f32)
        ).astype(bf16)
        fin[u] = total

        @pl.when(j == 0)
        def _():
            ret[s, h] = fin[u, y]
            homeward(j, h, other_y).start()

        @pl.when(j > 0)
        def _():
            for source in range(2):
                homeward(j, h, source).start()

    def gather(plane, put):
        for source in range(2):
            for h in range(2):
                origin = plane * 2 + source

                @pl.when(origin != s)
                def _():
                    returned(origin, h).wait_recv()

        slots = pl.ds(pl.multiple_of(plane * 2 * cap, 2 * cap), 2 * cap)

        @pl.loop(0, width // wide)
        def _(c):
            at = pl.ds(pl.multiple_of(c * wide, wide), wide)
            got = ret[pl.ds(plane * 2, 2), :, :, at].reshape(2 * cap, wide)
            put(
                at,
                rows[:, at]
                + jnp.dot(spread[0, :, slots], got, preferred_element_type=f32)
                + jnp.dot(spread[1, :, slots], got, preferred_element_type=f32),
            )

    def keep(at, value):
        rows[:, at] = value

    def finish(at, value):
        out_ref[:, at] = value.astype(bf16)

    at_end = (z == 0) | (z == planes - 1)
    late = jnp.where(at_end, 1, 0)

    def far_near(j):
        dispatch_far(j, y, False)

    def far_other(j):
        dispatch_far(j, other_y, True)

    def home_pair(j):
        send_home(j, 0)
        send_home(j, 1)

    def take(j):
        hear(j)
        dispatch_own(j)
        dispatch_other(j)

    last = planes - 1
    middle_start = [
        (dispatch_own, 0), (arrive_far, 0), (arrive, 1), (arrive, last), (hear, 1),
        (dispatch_other, 1), (dispatch_own, 1), (arrive_far, 1), (arrive_far, last),
        (dispatch_early, 1), (hear, last), (dispatch_other, last), (dispatch_early, last),
        (far_near, 1), (dispatch_beside, 1), (dispatch_own, last), (dispatch_other, 0),
        (dispatch_early, 0), (far_other, 1),
    ]
    middle_after = [
        [
            (arrive, 2), (sum_far, 1, 0), (dispatch_beside, last), (take, 2), (arrive_far, 2),
            (dispatch_early, 2),
        ],
        [(sum_far, 1, 1), (send_home, 1, 0), (far_near, last), (far_other, last), (dispatch_beside, 2)],
        [(sum_far, last, 0), (far_near, 2), (send_home, 1, 1), (far_other, 2)],
        [(sum_far, 2, 0), (send_home, last, 0)],
        [(sum_far, last, 1), (dispatch_beside, 0)],
        [
            (send_home, 2, 0), (sum_far, 2, 1), (far_near, 0), (send_home, last, 1),
            (far_other, 0),
        ],
        [(sum_far, 0, 0)],
        [(sum_far, 0, 1), (send_home, 2, 1)],
    ]
    end_start = [
        (dispatch_own, 0), (dispatch_other, 0), (arrive_far, 0), (arrive, 1), (dispatch_early, 0),
        (dispatch_beside, 0), (take, 1), (arrive_far, 1), (dispatch_early, 1),
        (far_near, 0), (far_other, 0),
    ]
    end_after = [
        [(sum_far, 0, 0), (dispatch_beside, 1)],
        [
            (arrive, 2), (take, 2), (arrive_far, 2), (dispatch_early, 2),
            (far_near, 1), (far_other, 1),
        ],
        [(dispatch_beside, 2)],
        [
            (sum_far, 1, 0), (arrive, last), (take, last), (arrive_far, last),
            (dispatch_early, last), (far_near, 2), (far_other, 2),
        ],
        [(sum_far, 2, 0), (send_home, 1, 0), (dispatch_beside, last)],
        [(sum_far, 2, 1), (far_near, last), (send_home, 2, 0), (far_other, last)],
        [(sum_far, last, 0)],
        [
            (send_home, 2, 1), (sum_far, last, 1), (sum_far, 1, 1), (sum_far, 0, 1),
            (send_home, 0, 0), (send_home, last, 0), (send_home, last, 1), (send_home, 1, 1),
        ],
    ]

    def carry_out(actions):
        for act, *where in actions:
            act(*[jnp.int32(place) for place in where])

    @pl.when(late == 0)
    def _():
        carry_out(middle_start)

    @pl.when(late == 1)
    def _():
        carry_out(end_start)

    for copy in loads[5:]:
        copy.wait()

    @pl.loop(0, units)
    def _(k):
        woven = (k > 1) & (k < units - 2)
        middle_plane = jnp.where(k < 2, 1, jnp.where(woven, jnp.where(k % 2 == 0, last, 2), 0))
        middle_half = jnp.where(woven, k // planes, k % 2)
        ffn(jnp.where(late == 1, k // 2, middle_plane), jnp.where(late == 1, k % 2, middle_half))
        for step in range(units):
            @pl.when((k == step) & (late == 0))
            def _():
                carry_out(middle_after[step])

            @pl.when((k == step) & (late == 1))
            def _():
                carry_out(end_after[step])

    @pl.when(late == 1)
    def _():
        send_home(jnp.int32(0), jnp.int32(1))

    @pl.loop(1, planes - 1)
    def _(j):
        gather(plane_of(j + late, z, planes), keep)

    @pl.when(late == 0)
    def _():
        send_home(jnp.int32(0), jnp.int32(0))
        send_home(jnp.int32(0), jnp.int32(1))

    gather(plane_of(jnp.where(late == 1, 1, planes - 1), z, planes), keep)
    for copy in edges:
        copy.wait_send()
    for p in range(pieces):
        to_mate(0, mate_across, p).wait_send()
        to_mate(1, mate, p).wait_send()
        to_across(p).wait_send()

    @pl.loop(0, planes)
    def _(j):
        @pl.when(j > 0)
        def _():
            tell(j).wait_send()

        tell_far(j).wait_send()

        @pl.when(has_up(j))
        def _():
            along(j, 1).wait_send()
            along_far(j, 1).wait_send()

        @pl.when(has_down(j))
        def _():
            along(j, 0).wait_send()
            along_far(j, 0).wait_send()

    cross().wait_send()

    def sent(ref, sem):
        remote(ref, ref, sem, rgot.at[z], (s, mate)).wait_send()

    sent(ysend, ysem.at[0])
    sent(far_ysend, fysem.at[0])
    sent(recv.at[:, :, t, :, :, last_columns], dsend.at[0])
    sent(recv.at[:, :, t], dsend.at[1])
    sent(recv.at[:, :, across], dsend.at[2])
    sent(part.at[:, mate], psend.at[0])
    sent(part.at[:, mate_across], psend.at[1])
    sent(psum, psend.at[2])
    gather(z, finish)
    sent(fin.at[pl.ds(0, units - 1)], hsend.at[0])


def relay_body(
    gate_in, value_in, gate_out, conv_taps, proj_weight, residual, norm_gain,
    routes, route_weight, expert_gate, expert_up, expert_down,
):
    n, tp = lax.axis_size("sp"), lax.axis_size("tp")
    tokens, channels = gate_in.shape
    quarter, width = residual.shape
    cap = 2 * quarter * routes.shape[1] // n
    units_hidden = expert_gate.shape[2]
    planes, half = n // 2, cap // 2
    units = 2 * planes
    halo, pieces = 16, 8
    early = width // 1024 * 384
    part_width = width // pieces
    vmem = pl.BlockSpec(memory_space=pltpu.VMEM)
    hbm = pl.BlockSpec(memory_space=pl.ANY)
    bf16, f32 = jnp.bfloat16, jnp.float32
    dma = pltpu.SemaphoreType.DMA
    rows = (2, half, width)
    return pl.pallas_call(
        functools.partial(layer_kernel, n, tp, halo, pieces, cap, early),
        out_shape=jax.ShapeDtypeStruct((quarter, width), bf16),
        in_specs=[vmem] * 4 + [hbm] * 8,
        out_specs=vmem,
        scratch_shapes=[
            pltpu.VMEM((tokens, channels), bf16),
            pltpu.VMEM((tokens, channels), bf16),
            pltpu.VMEM((tokens, channels), bf16),
            pltpu.VMEM(proj_weight.shape, bf16),
            pltpu.VMEM((quarter, width), bf16),
            pltpu.VMEM((width, units_hidden), bf16),
            pltpu.VMEM((width, units_hidden), bf16),
            pltpu.VMEM((units_hidden, width), bf16),
            pltpu.VMEM((2, halo, channels), bf16),
            pltpu.VMEM((halo + tokens, channels), f32),
            pltpu.VMEM((tokens, channels), bf16),
            pltpu.VMEM((tp, pieces, quarter, part_width), bf16),
            pltpu.VMEM((2, pieces, quarter, part_width), bf16),
            pltpu.VMEM((pieces, quarter, part_width), bf16),
            pltpu.VMEM((pieces, quarter, part_width), bf16),
            pltpu.VMEM((quarter, width), f32),
            pltpu.VMEM((planes, 8, quarter), f32),
            pltpu.VMEM((planes, 8, quarter), f32),
            pltpu.VMEM((2, quarter, n * cap), bf16),
            pltpu.VMEM((planes, quarter, width), bf16),
            pltpu.VMEM((planes, quarter, early), bf16),
            pltpu.VMEM((planes,) + rows, bf16),
            pltpu.VMEM((planes, 2, half, early), bf16),
            pltpu.VMEM((planes, 2, tp) + rows, bf16),
            pltpu.VMEM((units, tp) + rows, bf16),
            pltpu.VMEM((units, 2) + rows, bf16),
            pltpu.VMEM((units,) + rows, bf16),
            pltpu.VMEM((units,) + rows, bf16),
            pltpu.VMEM((units,) + rows, bf16),
            pltpu.VMEM((n,) + rows, bf16),
            pltpu.VMEM((tp * cap, units_hidden), bf16),
            dma((8,)),
            dma((2 + 3 * pieces,)),
            dma((2 + 3 * pieces,)),
            dma((planes,)),
            dma((planes,)),
            dma((2, planes)),
            dma((planes,)),
            dma((1,)),
            dma((planes, 2)),
            dma((3,)),
            dma((3, planes, 2, 2)),
            dma((3,)),
            dma((3, units)),
            dma((1,)),
            dma((n, 2)),
            dma((1,)),
            dma((planes,)),
            dma((planes,)),
            dma((2, planes)),
            dma((planes,)),
            dma((1,)),
            dma((planes, 2)),
        ],
        compiler_params=pltpu.CompilerParams(
            collective_id=3, has_side_effects=True, vmem_limit_bytes=60 * 1024 * 1024
        ),
    )(
        routes.T, route_weight.T, conv_taps, norm_gain.reshape(1, width),
        gate_in, value_in, gate_out, proj_weight, residual,
        expert_gate[0], expert_up[0], expert_down[0],
    )


def body(*args):
    residual, routes = args[5], args[7]
    n, tp = lax.axis_size("sp"), lax.axis_size("tp")
    quarter = residual.shape[0]
    capacity = 2 * quarter * routes.shape[1] // n
    relay = n == 2 * tp and tp == 4 and capacity % 32 == 0 and quarter % 128 == 0 and residual.shape[1] % 1024 == 0
    if relay and (n // 2) * quarter <= n * capacity:
        return relay_body(*args)
    return exchange_body(*args)


def solution(mesh):
    placed = (
        P("sp", "tp"),
        P("sp", "tp"),
        P("sp", "tp"),
        P(None, "tp"),
        P("tp", None),
        P(("sp", "tp"), None),
        P(),
        P("sp", None),
        P("sp", None),
        P("sp", None, "tp"),
        P("sp", None, "tp"),
        P("sp", "tp", None),
    )
    return jax.shard_map(
        body, mesh=mesh, in_specs=placed, out_specs=P(("sp", "tp"), None), check_vma=False
    )
```
